32 devices in a mesh: fs: 16 (over z, y, x), tp: 2 (over core).
Axes of the slice: x: 2, y: 2, z: 4, core: 2. Of those that a mesh axis runs over, the one named last changes fastest.
Arguments:
- tokens: bfloat16 [8192, 2048], P('fs', 'tp'), may hold values from -24 to 24
- u_weight: bfloat16 [2048, 1024], P('fs', 'tp'), may hold values from -0.125 to 0.125
- v_weight: bfloat16 [2048, 1024], P('fs', 'tp'), may hold values from -0.125 to 0.125
- sg_gain: float32 [1024], P('tp'), may hold values from 0.1 to 1.9
- spatial_weight: bfloat16 [8, 128, 128], P('tp'), may hold values from -0.5 to 0.5
- spatial_bias: float32 [8, 128], P('tp'), may hold values from 0.1 to 1.9
- out_weight: bfloat16 [1024, 2048], P('tp', 'fs'), may hold values from -0.1875 to 0.1875
- gain_one: float32 [2048], P('tp'), may hold values from 0.1 to 1.9
- gate_weight: bfloat16 [2048, 5632], P('fs', 'tp'), may hold values from -0.125 to 0.125
- up_weight: bfloat16 [2048, 5632], P('fs', 'tp'), may hold values from -0.125 to 0.125
- down_weight: bfloat16 [5632, 2048], P('tp', 'fs'), may hold values from -0.078125 to 0.078125
- gain_two: float32 [2048], P('tp'), may hold values from 0.1 to 1.9
Outputs:
- layer_out: bfloat16 [8192, 2048], P('fs', 'tp')
The draws below stay inside these ranges and needn't reach their ends.
All inputs are finite; a program needn't handle non-finite values.
Results may differ from the reference program's by a relative error of at most 0.014.
Values may be sent and summed in bfloat16 or wider, within the bound.
A program may use at most 128 MiB of HBM per device.

```python
import math
import jax
import jax.numpy as jnp
from jax import lax

D = 2048
FF = 5632
GROUPS = 8
GROUP_DIM = 128
BLOCK = 128
D_SG = 1024
TOKENS = 8192
N_TP = 2


def draw_tokens(key, part):
    first_key, second_key, third_key = jax.random.split(jax.random.fold_in(key, 11), 3)
    width = D // 16
    scales = jnp.exp(jax.random.uniform(second_key, (16,), jnp.float32, -math.log(4.0), math.log(4.0)))
    base = jax.random.normal(first_key, (TOKENS, D), jnp.float32)
    base = jnp.clip(base, -6.0, 6.0)
    return (base * jnp.repeat(scales, width)[None, :]).astype(jnp.bfloat16)


def steps_of(key, shape, pieces, least, high):
    factor_of, own = 1.0, jax.random.fold_in(key, 6)
    for position, blocks in pieces:
        draws = jnp.exp(jax.random.uniform(jax.random.fold_in(own, position), (blocks,), jnp.float32, least / len(pieces), high / len(pieces)))
        factor_of = factor_of * jnp.repeat(draws, shape[position] // blocks).reshape([-1 if axis == position else 1 for axis in range(len(shape))])
    return factor_of


def bell_draw(rng, extent, deviation, most, shards=(), kind=jnp.bfloat16):
    entries = deviation * jax.random.normal(rng, extent, jnp.float32)
    if shards:
        entries = entries * steps_of(rng, extent, shards, -0.22, 0.18)
    return jnp.clip(entries, -most, most).astype(kind)


def setup_inputs(seed: int = 0) -> dict:
    seeds = jax.random.split(jax.random.key(seed), 13)
    tokens = draw_tokens(jax.random.fold_in(seeds[12], 71), 0)
    u_weight = bell_draw(seeds[1], (D, D_SG), D ** -0.5, 0.125, ((0, 16), (1, 2)))
    v_weight = bell_draw(seeds[2], (D, D_SG), D ** -0.5, 0.125, ((0, 16), (1, 2)))
    sg_gain = jnp.clip(1.0 + 0.18 * jax.random.normal(seeds[3], (D_SG,), jnp.float32), 0.1, 1.9)
    spatial_weight = bell_draw(seeds[4], (GROUPS, BLOCK, BLOCK), BLOCK ** -0.5, 0.5, ((0, 2),))
    spatial_bias = jnp.clip(1.0 + 0.18 * jax.random.normal(seeds[5], (GROUPS, BLOCK), jnp.float32), 0.1, 1.9)
    out_weight = bell_draw(seeds[6], (D_SG, D), D_SG ** -0.5, 0.1875, ((0, 2), (1, 16)))
    gain_one = jnp.clip(1.0 + 0.18 * jax.random.normal(seeds[7], (D,), jnp.float32), 0.1, 1.9)
    gate_weight = bell_draw(seeds[8], (D, FF), D ** -0.5, 0.125, ((0, 16), (1, 2)))
    up_weight = bell_draw(seeds[9], (D, FF), D ** -0.5, 0.125, ((0, 16), (1, 2)))
    down_weight = bell_draw(seeds[10], (FF, D), FF ** -0.5, 0.078125, ((0, 2), (1, 16)))
    gain_two = jnp.clip(1.0 + 0.18 * jax.random.normal(seeds[11], (D,), jnp.float32), 0.1, 1.9)
    return {"tokens": tokens, "u_weight": u_weight, "v_weight": v_weight, "sg_gain": sg_gain, "spatial_weight": spatial_weight, "spatial_bias": spatial_bias, "out_weight": out_weight, "gain_one": gain_one, "gate_weight": gate_weight, "up_weight": up_weight, "down_weight": down_weight, "gain_two": gain_two}


EPS = 1e-05
ALPHA = 2.0 ** 0.25

def norm_rows(vals, gain):
    count = vals.shape[1]
    mean = lax.optimization_barrier(jnp.sum(vals, axis=1, keepdims=True)) / count
    square = lax.optimization_barrier(jnp.sum(vals * vals, axis=1, keepdims=True)) / count
    return (vals - mean) * lax.rsqrt(square - mean * mean + EPS) * gain.astype(jnp.float32)[None, :]

def split_sum(left, weight):
    width = weight.shape[0] // N_TP
    total = jnp.zeros((left.shape[0], weight.shape[1]), jnp.float32)
    for index in range(N_TP):
        part = jnp.dot(left[:, index * width:(index + 1) * width], weight[index * width:(index + 1) * width], preferred_element_type=jnp.float32).astype(jnp.bfloat16)
        part = lax.optimization_barrier(part)
        total = total + part.astype(jnp.float32)
    return total.astype(jnp.bfloat16)

def reference(tokens, u_weight, v_weight, sg_gain, spatial_weight, spatial_bias, out_weight, gain_one, gate_weight, up_weight, down_weight, gain_two):
    gated = jax.nn.gelu(jnp.dot(tokens, u_weight, preferred_element_type=jnp.float32))
    valued = jax.nn.gelu(jnp.dot(tokens, v_weight, preferred_element_type=jnp.float32))
    normed = norm_rows(valued, sg_gain).astype(jnp.bfloat16)
    blocks = TOKENS // BLOCK
    shaped = normed.reshape(blocks, BLOCK, GROUPS, GROUP_DIM).astype(jnp.float32)
    lower = jnp.tril(jnp.ones((BLOCK, BLOCK), jnp.float32))
    masked = spatial_weight.astype(jnp.float32) * lower[None]
    mixed = jnp.einsum('gij,njgd->nigd', masked, shaped)
    mixed = mixed + spatial_bias.astype(jnp.float32).T[None, :, :, None]
    gated_out = (gated * mixed.reshape(TOKENS, D_SG)).astype(jnp.bfloat16)
    mix = split_sum(gated_out, out_weight)
    first = norm_rows(ALPHA * tokens.astype(jnp.float32) + mix.astype(jnp.float32), gain_one).astype(jnp.bfloat16)
    gate = jnp.dot(first, gate_weight, preferred_element_type=jnp.float32)
    upper = jnp.dot(first, up_weight, preferred_element_type=jnp.float32)
    hidden = (jax.nn.silu(gate) * upper).astype(jnp.bfloat16)
    ffn = split_sum(hidden, down_weight)
    layer_out = norm_rows(ALPHA * first.astype(jnp.float32) + ffn.astype(jnp.float32), gain_two)
    return layer_out.astype(jnp.bfloat16)
```

```python
import functools

import jax
import jax.numpy as jnp
from jax import lax
from jax.experimental import pallas as pl
from jax.experimental.pallas import tpu as pltpu
from jax.sharding import PartitionSpec as P

EPS = 1e-05
ALPHA = 2.0**0.25


def add_rows(left, piece):
    return jnp.dot(left, piece, preferred_element_type=jnp.float32)


def scaled_rows(vals, sums, gain, count):
    mean = sums[0][:, None] / count
    square = sums[1][:, None] / count
    return (vals - mean) * lax.rsqrt(square - mean * mean + EPS) * gain[None, :]


def chip_sizes(count):
    across = 2 if count % 2 == 0 else 1
    down = 2 if (count // across) % 2 == 0 else 1
    return count // (across * down), down, across


def shift(value, sizes, axis, step=1):
    count = sizes[0] * sizes[1] * sizes[2]
    stride = sizes[1] * sizes[2] if axis == 0 else (sizes[2] if axis == 1 else 1)
    pairs = []
    for source in range(count):
        place = (source // stride) % sizes[axis]
        pairs.append((source, source + ((place + step) % sizes[axis] - place) * stride))
    return lax.ppermute(value, "fs", pairs)


def around(value, sizes, axis):
    if sizes[axis] == 4:
        near = shift(value, sizes, axis, 1)
        last = shift(value, sizes, axis, -1)
        return [value, near, shift(near, sizes, axis, 1), last]
    pieces = [value]
    for _ in range(sizes[axis] - 1):
        pieces.append(shift(pieces[-1], sizes, axis))
    return pieces


def ring(value, sizes, axis, place):
    return in_order(around(value, sizes, axis), place)


def other_core(value):
    return lax.ppermute(value, "tp", [(0, 1), (1, 0)])


def all_features(value):
    if lax.axis_size("tp") != 2:
        return lax.all_gather(value, "tp", axis=1, tiled=True)
    return jnp.concatenate(in_two(value, other_core(value), lax.axis_index("tp")), axis=1)


def in_two(mine, other, place):
    return [jnp.where(place == 0, mine, other), jnp.where(place == 0, other, mine)]


def sum_shares(terms):
    if lax.axis_size("tp") != 2:
        return lax.psum_scatter(terms, "tp", scatter_dimension=1, tiled=True)
    core = lax.axis_index("tp")
    half = terms.shape[1] // 2
    mine = lax.dynamic_slice_in_dim(terms, core * half, half, 1)
    sent = lax.dynamic_slice_in_dim(terms, (1 - core) * half, half, 1)
    return (mine.astype(jnp.float32) + other_core(sent).astype(jnp.float32)).astype(jnp.bfloat16)


def in_order(pieces, place):
    count = len(pieces)
    if count == 1:
        return pieces[0][None]
    held = jnp.zeros((count,) + pieces[0].shape, pieces[0].dtype)
    for step, piece in enumerate(pieces):
        start = lax.rem(place - step + count, count)
        held = lax.dynamic_update_slice_in_dim(held, piece[None], start, 0)
    return held


def gather_all(piece, sizes, places, order):
    held = piece
    for axis in order:
        held = ring(held, sizes, axis, places[axis])
    back = [order[::-1].index(axis) for axis in range(3)]
    rest = [3 + i for i in range(piece.ndim)]
    return jnp.transpose(held, back + rest)


def after(value, *others):
    return lax.optimization_barrier((value,) + others)[0]


def share_pieces(weight, dim, sizes, places, level, marks):
    across = sizes[2]
    width = weight.shape[dim] // across
    if across == 2:
        mine = lax.dynamic_slice_in_dim(weight, places[2] * width, width, dim)
        other = lax.dynamic_slice_in_dim(weight, (1 - places[2]) * width, width, dim)
        block = jnp.stack(in_two(mine, shift(other, sizes, 2), places[2]))
    else:
        block = weight[None]
    if sizes[0] != 4 or sizes[1] != 2:
        first = around(block, sizes, 0)
        return [[piece] if sizes[1] == 1 else [piece, shift(piece, sizes, 1)] for piece in first]
    if marks[0] is not None:
        block = after(block, marks[0])
    near, last = shift(block, sizes, 0, 1), shift(block, sizes, 0, -1)
    beside = shift(block if marks[0] is None else after(block, marks[1]), sizes, 1)
    near, last = after(near, marks[1]), after(last, marks[1])
    far = shift(near, sizes, 0)
    near_beside, last_beside = shift(near, sizes, 1), shift(last, sizes, 1)
    if level:
        far_beside = shift(after(near_beside, marks[2]), sizes, 0)
    else:
        far = after(far, marks[2])
        far_beside = shift(far, sizes, 1)
    return [[block, beside], [near, near_beside], [far, far_beside], [last, last_beside]]


def place_pieces(pieces, places):
    shape = pieces[0][0].shape
    count, down = len(pieces), len(pieces[0])
    held = jnp.zeros((count, down) + shape, pieces[0][0].dtype)
    for step, pair in enumerate(pieces):
        start = lax.rem(places[0] - step + count, count)
        for turn, piece in enumerate(pair):
            spot = places[1] if turn == 0 else 1 - places[1]
            held = lax.dynamic_update_slice(held, piece[None, None], [start, spot] + [0] * len(shape))
    return held


def on_device(
    tokens,
    u_weight,
    v_weight,
    sg_gain,
    spatial_weight,
    spatial_bias,
    out_weight,
    gain_one,
    gate_weight,
    up_weight,
    down_weight,
    gain_two,
):
    parts = lax.axis_size("tp")
    sizes = chip_sizes(lax.axis_size("fs"))
    index = lax.axis_index("fs")
    places = (index // (sizes[1] * sizes[2]), (index // sizes[2]) % sizes[1], index % sizes[2])
    whole = all_features(tokens)
    rows = whole.shape[0]
    width_sg = u_weight.shape[1]

    def add_one(piece):
        return add_rows(whole, piece)

    pre_u = add_one(gather_all(u_weight, sizes, places, [0, 1, 2]).reshape(-1, width_sg))
    pre_v = add_one(gather_all(v_weight, sizes, places, [0, 2, 1]).reshape(-1, width_sg))
    gated = jax.nn.gelu(pre_u)
    valued = jax.nn.gelu(pre_v)
    stats = lax.psum((jnp.sum(valued, axis=1), jnp.sum(valued * valued, axis=1)), "tp")
    normed = scaled_rows(valued, stats, sg_gain, width_sg * parts).astype(jnp.bfloat16)
    groups_here = spatial_weight.shape[0]
    block = spatial_weight.shape[1]
    group_width = width_sg // groups_here
    shaped = normed.reshape(rows // block, block, groups_here, group_width)
    lower = jnp.tril(jnp.ones((block, block), jnp.bool_))
    masked = jnp.where(lower[None], spatial_weight, jnp.zeros_like(spatial_weight))
    mixed = jnp.einsum("gij,njgd->nigd", masked, shaped, preferred_element_type=jnp.float32)
    mixed = mixed + spatial_bias.T[None, :, :, None]
    gated_out = (gated * mixed.reshape(rows, width_sg)).astype(jnp.bfloat16)
    out_all = gather_all(out_weight, sizes, places, [0, 1, 2])
    out_all = out_all.reshape((-1,) + out_weight.shape)
    terms = jnp.einsum("tk,nkc->tnc", gated_out, out_all, preferred_element_type=jnp.float32)
    mix = sum_shares(terms.reshape(rows, -1).astype(jnp.bfloat16))
    resid = ALPHA * tokens.astype(jnp.float32) + mix.astype(jnp.float32)
    first_sums = lax.psum((jnp.sum(resid, axis=1), jnp.sum(resid * resid, axis=1)), "tp")
    first = scaled_rows(resid, first_sums, gain_one, resid.shape[1] * parts).astype(jnp.bfloat16)
    gate_pieces = share_pieces(gate_weight, 1, sizes, places, False, (None, normed, mix))
    up_pieces = share_pieces(up_weight, 1, sizes, places, True, (None, normed, mix))
    down_pieces = share_pieces(down_weight, 0, sizes, places, False, (normed, first, first))
    gate_all = place_pieces(gate_pieces, places)
    gate_all = gate_all.reshape(-1, gate_all.shape[-1])
    up_all = place_pieces(up_pieces, places)
    up_all = up_all.reshape(-1, up_all.shape[-1])
    def feed(part):
        whole_part = all_features(part)
        gate = add_rows(whole_part, gate_all)
        upper = add_rows(whole_part, up_all)
        return (jax.nn.silu(gate) * upper).astype(jnp.bfloat16)

    two = sizes[2] == 2
    if two:
        there = feed(shift(first, sizes, 2))
        here = feed(first)
        down_pieces = [[pair[0]] + [after(piece, there, here) for piece in pair[1:]] for pair in down_pieces]
    else:
        here = feed(first)
    down_all = place_pieces(down_pieces, places)
    down_all = down_all.reshape((-1,) + down_all.shape[-2:])

    def project(hidden):
        made = jnp.einsum("tf,nfc->tnc", hidden, down_all, preferred_element_type=jnp.float32)
        return sum_shares(made.reshape(rows, -1).astype(jnp.bfloat16))

    if two:
        there = project(there)
        sent = shift(there, sizes, 2)
        ffn = project(after(here, there)).astype(jnp.float32) + sent.astype(jnp.float32)
    else:
        ffn = project(here).astype(jnp.float32)
    second = ALPHA * first.astype(jnp.float32) + ffn.astype(jnp.float32)
    last_sums = lax.psum((jnp.sum(second, axis=1), jnp.sum(second * second, axis=1)), "tp")
    return scaled_rows(second, last_sums, gain_two, second.shape[1] * parts).astype(jnp.bfloat16)


MESH = pl.DeviceIdType.MESH
PLANE = 4
HALVES = 2


def layer_kernel(
    sizes,
    tok,
    u_in,
    v_in,
    sg_gain,
    spatial,
    bias,
    o_in,
    gain_one,
    gate_in,
    up_in,
    down_in,
    gain_two,
    out,
    tok_o,
    u_all,
    v_all,
    o_all,
    gate_all,
    up_all,
    down_all,
    gated,
    valued,
    normed,
    gated_out,
    st_s,
    st_r,
    terms_r,
    resid,
    first_all,
    hidden,
    gate_acc,
    p_s,
    p_r,
    p_own,
    r_r,
    sg_r,
    sg_z,
    sg_p,
    a2_s,
    a2_r,
    z_s,
    z_r,
    tok_sem,
    st_sem,
    terms_sem,
    first_s,
    first_r,
    swap_s,
    swap_r,
    d2_s,
    d2_r,
    rs_s,
    rs_r,
):
    nz = sizes[0]
    fs, c = lax.axis_index("fs"), lax.axis_index("tp")
    oc = 1 - c
    z, p = fs // PLANE, fs % PLANE
    y, x = p // 2, p % 2
    peers = [z * PLANE + (y + j // 2) % 2 * 2 + (x + j % 2) % 2 for j in range(PLANE)]
    inplane = [(y + j // 2) % 2 * 2 + (x + j % 2) % 2 for j in range(PLANE)]
    has_up, has_down = z < nz - 1, z > 0
    up_dev = jnp.where(has_up, fs + PLANE, fs - PLANE)
    down_dev = jnp.where(has_down, fs - PLANE, fs + PLANE)
    rows, feats = tok.shape
    kb, width_sg = u_in.shape
    depth = rows // PLANE
    quarter = hidden.shape[1]
    plane_cols = PLANE * kb
    half_cols = plane_cols // HALVES

    def mult(value, by):
        return pl.multiple_of(value, by)

    def seq(k):
        swapped = jnp.where(k < 2, 1 - k, k)
        return jnp.where(z == 0, k, jnp.where(z == 1, swapped, jnp.where(z == 2, nz - 1 - swapped, nz - 1 - k)))

    def remote(src, dst, send, recv, dev, core=None):
        where_to = (dev, c if core is None else core)
        return pltpu.make_async_remote_copy(
            src_ref=src, dst_ref=dst, send_sem=send, recv_sem=recv, device_id=where_to, device_id_type=MESH
        )

    def start_if(pred, copy):
        pl.when(pred)(lambda: copy.start())

    def sent_if(pred, copy):
        pl.when(pred)(lambda: copy.wait_send())

    barrier = pltpu.get_barrier_semaphore()
    for dev, core in [(fs, oc)] + [(peers[j], c) for j in range(1, PLANE)]:
        pl.semaphore_signal(barrier, inc=1, device_id=(dev, core), device_id_type=MESH)
    for pred, dev in [(has_up, up_dev), (has_down, down_dev)]:
        @pl.when(pred)
        def _():
            pl.semaphore_signal(barrier, inc=1, device_id=(dev, c), device_id_type=MESH)
    pl.semaphore_wait(barrier, PLANE + jnp.where(has_up, 1, 0) + jnp.where(has_down, 1, 0))

    def rows_of(ref):
        return lambda i: ref.at[pl.ds(mult(i * kb, kb), kb), :]

    def cols_of(ref, part):
        height = width_sg // 2
        return lambda i: ref.at[pl.ds(part * height, height), pl.ds(mult(i * kb, kb), kb)]

    half_o = width_sg // 2
    items = [
        (u_in, rows_of(u_all), 1, 2),
        (v_in, rows_of(v_all), 2, 1),
        (o_in.at[pl.ds(0, half_o), :], cols_of(o_all, 0), 1, 2),
        (o_in.at[pl.ds(half_o, half_o), :], cols_of(o_all, 1), 2, 1),
    ]

    def own_copies(n):
        src, at, one, two = items[n]
        return [
            (has_up, remote(src, at(fs), sg_z.at[n, 0, 0], sg_r.at[n, fs], up_dev)),
            (has_down, remote(src, at(fs), sg_z.at[n, 0, 1], sg_r.at[n, fs], down_dev)),
            (None, remote(src, at(fs), sg_p.at[n, 0, 0], sg_r.at[n, fs], peers[one])),
            (None, remote(src, at(fs), sg_p.at[n, 0, 1], sg_r.at[n, fs], peers[two])),
        ]

    def own_start(n):
        for pred, copy in own_copies(n):
            if pred is None:
                copy.start()
            else:
                start_if(pred, copy)

    def forward_to(b):
        going_up = b < z
        return (going_up & has_up) | ((b > z) & has_down), jnp.where(going_up, up_dev, down_dev)

    def column_copies(n, k):
        _, at, one, two = items[n]
        b = seq(k)
        idx = b * PLANE + p
        pred, dev = forward_to(b)
        ref, recv = at(idx), sg_r.at[n, idx]
        return [
            (pred, remote(ref, ref, sg_z.at[n, k, 0], recv, dev)),
            (None, remote(ref, ref, sg_p.at[n, k, 0], recv, peers[one])),
            (None, remote(ref, ref, sg_p.at[n, k, 1], recv, peers[two])),
        ]

    def column(n, k):
        copies = column_copies(n, k)
        copies[0][1].wait_recv()
        start_if(*copies[0])
        copies[1][1].start()
        copies[2][1].start()

    def beside_copy(n, k):
        _, at, one, two = items[n]
        idx = seq(k) * PLANE + inplane[one]
        ref, recv = at(idx), sg_r.at[n, idx]
        return remote(ref, ref, sg_p.at[n, k, 2], recv, peers[two])

    def beside(n, k):
        copy = beside_copy(n, k)
        copy.wait_recv()
        copy.start()

    def gathered(n):
        _, at, one, two = items[n]

        def arrive(b, carry):
            for j in (two, 3):
                idx = b * PLANE + inplane[j]
                ref = at(idx)
                remote(ref, ref, sg_p.at[n, 0, 0], sg_r.at[n, idx], peers[two]).wait_recv()
            return carry

        lax.fori_loop(0, nz, arrive, 0)

    wides = [(gate_in, gate_all), (up_in, up_all), (down_in, down_all)]

    def quarter_copy(w, j):
        src, dst = wides[w]
        theirs = pl.ds(mult(inplane[j] * quarter, 16), quarter)
        mine = pl.ds(mult(fs * kb, kb), kb)
        return remote(src.at[theirs, :], dst.at[:, mine], a2_s.at[w, j - 1], a2_r.at[w, j - 1], peers[j])

    def quarters_start(w):
        for j in range(1, PLANE):
            quarter_copy(w, j).start()

    def block(w, b, h):
        return wides[w][1].at[:, pl.ds(mult(b * plane_cols + h * half_cols, half_cols), half_cols)]

    def own_block_copies(w, h):
        ref, recv = block(w, z, h), z_r.at[w, z, h]
        return [
            (has_up, remote(ref, ref, z_s.at[w, 0, h, 0], recv, up_dev)),
            (has_down, remote(ref, ref, z_s.at[w, 0, h, 1], recv, down_dev)),
        ]

    def own_block(w):
        for j in range(1, PLANE):
            ref = wides[w][1].at[:, pl.ds(mult(peers[j] * kb, kb), kb)]
            remote(ref, ref, a2_s.at[w, j - 1], a2_r.at[w, j - 1], peers[j]).wait_recv()
        for h in range(HALVES):
            for pred, copy in own_block_copies(w, h):
                start_if(pred, copy)

    def pass_copy(w, k, h):
        b = seq(k)
        pred, dev = forward_to(b)
        ref = block(w, b, h)
        return pred, remote(ref, ref, z_s.at[w, k, h, 0], z_r.at[w, b, h], dev)

    def pass_on(w, k, h):
        pred, copy = pass_copy(w, k, h)

        @pl.when(pred)
        def _():
            copy.wait_recv()
            copy.start()

    def need(w, k, h):
        pred, copy = pass_copy(w, k, h)
        pl.when(jnp.logical_not(pred))(lambda: copy.wait_recv())

    lane = lax.broadcasted_iota(jnp.int32, (depth, 128), 1)

    def put_stats(which, place, vals):
        one = jnp.sum(vals, axis=1, keepdims=True)
        two = jnp.sum(vals * vals, axis=1, keepdims=True)
        st_s[which, place, :] = jnp.where(lane == 0, one, two)

    def stats_copy(which):
        return remote(st_s.at[which], st_r.at[which], st_sem.at[which, 0], st_sem.at[which, 1], fs, oc)

    def normalize(which, place, vals, gain, count):
        both = st_s[which, place, :] + st_r[which, place, :]
        mean = both[:, 0:1] / count
        square = both[:, 1:2] / count
        return (vals - mean) * lax.rsqrt(square - mean * mean + EPS) * gain

    def loop(count, body):
        lax.fori_loop(0, count, lambda i, carry: (body(i), carry)[1], 0)

    def part(i):
        return pl.ds(mult(i * depth, depth), depth)

    tok_copy = remote(tok, tok_o, tok_sem.at[0], tok_sem.at[1], fs, oc)
    own_start(0)
    own_start(1)
    quarters_start(0)
    tok_copy.start()
    own_rows = pl.ds(mult(fs * kb, kb), kb)
    u_all[own_rows, :] = u_in[...]
    v_all[own_rows, :] = v_in[...]
    o_all[:, own_rows] = o_in[...]
    own_quarter = pl.ds(mult(p * quarter, 16), quarter)
    for src, dst in wides:
        dst[:, own_rows] = src[own_quarter, :]

    for n in (0, 1):
        column(n, 1)
    own_start(2)
    own_start(3)
    for n in (0, 1):
        column(n, 2)
    for k in (0, 1):
        if k:
            for n in (0, 1):
                column(n, 3)
        for n in (0, 1):
            beside(n, k)
    own_block(0)
    for n in (2, 3):
        column(n, 1)
    for n in (0, 1):
        beside(n, 2)
    for n in (2, 3):
        column(n, 2)
    for n in (0, 1):
        beside(n, 3)
    for n in (2, 3):
        column(n, 3)
    for k in (0, 1):
        for n in (2, 3):
            beside(n, k)
    quarters_start(1)
    for h in range(HALVES):
        pass_on(0, 1, h)

    tok_copy.wait_recv()
    wide = 256
    mine_k = pl.ds(mult(c * feats, feats), feats)
    their_k = pl.ds(mult(oc * feats, feats), feats)

    def branch(weight, into):
        def step(n):
            cols = pl.ds(mult(n * wide, wide), wide)
            acc = add_rows(tok[...], weight[mine_k, cols]) + add_rows(tok_o[...], weight[their_k, cols])
            into[:, cols] = jax.nn.gelu(acc)

        loop(width_sg // wide, step)

    gathered(0)
    branch(u_all, gated)
    gathered(1)
    branch(v_all, valued)
    loop(rows // depth, lambda i: put_stats(0, part(i), valued[part(i), :]))
    stats_copy(0).start()
    for h in range(HALVES):
        pass_on(0, 2, h)
    for k in (2, 3):
        for n in (2, 3):
            beside(n, k)
    stats_copy(0).wait_recv()

    def norm_gate(i):
        vals = normalize(0, part(i), valued[part(i), :], sg_gain[...], 2 * width_sg)
        normed[part(i), :] = vals.astype(jnp.bfloat16)

    loop(rows // depth, norm_gate)
    groups, spread = spatial.shape[0], spatial.shape[1]
    row_at = lax.broadcasted_iota(jnp.int32, (spread, spread), 0)
    col_at = lax.broadcasted_iota(jnp.int32, (spread, spread), 1)
    group_dim = width_sg // groups

    def mix_block(n):
        place = pl.ds(mult(n * spread, spread), spread)
        for g in range(groups):
            cols = pl.ds(g * group_dim, group_dim)
            weight = jnp.where(col_at <= row_at, spatial[g], jnp.zeros_like(spatial[g]))
            shift_by = jnp.sum(jnp.where(col_at == row_at, bias[g : g + 1, :], 0.0), axis=1, keepdims=True)
            mixed = jnp.dot(weight, normed[place, cols], preferred_element_type=jnp.float32) + shift_by
            gated_out[place, cols] = (gated[place, cols] * mixed).astype(jnp.bfloat16)

    loop(rows // spread, mix_block)
    for n in (2, 3):
        gathered(n)

    terms_s, terms_o = p_s.at[pl.ds(0, rows), :], p_s.at[pl.ds(rows, rows), :]

    def project_out(which, into):
        def step(n):
            cols = pl.ds(mult(which * feats + n * wide, wide), wide)
            to = pl.ds(mult(n * wide, wide), wide)
            into[:, to] = add_rows(gated_out[...], o_all[:, cols]).astype(jnp.bfloat16)

        loop(feats // wide, step)

    project_out(oc, terms_s)
    terms_copy = remote(terms_s, terms_r, terms_sem.at[0], terms_sem.at[1], fs, oc)
    terms_copy.start()
    pass_on(0, 3, 0)
    project_out(c, terms_o)
    pass_on(0, 3, 1)
    own_block(1)
    terms_copy.wait_recv()

    def add_mix(i):
        mix = terms_o[part(i), :].astype(jnp.float32) + terms_r[part(i), :].astype(jnp.float32)
        vals = ALPHA * tok[part(i), :].astype(jnp.float32) + mix.astype(jnp.bfloat16).astype(jnp.float32)
        resid[part(i), :] = vals
        put_stats(1, part(i), vals)

    loop(rows // depth, add_mix)
    stats_copy(1).start()
    stats_copy(1).wait_recv()
    mine_cols = pl.ds(mult(c * feats, feats), feats)
    their_cols = pl.ds(mult(oc * feats, feats), feats)

    def norm_first(i):
        vals = normalize(1, part(i), resid[part(i), :], gain_one[...], 2 * feats)
        vals = vals.astype(jnp.bfloat16)
        first_all[pl.ds(mult(p * rows + i * depth, depth), depth), mine_cols] = vals
        resid[part(i), :] = ALPHA * vals.astype(jnp.float32)

    loop(rows // depth, norm_first)

    def place_of(j):
        return (y + j // 2) % 2 * 2 + (x + j % 2) % 2

    def tokens_of(j, cols):
        return first_all.at[pl.ds(mult(place_of(j) * rows, rows), rows), cols]

    def swap_copy(j):
        ref = tokens_of(j, mine_cols)
        return remote(ref, ref, swap_s.at[j], swap_r.at[j], fs, oc)

    own_tokens = tokens_of(0, mine_cols)
    first_copies = [
        remote(own_tokens, own_tokens, first_s.at[j], first_r.at[j], peers[j]) for j in range(1, PLANE)
    ]
    swap_copy(0).start()
    first_copies[0].start()
    first_copies[1].start()
    quarters_start(2)
    first_copies[2].start()

    for k in range(1, nz):
        for h in range(HALVES):
            need(0, k, h)

    tiles = [(t, min(wide, quarter - t)) for t in range(0, quarter, wide)]

    def across(left, weight, t, n):
        return lax.dot_general(
            left, weight[pl.ds(t, n), :], (((1,), (1,)), ((), ())), preferred_element_type=jnp.float32
        )

    def row_block(j):
        return pl.ds(mult(place_of(j) * rows, rows), rows)

    def gate_step(j):
        @pl.when(j > 0)
        def _():
            ref = tokens_of(j, mine_cols)
            remote(ref, ref, first_s.at[j], first_r.at[j], fs, oc).wait_recv()
            swap_copy(j).start()

        ref = tokens_of(j, their_cols)
        remote(ref, ref, swap_s.at[j], swap_r.at[j], fs, oc).wait_recv()
        left = row_block(j)
        for t, n in tiles:
            gate_acc[left, pl.ds(t, n)] = jax.nn.silu(across(first_all[left, :], gate_all, t, n))

        @pl.when(j < nz - 1)
        def _():
            for h in range(HALVES):
                pass_on(1, j + 1, h)

    loop(PLANE, gate_step)
    own_block(2)
    for k in range(1, nz):
        for h in range(HALVES):
            need(1, k, h)

    def up_step(j):
        left = row_block(j)
        for t, n in tiles:
            acc = gate_acc[left, pl.ds(t, n)] * across(first_all[left, :], up_all, t, n)
            hidden[left, pl.ds(t, n)] = acc.astype(jnp.bfloat16)

        @pl.when(j == PLANE - 2)
        def _():
            for h in range(HALVES):
                pass_on(2, 1, h)

    loop(PLANE, up_step)
    terms_copy.wait_send()

    steps = nz * HALVES
    per_core = steps // 2

    def piece(i):
        k, h = i // HALVES, i % HALVES
        b = seq(k)
        at = b * HALVES + h
        owner = at // per_core
        return k, h, b, at, owner, pl.ds(mult(at % per_core * half_cols, half_cols), half_cols)

    def pair_copy(i):
        at, cols = piece(i)[3], piece(i)[5]
        return remote(p_s.at[:, cols], p_r.at[:, cols], d2_s.at[at], d2_r.at[at], fs, oc)

    def rows_copy(i, j):
        at, cols = piece(i)[3], piece(i)[5]
        theirs = pl.ds(mult(place_of(j) * rows, rows), rows)
        return remote(
            p_r.at[theirs, cols], r_r.at[j - 1, :, cols], rs_s.at[at, j - 1], rs_r.at[at % per_core, j - 1], peers[j]
        )

    def finish(i):
        owner, cols = piece(i)[4], piece(i)[5]

        @pl.when(owner == c)
        def _():
            pair_copy(i).wait_recv()

            def add(r):
                place = pl.ds(mult(r * rows, rows), rows)
                both = p_own[i % 2, place, :].astype(jnp.float32) + p_r[place, cols].astype(jnp.float32)
                p_r[place, cols] = both.astype(jnp.bfloat16)

            loop(PLANE, add)
            for j in range(1, PLANE):
                rows_copy(i, j).start()

    def down_step(i):
        k, h, b, at, owner, cols = piece(i)

        @pl.when(k > 0)
        def _():
            @pl.when(k > 1)
            def _():
                pass_on(2, k, h)

            need(2, k, h)

        from_cols = pl.ds(mult(at * half_cols, half_cols), half_cols)

        def project(r):
            place = pl.ds(mult(r * rows, rows), rows)
            made = add_rows(hidden[place, :], down_all[:, from_cols]).astype(jnp.bfloat16)

            @pl.when(owner == c)
            def _():
                p_own[i % 2, place, :] = made

            @pl.when(owner != c)
            def _():
                p_s[place, cols] = made

        loop(PLANE, project)
        pl.when(owner != c)(lambda: pair_copy(i).start())
        pl.when(i > 0)(lambda: finish(i - 1))

    loop(steps, down_step)
    finish(steps - 1)

    def arrive(q):
        for j in range(1, PLANE):
            cols = pl.ds(mult(q * half_cols, half_cols), half_cols)
            ref = r_r.at[j - 1, :, cols]
            remote(ref, ref, rs_s.at[0, j - 1], rs_r.at[q, j - 1], peers[j]).wait_recv()

    loop(per_core, arrive)

    def add_ffn(i):
        total = p_r[pl.ds(mult(p * rows + i * depth, depth), depth), :].astype(jnp.float32)
        for j in range(1, PLANE):
            total = total + r_r[j - 1, part(i), :].astype(jnp.float32)
        vals = resid[part(i), :] + total.astype(jnp.bfloat16).astype(jnp.float32)
        resid[part(i), :] = vals
        put_stats(2, part(i), vals)

    loop(rows // depth, add_ffn)
    stats_copy(2).start()
    stats_copy(2).wait_recv()

    def norm_last(i):
        vals = normalize(2, part(i), resid[part(i), :], gain_two[...], 2 * feats)
        out[part(i), :] = vals.astype(out.dtype)

    loop(rows // depth, norm_last)

    tok_copy.wait_send()
    for which in range(3):
        stats_copy(which).wait_send()
    for copy in first_copies:
        copy.wait_send()
    loop(PLANE, lambda j: swap_copy(j).wait_send())
    for n in range(len(items)):
        for pred, copy in own_copies(n):
            sent_if(True if pred is None else pred, copy) if pred is not None else copy.wait_send()

        def sent(i):
            copies = column_copies(n, i + 1)
            sent_if(*copies[0])
            copies[1][1].wait_send()
            copies[2][1].wait_send()

        loop(nz - 1, sent)
        loop(nz, lambda k: beside_copy(n, k).wait_send())
    for w in range(len(wides)):
        for j in range(1, PLANE):
            quarter_copy(w, j).wait_send()
        for h in range(HALVES):
            for pred, copy in own_block_copies(w, h):
                sent_if(pred, copy)
            loop(nz - 1, lambda i: sent_if(*pass_copy(w, i + 1, h)))

    def pieces_sent(i):
        owner = piece(i)[4]
        pl.when(owner != c)(lambda: pair_copy(i).wait_send())

        @pl.when(owner == c)
        def _():
            for j in range(1, PLANE):
                rows_copy(i, j).wait_send()

    loop(steps, pieces_sent)


def in_one_kernel(*args):
    (tokens, u_weight, v_weight, sg_gain, spatial, bias, out_weight, gain_one, gate, up, down, gain_two) = args
    nz = lax.axis_size("fs") // PLANE
    rows, feats = tokens.shape
    width_sg = u_weight.shape[1]
    quarter = down.shape[0] // PLANE
    wide = 2 * feats
    plane_rows = PLANE * rows
    bf16, f32 = jnp.bfloat16, jnp.float32
    vmem, dma = pltpu.VMEM, pltpu.SemaphoreType.DMA
    steps = nz * HALVES
    half_cols = wide // steps
    scratch = [
        vmem((rows, feats), bf16),
        vmem((wide, width_sg), bf16),
        vmem((wide, width_sg), bf16),
        vmem((width_sg, wide), bf16),
        vmem((quarter, wide), bf16),
        vmem((quarter, wide), bf16),
        vmem((quarter, wide), bf16),
        vmem((rows, width_sg), f32),
        vmem((rows, width_sg), f32),
        vmem((rows, width_sg), bf16),
        vmem((rows, width_sg), bf16),
        vmem((3, rows, 128), f32),
        vmem((3, rows, 128), f32),
        vmem((rows, feats), bf16),
        vmem((rows, feats), f32),
        vmem((plane_rows, wide), bf16),
        vmem((plane_rows, quarter), bf16),
        vmem((plane_rows, quarter), f32),
        vmem((plane_rows, feats), bf16),
        vmem((plane_rows, feats), bf16),
        vmem((2, plane_rows, half_cols), bf16),
        vmem((PLANE - 1, rows, feats), bf16),
        dma((4, nz * PLANE)),
        dma((4, nz, 2)),
        dma((4, nz, 3)),
        dma((3, PLANE - 1)),
        dma((3, PLANE - 1)),
        dma((3, nz, HALVES, 2)),
        dma((3, nz, HALVES)),
        dma((2,)),
        dma((3, 2)),
        dma((2,)),
        dma((PLANE,)),
        dma((PLANE,)),
        dma((PLANE,)),
        dma((PLANE,)),
        dma((steps,)),
        dma((steps,)),
        dma((steps, PLANE - 1)),
        dma((steps // 2, PLANE - 1)),
    ]
    spec = pl.BlockSpec(memory_space=pltpu.VMEM)
    return pl.pallas_call(
        functools.partial(layer_kernel, (nz,)),
        name="layer",
        out_shape=jax.ShapeDtypeStruct((rows, feats), tokens.dtype),
        in_specs=[spec] * 12,
        out_specs=spec,
        scratch_shapes=scratch,
        compiler_params=pltpu.CompilerParams(
            collective_id=0, has_side_effects=True, vmem_limit_bytes=67_043_328
        ),
    )(
        tokens,
        u_weight,
        v_weight,
        sg_gain[None],
        spatial,
        bias,
        out_weight,
        gain_one[None],
        gate.T,
        up.T,
        down,
        gain_two[None],
    )


def fits(tokens, u_weight, gate_weight, spatial_weight):
    if lax.axis_size("tp") != 2 or lax.axis_size("fs") != 4 * PLANE:
        return False
    quarter = gate_weight.shape[1] % PLANE == 0 and gate_weight.shape[1] // PLANE % 16 == 0
    lanes = u_weight.shape[0] % 128 == 0 and u_weight.shape[1] % 256 == 0
    return quarter and lanes and tokens.shape[0] % (PLANE * spatial_weight.shape[1]) == 0


def choose(*args):
    if fits(args[0], args[1], args[8], args[4]):
        return in_one_kernel(*args)
    return on_device(*args)


def solution(mesh):
    return jax.shard_map(
        choose,
        mesh=mesh,
        in_specs=(
            P("fs", "tp"),
            P("fs", "tp"),
            P("fs", "tp"),
            P("tp"),
            P("tp", None, None),
            P("tp", None),
            P("tp", "fs"),
            P("tp"),
            P("fs", "tp"),
            P("fs", "tp"),
            P("tp", "fs"),
            P("tp"),
        ),
        out_specs=P("fs", "tp"),
        check_vma=False,
    )
```

```python
import functools

import jax
import jax.numpy as jnp
from jax import lax
from jax.experimental import pallas as pl
from jax.experimental.pallas import tpu as pltpu
from jax.sharding import PartitionSpec as P

EPS = 1e-05
ALPHA = 2.0**0.25


def add_rows(left, piece):
    return jnp.dot(left, piece, preferred_element_type=jnp.float32)


def scaled_rows(vals, sums, gain, count):
    mean = sums[0][:, None] / count
    square = sums[1][:, None] / count
    return (vals - mean) * lax.rsqrt(square - mean * mean + EPS) * gain[None, :]


def chip_sizes(count):
    across = 2 if count % 2 == 0 else 1
    down = 2 if (count // across) % 2 == 0 else 1
    return count // (across * down), down, across


def shift(value, sizes, axis, step=1):
    count = sizes[0] * sizes[1] * sizes[2]
    stride = sizes[1] * sizes[2] if axis == 0 else (sizes[2] if axis == 1 else 1)
    pairs = []
    for source in range(count):
        place = (source // stride) % sizes[axis]
        pairs.append((source, source + ((place + step) % sizes[axis] - place) * stride))
    return lax.ppermute(value, "fs", pairs)


def around(value, sizes, axis):
    if sizes[axis] == 4:
        near = shift(value, sizes, axis, 1)
        last = shift(value, sizes, axis, -1)
        return [value, near, shift(near, sizes, axis, 1), last]
    pieces = [value]
    for _ in range(sizes[axis] - 1):
        pieces.append(shift(pieces[-1], sizes, axis))
    return pieces


def ring(value, sizes, axis, place):
    return in_order(around(value, sizes, axis), place)


def other_core(value):
    return lax.ppermute(value, "tp", [(0, 1), (1, 0)])


def all_features(value):
    if lax.axis_size("tp") != 2:
        return lax.all_gather(value, "tp", axis=1, tiled=True)
    return jnp.concatenate(in_two(value, other_core(value), lax.axis_index("tp")), axis=1)


def in_two(mine, other, place):
    return [jnp.where(place == 0, mine, other), jnp.where(place == 0, other, mine)]


def sum_shares(terms):
    if lax.axis_size("tp") != 2:
        return lax.psum_scatter(terms, "tp", scatter_dimension=1, tiled=True)
    core = lax.axis_index("tp")
    half = terms.shape[1] // 2
    mine = lax.dynamic_slice_in_dim(terms, core * half, half, 1)
    sent = lax.dynamic_slice_in_dim(terms, (1 - core) * half, half, 1)
    return (mine.astype(jnp.float32) + other_core(sent).astype(jnp.float32)).astype(jnp.bfloat16)


def in_order(pieces, place):
    count = len(pieces)
    if count == 1:
        return pieces[0][None]
    held = jnp.zeros((count,) + pieces[0].shape, pieces[0].dtype)
    for step, piece in enumerate(pieces):
        start = lax.rem(place - step + count, count)
        held = lax.dynamic_update_slice_in_dim(held, piece[None], start, 0)
    return held


def gather_all(piece, sizes, places, order):
    held = piece
    for axis in order:
        held = ring(held, sizes, axis, places[axis])
    back = [order[::-1].index(axis) for axis in range(3)]
    rest = [3 + i for i in range(piece.ndim)]
    return jnp.transpose(held, back + rest)


def after(value, *others):
    return lax.optimization_barrier((value,) + others)[0]


def share_pieces(weight, dim, sizes, places, level, marks):
    across = sizes[2]
    width = weight.shape[dim] // across
    if across == 2:
        mine = lax.dynamic_slice_in_dim(weight, places[2] * width, width, dim)
        other = lax.dynamic_slice_in_dim(weight, (1 - places[2]) * width, width, dim)
        block = jnp.stack(in_two(mine, shift(other, sizes, 2), places[2]))
    else:
        block = weight[None]
    if sizes[0] != 4 or sizes[1] != 2:
        first = around(block, sizes, 0)
        return [[piece] if sizes[1] == 1 else [piece, shift(piece, sizes, 1)] for piece in first]
    if marks[0] is not None:
        block = after(block, marks[0])
    near, last = shift(block, sizes, 0, 1), shift(block, sizes, 0, -1)
    beside = shift(block if marks[0] is None else after(block, marks[1]), sizes, 1)
    near, last = after(near, marks[1]), after(last, marks[1])
    far = shift(near, sizes, 0)
    near_beside, last_beside = shift(near, sizes, 1), shift(last, sizes, 1)
    if level:
        far_beside = shift(after(near_beside, marks[2]), sizes, 0)
    else:
        far = after(far, marks[2])
        far_beside = shift(far, sizes, 1)
    return [[block, beside], [near, near_beside], [far, far_beside], [last, last_beside]]


def place_pieces(pieces, places):
    shape = pieces[0][0].shape
    count, down = len(pieces), len(pieces[0])
    held = jnp.zeros((count, down) + shape, pieces[0][0].dtype)
    for step, pair in enumerate(pieces):
        start = lax.rem(places[0] - step + count, count)
        for turn, piece in enumerate(pair):
            spot = places[1] if turn == 0 else 1 - places[1]
            held = lax.dynamic_update_slice(held, piece[None, None], [start, spot] + [0] * len(shape))
    return held


def on_device(
    tokens,
    u_weight,
    v_weight,
    sg_gain,
    spatial_weight,
    spatial_bias,
    out_weight,
    gain_one,
    gate_weight,
    up_weight,
    down_weight,
    gain_two,
):
    parts = lax.axis_size("tp")
    sizes = chip_sizes(lax.axis_size("fs"))
    index = lax.axis_index("fs")
    places = (index // (sizes[1] * sizes[2]), (index // sizes[2]) % sizes[1], index % sizes[2])
    whole = all_features(tokens)
    rows = whole.shape[0]
    width_sg = u_weight.shape[1]

    def add_one(piece):
        return add_rows(whole, piece)

    pre_u = add_one(gather_all(u_weight, sizes, places, [0, 1, 2]).reshape(-1, width_sg))
    pre_v = add_one(gather_all(v_weight, sizes, places, [0, 2, 1]).reshape(-1, width_sg))
    gated = jax.nn.gelu(pre_u)
    valued = jax.nn.gelu(pre_v)
    stats = lax.psum((jnp.sum(valued, axis=1), jnp.sum(valued * valued, axis=1)), "tp")
    normed = scaled_rows(valued, stats, sg_gain, width_sg * parts).astype(jnp.bfloat16)
    groups_here = spatial_weight.shape[0]
    block = spatial_weight.shape[1]
    group_width = width_sg // groups_here
    shaped = normed.reshape(rows // block, block, groups_here, group_width)
    lower = jnp.tril(jnp.ones((block, block), jnp.bool_))
    masked = jnp.where(lower[None], spatial_weight, jnp.zeros_like(spatial_weight))
    mixed = jnp.einsum("gij,njgd->nigd", masked, shaped, preferred_element_type=jnp.float32)
    mixed = mixed + spatial_bias.T[None, :, :, None]
    gated_out = (gated * mixed.reshape(rows, width_sg)).astype(jnp.bfloat16)
    out_all = gather_all(out_weight, sizes, places, [0, 1, 2])
    out_all = out_all.reshape((-1,) + out_weight.shape)
    terms = jnp.einsum("tk,nkc->tnc", gated_out, out_all, preferred_element_type=jnp.float32)
    mix = sum_shares(terms.reshape(rows, -1).astype(jnp.bfloat16))
    resid = ALPHA * tokens.astype(jnp.float32) + mix.astype(jnp.float32)
    first_sums = lax.psum((jnp.sum(resid, axis=1), jnp.sum(resid * resid, axis=1)), "tp")
    first = scaled_rows(resid, first_sums, gain_one, resid.shape[1] * parts).astype(jnp.bfloat16)
    gate_pieces = share_pieces(gate_weight, 1, sizes, places, False, (None, normed, mix))
    up_pieces = share_pieces(up_weight, 1, sizes, places, True, (None, normed, mix))
    down_pieces = share_pieces(down_weight, 0, sizes, places, False, (normed, first, first))
    gate_all = place_pieces(gate_pieces, places)
    gate_all = gate_all.reshape(-1, gate_all.shape[-1])
    up_all = place_pieces(up_pieces, places)
    up_all = up_all.reshape(-1, up_all.shape[-1])
    def feed(part):
        whole_part = all_features(part)
        gate = add_rows(whole_part, gate_all)
        upper = add_rows(whole_part, up_all)
        return (jax.nn.silu(gate) * upper).astype(jnp.bfloat16)

    two = sizes[2] == 2
    if two:
        there = feed(shift(first, sizes, 2))
        here = feed(first)
        down_pieces = [[pair[0]] + [after(piece, there, here) for piece in pair[1:]] for pair in down_pieces]
    else:
        here = feed(first)
    down_all = place_pieces(down_pieces, places)
    down_all = down_all.reshape((-1,) + down_all.shape[-2:])

    def project(hidden):
        made = jnp.einsum("tf,nfc->tnc", hidden, down_all, preferred_element_type=jnp.float32)
        return sum_shares(made.reshape(rows, -1).astype(jnp.bfloat16))

    if two:
        there = project(there)
        sent = shift(there, sizes, 2)
        ffn = project(after(here, there)).astype(jnp.float32) + sent.astype(jnp.float32)
    else:
        ffn = project(here).astype(jnp.float32)
    second = ALPHA * first.astype(jnp.float32) + ffn.astype(jnp.float32)
    last_sums = lax.psum((jnp.sum(second, axis=1), jnp.sum(second * second, axis=1)), "tp")
    return scaled_rows(second, last_sums, gain_two, second.shape[1] * parts).astype(jnp.bfloat16)


MESH = pl.DeviceIdType.MESH
PLANE = 4
HALVES = 2


def layer_kernel(
    sizes,
    tok_in,
    u_in,
    v_in,
    sg_gain_in,
    spatial_in,
    bias_in,
    o_in,
    gain_one_in,
    gate_in,
    up_in,
    down_in,
    gain_two_in,
    out,
    tok,
    sg_gain,
    spatial,
    bias,
    gain_one,
    gain_two,
    gate_own,
    up_own,
    gate_turned,
    up_turned,
    tok_o,
    u_all,
    v_all,
    o_all,
    gate_all,
    up_all,
    down_all,
    gated,
    valued,
    normed,
    gated_out,
    st_s,
    st_r,
    terms_r,
    resid,
    first_all,
    hidden,
    gate_acc,
    p_s,
    p_r,
    p_own,
    r_r,
    in_sem,
    sg_r,
    sg_z,
    sg_p,
    a2_s,
    a2_r,
    z_s,
    z_r,
    tok_sem,
    st_sem,
    terms_sem,
    first_s,
    first_r,
    swap_s,
    swap_r,
    d2_s,
    d2_r,
    rs_s,
    rs_r,
):
    nz = sizes[0]
    fs, c = lax.axis_index("fs"), lax.axis_index("tp")
    oc = 1 - c
    z, p = fs // PLANE, fs % PLANE
    y, x = p // 2, p % 2
    peers = [z * PLANE + (y + j // 2) % 2 * 2 + (x + j % 2) % 2 for j in range(PLANE)]
    inplane = [(y + j // 2) % 2 * 2 + (x + j % 2) % 2 for j in range(PLANE)]
    has_up, has_down = z < nz - 1, z > 0
    up_dev = jnp.where(has_up, fs + PLANE, fs - PLANE)
    down_dev = jnp.where(has_down, fs - PLANE, fs + PLANE)
    rows, feats = tok.shape
    kb, width_sg = u_in.shape
    depth = rows // PLANE
    quarter = hidden.shape[1]
    plane_cols = PLANE * kb
    half_cols = plane_cols // HALVES

    def mult(value, by):
        return pl.multiple_of(value, by)

    def seq(k):
        swapped = jnp.where(k < 2, 1 - k, k)
        return jnp.where(z == 0, k, jnp.where(z == 1, swapped, jnp.where(z == 2, nz - 1 - swapped, nz - 1 - k)))

    def remote(src, dst, send, recv, dev, core=None):
        where_to = (dev, c if core is None else core)
        return pltpu.make_async_remote_copy(
            src_ref=src, dst_ref=dst, send_sem=send, recv_sem=recv, device_id=where_to, device_id_type=MESH
        )

    def start_if(pred, copy):
        pl.when(pred)(lambda: copy.start())

    def sent_if(pred, copy):
        pl.when(pred)(lambda: copy.wait_send())

    own_rows = pl.ds(mult(fs * kb, kb), kb)
    own_quarter = pl.ds(mult(p * quarter, 16), quarter)
    loads = [
        (gate_in, gate_own),
        (up_in, up_own),
        (u_in, u_all.at[own_rows, :]),
        (v_in, v_all.at[own_rows, :]),
        (o_in, o_all.at[:, own_rows]),
        (down_in.at[own_quarter, :], down_all.at[:, own_rows]),
        (tok_in, tok),
        (sg_gain_in, sg_gain),
        (spatial_in, spatial),
        (bias_in, bias),
        (gain_one_in, gain_one),
        (gain_two_in, gain_two),
    ]
    loads = [pltpu.make_async_copy(src, dst, in_sem.at[i]) for i, (src, dst) in enumerate(loads)]
    for load in loads:
        load.start()
    barrier = pltpu.get_barrier_semaphore()
    for dev, core in [(fs, oc)] + [(peers[j], c) for j in range(1, PLANE)]:
        pl.semaphore_signal(barrier, inc=1, device_id=(dev, core), device_id_type=MESH)
    for pred, dev in [(has_up, up_dev), (has_down, down_dev)]:
        @pl.when(pred)
        def _():
            pl.semaphore_signal(barrier, inc=1, device_id=(dev, c), device_id_type=MESH)
    pl.semaphore_wait(barrier, PLANE + jnp.where(has_up, 1, 0) + jnp.where(has_down, 1, 0))

    def rows_of(ref):
        return lambda i: ref.at[pl.ds(mult(i * kb, kb), kb), :]

    def cols_of(ref, part):
        height = width_sg // 2
        return lambda i: ref.at[pl.ds(part * height, height), pl.ds(mult(i * kb, kb), kb)]

    half_o = width_sg // 2
    items = [
        (u_in, rows_of(u_all), 1, 2),
        (v_in, rows_of(v_all), 2, 1),
        (o_in.at[pl.ds(0, half_o), :], cols_of(o_all, 0), 1, 2),
        (o_in.at[pl.ds(half_o, half_o), :], cols_of(o_all, 1), 2, 1),
    ]

    def own_copies(n):
        src, at, one, two = items[n]
        return [
            (has_up, remote(src, at(fs), sg_z.at[n, 0, 0], sg_r.at[n, fs], up_dev)),
            (has_down, remote(src, at(fs), sg_z.at[n, 0, 1], sg_r.at[n, fs], down_dev)),
            (None, remote(src, at(fs), sg_p.at[n, 0, 0], sg_r.at[n, fs], peers[one])),
            (None, remote(src, at(fs), sg_p.at[n, 0, 1], sg_r.at[n, fs], peers[two])),
        ]

    def own_start(n):
        for pred, copy in own_copies(n):
            if pred is None:
                copy.start()
            else:
                start_if(pred, copy)

    def forward_to(b):
        going_up = b < z
        return (going_up & has_up) | ((b > z) & has_down), jnp.where(going_up, up_dev, down_dev)

    def column_copies(n, k):
        _, at, one, two = items[n]
        b = seq(k)
        idx = b * PLANE + p
        pred, dev = forward_to(b)
        ref, recv = at(idx), sg_r.at[n, idx]
        return [
            (pred, remote(ref, ref, sg_z.at[n, k, 0], recv, dev)),
            (None, remote(ref, ref, sg_p.at[n, k, 0], recv, peers[one])),
            (None, remote(ref, ref, sg_p.at[n, k, 1], recv, peers[two])),
        ]

    def column(n, k):
        copies = column_copies(n, k)
        copies[0][1].wait_recv()
        start_if(*copies[0])
        copies[1][1].start()
        copies[2][1].start()

    def beside_copy(n, k):
        _, at, one, two = items[n]
        idx = seq(k) * PLANE + inplane[one]
        ref, recv = at(idx), sg_r.at[n, idx]
        return remote(ref, ref, sg_p.at[n, k, 2], recv, peers[two])

    def beside(n, k):
        copy = beside_copy(n, k)
        copy.wait_recv()
        copy.start()

    def gathered(n):
        _, at, one, two = items[n]

        def arrive(b, carry):
            for j in (two, 3):
                idx = b * PLANE + inplane[j]
                ref = at(idx)
                remote(ref, ref, sg_p.at[n, 0, 0], sg_r.at[n, idx], peers[two]).wait_recv()
            return carry

        lax.fori_loop(0, nz, arrive, 0)

    wides = [(gate_turned, gate_all), (up_turned, up_all), (down_in, down_all)]

    def quarter_copy(w, j):
        src, dst = wides[w]
        theirs = pl.ds(mult(inplane[j] * quarter, 16), quarter)
        mine = pl.ds(mult(fs * kb, kb), kb)
        return remote(src.at[theirs, :], dst.at[:, mine], a2_s.at[w, j - 1], a2_r.at[w, j - 1], peers[j])

    def quarters_start(w):
        for j in range(1, PLANE):
            quarter_copy(w, j).start()

    def block(w, b, h):
        return wides[w][1].at[:, pl.ds(mult(b * plane_cols + h * half_cols, half_cols), half_cols)]

    def own_block_copies(w, h):
        ref, recv = block(w, z, h), z_r.at[w, z, h]
        return [
            (has_up, remote(ref, ref, z_s.at[w, 0, h, 0], recv, up_dev)),
            (has_down, remote(ref, ref, z_s.at[w, 0, h, 1], recv, down_dev)),
        ]

    def own_block(w):
        for j in range(1, PLANE):
            ref = wides[w][1].at[:, pl.ds(mult(peers[j] * kb, kb), kb)]
            remote(ref, ref, a2_s.at[w, j - 1], a2_r.at[w, j - 1], peers[j]).wait_recv()
        for h in range(HALVES):
            for pred, copy in own_block_copies(w, h):
                start_if(pred, copy)

    def pass_copy(w, k, h):
        b = seq(k)
        pred, dev = forward_to(b)
        ref = block(w, b, h)
        return pred, remote(ref, ref, z_s.at[w, k, h, 0], z_r.at[w, b, h], dev)

    def pass_on(w, k, h):
        pred, copy = pass_copy(w, k, h)

        @pl.when(pred)
        def _():
            copy.wait_recv()
            copy.start()

    def need(w, k, h):
        pred, copy = pass_copy(w, k, h)
        pl.when(jnp.logical_not(pred))(lambda: copy.wait_recv())

    lane = lax.broadcasted_iota(jnp.int32, (depth, 128), 1)

    def put_stats(which, place, vals):
        one = jnp.sum(vals, axis=1, keepdims=True)
        two = jnp.sum(vals * vals, axis=1, keepdims=True)
        st_s[which, place, :] = jnp.where(lane == 0, one, two)

    def stats_copy(which):
        return remote(st_s.at[which], st_r.at[which], st_sem.at[which, 0], st_sem.at[which, 1], fs, oc)

    def normalize(which, place, vals, gain, count):
        both = st_s[which, place, :] + st_r[which, place, :]
        mean = both[:, 0:1] / count
        square = both[:, 1:2] / count
        return (vals - mean) * lax.rsqrt(square - mean * mean + EPS) * gain

    def loop(count, body):
        lax.fori_loop(0, count, lambda i, carry: (body(i), carry)[1], 0)

    def part(i):
        return pl.ds(mult(i * depth, depth), depth)

    tok_copy = remote(tok_in, tok_o, tok_sem.at[0], tok_sem.at[1], fs, oc)
    own_start(0)
    own_start(1)

    def turn(src, dst):
        def step(i):
            place = pl.ds(mult(i * kb, kb), kb)
            dst[place, :] = src[:, place].T

        loop(src.shape[1] // kb, step)

    loads[0].wait()
    turn(gate_own, gate_turned)
    quarters_start(0)
    own_start(2)
    own_start(3)
    tok_copy.start()
    for load in loads[1:]:
        load.wait()
    turn(up_own, up_turned)
    gate_all[:, own_rows] = gate_turned[own_quarter, :]
    up_all[:, own_rows] = up_turned[own_quarter, :]

    for n in (0, 1):
        column(n, 1)
    for n in (0, 1):
        column(n, 2)
    for n in (2, 3):
        column(n, 1)
    for n in (0, 1):
        column(n, 3)
    for n in (2, 3):
        column(n, 2)
    own_block(0)
    for k in (0, 1):
        for n in (0, 1):
            beside(n, k)
    for n in (2, 3):
        column(n, 3)
    pass_on(0, 1, 0)
    pass_on(0, 2, 0)
    for n in (0, 1):
        beside(n, 2)
    pass_on(0, 1, 1)
    pass_on(0, 2, 1)
    for n in (0, 1):
        beside(n, 3)
    quarters_start(1)
    for n in (2, 3):
        beside(n, 0)
    for n in (2, 3):
        beside(n, 1)
    pass_on(0, 3, 0)
    for n in (2, 3):
        beside(n, 2)

    tok_copy.wait_recv()
    wide = 256
    mine_k = pl.ds(mult(c * feats, feats), feats)
    their_k = pl.ds(mult(oc * feats, feats), feats)

    def branch(weight, into):
        def step(n):
            cols = pl.ds(mult(n * wide, wide), wide)
            acc = add_rows(tok[...], weight[mine_k, cols]) + add_rows(tok_o[...], weight[their_k, cols])
            into[:, cols] = jax.nn.gelu(acc)

        loop(width_sg // wide, step)

    gathered(0)
    branch(u_all, gated)
    gathered(1)
    branch(v_all, valued)
    for n in (2, 3):
        beside(n, 3)
    pass_on(0, 3, 1)
    loop(rows // depth, lambda i: put_stats(0, part(i), valued[part(i), :]))
    stats_copy(0).start()
    stats_copy(0).wait_recv()

    def norm_gate(i):
        vals = normalize(0, part(i), valued[part(i), :], sg_gain[...], 2 * width_sg)
        normed[part(i), :] = vals.astype(jnp.bfloat16)

    loop(rows // depth, norm_gate)
    groups, spread = spatial.shape[0], spatial.shape[1]
    row_at = lax.broadcasted_iota(jnp.int32, (spread, spread), 0)
    col_at = lax.broadcasted_iota(jnp.int32, (spread, spread), 1)
    group_dim = width_sg // groups

    def mix_block(n):
        place = pl.ds(mult(n * spread, spread), spread)
        for g in range(groups):
            cols = pl.ds(g * group_dim, group_dim)
            weight = jnp.where(col_at <= row_at, spatial[g], jnp.zeros_like(spatial[g]))
            shift_by = jnp.sum(jnp.where(col_at == row_at, bias[g : g + 1, :], 0.0), axis=1, keepdims=True)
            mixed = jnp.dot(weight, normed[place, cols], preferred_element_type=jnp.float32) + shift_by
            gated_out[place, cols] = (gated[place, cols] * mixed).astype(jnp.bfloat16)

    loop(rows // spread, mix_block)
    for n in (2, 3):
        gathered(n)

    terms_s, terms_o = p_s.at[pl.ds(0, rows), :], p_s.at[pl.ds(rows, rows), :]

    def project_out(which, into):
        def step(n):
            cols = pl.ds(mult(which * feats + n * wide, wide), wide)
            to = pl.ds(mult(n * wide, wide), wide)
            into[:, to] = add_rows(gated_out[...], o_all[:, cols]).astype(jnp.bfloat16)

        loop(feats // wide, step)

    project_out(oc, terms_s)
    terms_copy = remote(terms_s, terms_r, terms_sem.at[0], terms_sem.at[1], fs, oc)
    terms_copy.start()
    project_out(c, terms_o)
    own_block(1)
    terms_copy.wait_recv()

    def add_mix(i):
        mix = terms_o[part(i), :].astype(jnp.float32) + terms_r[part(i), :].astype(jnp.float32)
        vals = ALPHA * tok[part(i), :].astype(jnp.float32) + mix.astype(jnp.bfloat16).astype(jnp.float32)
        resid[part(i), :] = vals
        put_stats(1, part(i), vals)

    loop(rows // depth, add_mix)
    stats_copy(1).start()
    stats_copy(1).wait_recv()
    mine_cols = pl.ds(mult(c * feats, feats), feats)
    their_cols = pl.ds(mult(oc * feats, feats), feats)

    def norm_first(i):
        vals = normalize(1, part(i), resid[part(i), :], gain_one[...], 2 * feats)
        vals = vals.astype(jnp.bfloat16)
        first_all[pl.ds(mult(p * rows + i * depth, depth), depth), mine_cols] = vals
        resid[part(i), :] = ALPHA * vals.astype(jnp.float32)

    loop(rows // depth, norm_first)

    def place_of(j):
        return (y + j // 2) % 2 * 2 + (x + j % 2) % 2

    def tokens_of(j, cols):
        return first_all.at[pl.ds(mult(place_of(j) * rows, rows), rows), cols]

    def swap_copy(j):
        ref = tokens_of(j, mine_cols)
        return remote(ref, ref, swap_s.at[j], swap_r.at[j], fs, oc)

    own_tokens = tokens_of(0, mine_cols)
    first_copies = [
        remote(own_tokens, own_tokens, first_s.at[j], first_r.at[j], peers[j]) for j in (1, 2)
    ]

    def corner_copy(j):
        start = mult(place_of(j) * rows + (j - 1) * (rows // 2), rows // 2)
        ref = first_all.at[pl.ds(start, rows // 2), mine_cols]
        return remote(ref, ref, first_s.at[j + 2], first_r.at[j + 2], z * PLANE + place_of(PLANE - 1 - j))

    swap_copy(0).start()
    for copy in first_copies:
        copy.start()
    quarters_start(2)

    for k in range(1, nz):
        for h in range(HALVES):
            need(0, k, h)

    tiles = [(t, min(wide, quarter - t)) for t in range(0, quarter, wide)]

    def across(left, weight, t, n):
        return lax.dot_general(
            left, weight[pl.ds(t, n), :], (((1,), (1,)), ((), ())), preferred_element_type=jnp.float32
        )

    def row_block(j):
        return pl.ds(mult(place_of(j) * rows, rows), rows)

    def gate_step(j):
        @pl.when((j == 1) | (j == 2))
        def _():
            ref = tokens_of(j, mine_cols)
            remote(ref, ref, first_s.at[j], first_r.at[j], fs, oc).wait_recv()
            corner_copy(j).start()

        @pl.when(j == PLANE - 1)
        def _():
            for half in (0, 1):
                start = mult(place_of(j) * rows + half * (rows // 2), rows // 2)
                ref = first_all.at[pl.ds(start, rows // 2), mine_cols]
                remote(ref, ref, first_s.at[half + 3], first_r.at[half + 3], fs, oc).wait_recv()

        @pl.when(j > 0)
        def _():
            swap_copy(j).start()

        ref = tokens_of(j, their_cols)
        remote(ref, ref, swap_s.at[j], swap_r.at[j], fs, oc).wait_recv()
        left = row_block(j)
        for t, n in tiles:
            gate_acc[left, pl.ds(t, n)] = jax.nn.silu(across(first_all[left, :], gate_all, t, n))

        @pl.when(j == 0)
        def _():
            for h in range(HALVES):
                pass_on(1, 1, h)
                pass_on(1, 2, h)

        @pl.when((j == 1) | (j == 2))
        def _():
            pass_on(1, 3, j - 1)

        pl.when(j == 2)(lambda: own_block(2))

    loop(PLANE, gate_step)
    for k in range(1, nz):
        for h in range(HALVES):
            need(1, k, h)

    def up_step(j):
        left = row_block(j)
        for t, n in tiles:
            acc = gate_acc[left, pl.ds(t, n)] * across(first_all[left, :], up_all, t, n)
            hidden[left, pl.ds(t, n)] = acc.astype(jnp.bfloat16)

    loop(PLANE, up_step)
    terms_copy.wait_send()

    steps = nz * HALVES
    per_core = steps // 2

    def piece(i):
        inner = (i >= HALVES) & (i < 3 * HALVES) & has_up & has_down
        k = jnp.where(inner, 1 + i % 2, i // HALVES)
        h = jnp.where(inner, (i - 2) // 2, i % HALVES)
        b = seq(k)
        at = b * HALVES + h
        owner = at // per_core
        return k, h, b, at, owner, pl.ds(mult(at % per_core * half_cols, half_cols), half_cols)

    def pair_copy(i):
        at, cols = piece(i)[3], piece(i)[5]
        return remote(p_s.at[:, cols], p_r.at[:, cols], d2_s.at[at], d2_r.at[at], fs, oc)

    def rows_copy(i, j):
        at, cols = piece(i)[3], piece(i)[5]
        theirs = pl.ds(mult(place_of(j) * rows, rows), rows)
        return remote(
            p_r.at[theirs, cols], r_r.at[j - 1, :, cols], rs_s.at[at, j - 1], rs_r.at[at % per_core, j - 1], peers[j]
        )

    def finish(i):
        owner, cols = piece(i)[4], piece(i)[5]

        @pl.when(owner == c)
        def _():
            pair_copy(i).wait_recv()

            def add(r):
                place = pl.ds(mult(r * rows, rows), rows)
                both = p_own[i % 2, place, :].astype(jnp.float32) + p_r[place, cols].astype(jnp.float32)
                p_r[place, cols] = both.astype(jnp.bfloat16)

            loop(PLANE, add)
            for j in range(1, PLANE):
                rows_copy(i, j).start()

    def down_step(i):
        k, h, b, at, owner, cols = piece(i)

        @pl.when(k > 0)
        def _():
            pass_on(2, k, h)
            need(2, k, h)

        from_cols = pl.ds(mult(at * half_cols, half_cols), half_cols)

        def project(r):
            place = pl.ds(mult(r * rows, rows), rows)
            made = add_rows(hidden[place, :], down_all[:, from_cols]).astype(jnp.bfloat16)

            @pl.when(owner == c)
            def _():
                p_own[i % 2, place, :] = made

            @pl.when(owner != c)
            def _():
                p_s[place, cols] = made

        loop(PLANE, project)
        pl.when(owner != c)(lambda: pair_copy(i).start())
        pl.when(i > 0)(lambda: finish(i - 1))

    loop(steps, down_step)
    finish(steps - 1)

    def arrive(q):
        for j in range(1, PLANE):
            cols = pl.ds(mult(q * half_cols, half_cols), half_cols)
            ref = r_r.at[j - 1, :, cols]
            remote(ref, ref, rs_s.at[0, j - 1], rs_r.at[q, j - 1], peers[j]).wait_recv()

    loop(per_core, arrive)

    def add_ffn(i):
        total = p_r[pl.ds(mult(p * rows + i * depth, depth), depth), :].astype(jnp.float32)
        for j in range(1, PLANE):
            total = total + r_r[j - 1, part(i), :].astype(jnp.float32)
        vals = resid[part(i), :] + total.astype(jnp.bfloat16).astype(jnp.float32)
        resid[part(i), :] = vals
        put_stats(2, part(i), vals)

    loop(rows // depth, add_ffn)
    stats_copy(2).start()
    stats_copy(2).wait_recv()

    def norm_last(i):
        vals = normalize(2, part(i), resid[part(i), :], gain_two[...], 2 * feats)
        out[part(i), :] = vals.astype(out.dtype)

    loop(rows // depth, norm_last)

    tok_copy.wait_send()
    for which in range(3):
        stats_copy(which).wait_send()
    for copy in first_copies:
        copy.wait_send()
    for j in (1, 2):
        corner_copy(j).wait_send()
    loop(PLANE, lambda j: swap_copy(j).wait_send())
    for n in range(len(items)):
        for pred, copy in own_copies(n):
            sent_if(True if pred is None else pred, copy) if pred is not None else copy.wait_send()

        def sent(i):
            copies = column_copies(n, i + 1)
            sent_if(*copies[0])
            copies[1][1].wait_send()
            copies[2][1].wait_send()

        loop(nz - 1, sent)
        loop(nz, lambda k: beside_copy(n, k).wait_send())
    for w in range(len(wides)):
        for j in range(1, PLANE):
            quarter_copy(w, j).wait_send()
        for h in range(HALVES):
            for pred, copy in own_block_copies(w, h):
                sent_if(pred, copy)
            loop(nz - 1, lambda i: sent_if(*pass_copy(w, i + 1, h)))

    def pieces_sent(i):
        owner = piece(i)[4]
        pl.when(owner != c)(lambda: pair_copy(i).wait_send())

        @pl.when(owner == c)
        def _():
            for j in range(1, PLANE):
                rows_copy(i, j).wait_send()

    loop(steps, pieces_sent)


def in_one_kernel(*args):
    (tokens, u_weight, v_weight, sg_gain, spatial, bias, out_weight, gain_one, gate, up, down, gain_two) = args
    nz = lax.axis_size("fs") // PLANE
    rows, feats = tokens.shape
    width_sg = u_weight.shape[1]
    quarter = down.shape[0] // PLANE
    wide = 2 * feats
    plane_rows = PLANE * rows
    bf16, f32 = jnp.bfloat16, jnp.float32
    vmem, dma = pltpu.VMEM, pltpu.SemaphoreType.DMA
    steps = nz * HALVES
    half_cols = wide // steps
    scratch = [
        vmem((rows, feats), bf16),
        vmem((1, width_sg), f32),
        vmem(spatial.shape, bf16),
        vmem(bias.shape, f32),
        vmem((1, feats), f32),
        vmem((1, feats), f32),
        vmem(gate.shape, bf16),
        vmem(gate.shape, bf16),
        vmem(gate.shape[::-1], bf16),
        vmem(gate.shape[::-1], bf16),
        vmem((rows, feats), bf16),
        vmem((wide, width_sg), bf16),
        vmem((wide, width_sg), bf16),
        vmem((width_sg, wide), bf16),
        vmem((quarter, wide), bf16),
        vmem((quarter, wide), bf16),
        vmem((quarter, wide), bf16),
        vmem((rows, width_sg), f32),
        vmem((rows, width_sg), f32),
        vmem((rows, width_sg), bf16),
        vmem((rows, width_sg), bf16),
        vmem((3, rows, 128), f32),
        vmem((3, rows, 128), f32),
        vmem((rows, feats), bf16),
        vmem((rows, feats), f32),
        vmem((plane_rows, wide), bf16),
        vmem((plane_rows, quarter), bf16),
        vmem((plane_rows, quarter), f32),
        vmem((plane_rows, feats), bf16),
        vmem((plane_rows, feats), bf16),
        vmem((2, plane_rows, half_cols), bf16),
        vmem((PLANE - 1, rows, feats), bf16),
        dma((12,)),
        dma((4, nz * PLANE)),
        dma((4, nz, 2)),
        dma((4, nz, 3)),
        dma((3, PLANE - 1)),
        dma((3, PLANE - 1)),
        dma((3, nz, HALVES, 2)),
        dma((3, nz, HALVES)),
        dma((2,)),
        dma((3, 2)),
        dma((2,)),
        dma((PLANE + 1,)),
        dma((PLANE + 1,)),
        dma((PLANE,)),
        dma((PLANE,)),
        dma((steps,)),
        dma((steps,)),
        dma((steps, PLANE - 1)),
        dma((steps // 2, PLANE - 1)),
    ]
    spec = pl.BlockSpec(memory_space=pltpu.VMEM)
    return pl.pallas_call(
        functools.partial(layer_kernel, (nz,)),
        name="layer",
        out_shape=jax.ShapeDtypeStruct((rows, feats), tokens.dtype),
        in_specs=[pl.BlockSpec(memory_space=pl.ANY)] * 12,
        out_specs=spec,
        scratch_shapes=scratch,
        compiler_params=pltpu.CompilerParams(
            collective_id=0, has_side_effects=True, vmem_limit_bytes=67_043_328
        ),
    )(
        tokens,
        u_weight,
        v_weight,
        sg_gain[None],
        spatial,
        bias,
        out_weight,
        gain_one[None],
        gate,
        up,
        down,
        gain_two[None],
    )


def fits(tokens, u_weight, gate_weight, spatial_weight):
    if lax.axis_size("tp") != 2 or lax.axis_size("fs") != 4 * PLANE:
        return False
    quarter = gate_weight.shape[1] % PLANE == 0 and gate_weight.shape[1] // PLANE % 16 == 0
    lanes = u_weight.shape[0] % 128 == 0 and u_weight.shape[1] % 256 == 0
    return quarter and lanes and tokens.shape[0] % (PLANE * spatial_weight.shape[1]) == 0


def choose(*args):
    if fits(args[0], args[1], args[8], args[4]):
        return in_one_kernel(*args)
    return on_device(*args)


def solution(mesh):
    return jax.shard_map(
        choose,
        mesh=mesh,
        in_specs=(
            P("fs", "tp"),
            P("fs", "tp"),
            P("fs", "tp"),
            P("tp"),
            P("tp", None, None),
            P("tp", None),
            P("tp", "fs"),
            P("tp"),
            P("fs", "tp"),
            P("fs", "tp"),
            P("tp", "fs"),
            P("tp"),
        ),
        out_specs=P("fs", "tp"),
        check_vma=False,
    )
```

```python
import functools

import jax
import jax.numpy as jnp
from jax import lax
from jax.experimental import pallas as pl
from jax.experimental.pallas import tpu as pltpu
from jax.sharding import PartitionSpec as P

EPS = 1e-05
ALPHA = 2.0**0.25


def add_rows(left, piece):
    return jnp.dot(left, piece, preferred_element_type=jnp.float32)


def scaled_rows(vals, sums, gain, count):
    mean = sums[0][:, None] / count
    square = sums[1][:, None] / count
    return (vals - mean) * lax.rsqrt(square - mean * mean + EPS) * gain[None, :]


def chip_sizes(count):
    across = 2 if count % 2 == 0 else 1
    down = 2 if (count // across) % 2 == 0 else 1
    return count // (across * down), down, across


def shift(value, sizes, axis, step=1):
    count = sizes[0] * sizes[1] * sizes[2]
    stride = sizes[1] * sizes[2] if axis == 0 else (sizes[2] if axis == 1 else 1)
    pairs = []
    for source in range(count):
        place = (source // stride) % sizes[axis]
        pairs.append((source, source + ((place + step) % sizes[axis] - place) * stride))
    return lax.ppermute(value, "fs", pairs)


def around(value, sizes, axis):
    if sizes[axis] == 4:
        near = shift(value, sizes, axis, 1)
        last = shift(value, sizes, axis, -1)
        return [value, near, shift(near, sizes, axis, 1), last]
    pieces = [value]
    for _ in range(sizes[axis] - 1):
        pieces.append(shift(pieces[-1], sizes, axis))
    return pieces


def ring(value, sizes, axis, place):
    return in_order(around(value, sizes, axis), place)


def other_core(value):
    return lax.ppermute(value, "tp", [(0, 1), (1, 0)])


def all_features(value):
    if lax.axis_size("tp") != 2:
        return lax.all_gather(value, "tp", axis=1, tiled=True)
    return jnp.concatenate(in_two(value, other_core(value), lax.axis_index("tp")), axis=1)


def in_two(mine, other, place):
    return [jnp.where(place == 0, mine, other), jnp.where(place == 0, other, mine)]


def sum_shares(terms):
    if lax.axis_size("tp") != 2:
        return lax.psum_scatter(terms, "tp", scatter_dimension=1, tiled=True)
    core = lax.axis_index("tp")
    half = terms.shape[1] // 2
    mine = lax.dynamic_slice_in_dim(terms, core * half, half, 1)
    sent = lax.dynamic_slice_in_dim(terms, (1 - core) * half, half, 1)
    return (mine.astype(jnp.float32) + other_core(sent).astype(jnp.float32)).astype(jnp.bfloat16)


def in_order(pieces, place):
    count = len(pieces)
    if count == 1:
        return pieces[0][None]
    held = jnp.zeros((count,) + pieces[0].shape, pieces[0].dtype)
    for step, piece in enumerate(pieces):
        start = lax.rem(place - step + count, count)
        held = lax.dynamic_update_slice_in_dim(held, piece[None], start, 0)
    return held


def gather_all(piece, sizes, places, order):
    held = piece
    for axis in order:
        held = ring(held, sizes, axis, places[axis])
    back = [order[::-1].index(axis) for axis in range(3)]
    rest = [3 + i for i in range(piece.ndim)]
    return jnp.transpose(held, back + rest)


def after(value, *others):
    return lax.optimization_barrier((value,) + others)[0]


def share_pieces(weight, dim, sizes, places, level, marks):
    across = sizes[2]
    width = weight.shape[dim] // across
    if across == 2:
        mine = lax.dynamic_slice_in_dim(weight, places[2] * width, width, dim)
        other = lax.dynamic_slice_in_dim(weight, (1 - places[2]) * width, width, dim)
        block = jnp.stack(in_two(mine, shift(other, sizes, 2), places[2]))
    else:
        block = weight[None]
    if sizes[0] != 4 or sizes[1] != 2:
        first = around(block, sizes, 0)
        return [[piece] if sizes[1] == 1 else [piece, shift(piece, sizes, 1)] for piece in first]
    if marks[0] is not None:
        block = after(block, marks[0])
    near, last = shift(block, sizes, 0, 1), shift(block, sizes, 0, -1)
    beside = shift(block if marks[0] is None else after(block, marks[1]), sizes, 1)
    near, last = after(near, marks[1]), after(last, marks[1])
    far = shift(near, sizes, 0)
    near_beside, last_beside = shift(near, sizes, 1), shift(last, sizes, 1)
    if level:
        far_beside = shift(after(near_beside, marks[2]), sizes, 0)
    else:
        far = after(far, marks[2])
        far_beside = shift(far, sizes, 1)
    return [[block, beside], [near, near_beside], [far, far_beside], [last, last_beside]]


def place_pieces(pieces, places):
    shape = pieces[0][0].shape
    count, down = len(pieces), len(pieces[0])
    held = jnp.zeros((count, down) + shape, pieces[0][0].dtype)
    for step, pair in enumerate(pieces):
        start = lax.rem(places[0] - step + count, count)
        for turn, piece in enumerate(pair):
            spot = places[1] if turn == 0 else 1 - places[1]
            held = lax.dynamic_update_slice(held, piece[None, None], [start, spot] + [0] * len(shape))
    return held


def on_device(
    tokens,
    u_weight,
    v_weight,
    sg_gain,
    spatial_weight,
    spatial_bias,
    out_weight,
    gain_one,
    gate_weight,
    up_weight,
    down_weight,
    gain_two,
):
    parts = lax.axis_size("tp")
    sizes = chip_sizes(lax.axis_size("fs"))
    index = lax.axis_index("fs")
    places = (index // (sizes[1] * sizes[2]), (index // sizes[2]) % sizes[1], index % sizes[2])
    whole = all_features(tokens)
    rows = whole.shape[0]
    width_sg = u_weight.shape[1]

    def add_one(piece):
        return add_rows(whole, piece)

    pre_u = add_one(gather_all(u_weight, sizes, places, [0, 1, 2]).reshape(-1, width_sg))
    pre_v = add_one(gather_all(v_weight, sizes, places, [0, 2, 1]).reshape(-1, width_sg))
    gated = jax.nn.gelu(pre_u)
    valued = jax.nn.gelu(pre_v)
    stats = lax.psum((jnp.sum(valued, axis=1), jnp.sum(valued * valued, axis=1)), "tp")
    normed = scaled_rows(valued, stats, sg_gain, width_sg * parts).astype(jnp.bfloat16)
    groups_here = spatial_weight.shape[0]
    block = spatial_weight.shape[1]
    group_width = width_sg // groups_here
    shaped = normed.reshape(rows // block, block, groups_here, group_width)
    lower = jnp.tril(jnp.ones((block, block), jnp.bool_))
    masked = jnp.where(lower[None], spatial_weight, jnp.zeros_like(spatial_weight))
    mixed = jnp.einsum("gij,njgd->nigd", masked, shaped, preferred_element_type=jnp.float32)
    mixed = mixed + spatial_bias.T[None, :, :, None]
    gated_out = (gated * mixed.reshape(rows, width_sg)).astype(jnp.bfloat16)
    out_all = gather_all(out_weight, sizes, places, [0, 1, 2])
    out_all = out_all.reshape((-1,) + out_weight.shape)
    terms = jnp.einsum("tk,nkc->tnc", gated_out, out_all, preferred_element_type=jnp.float32)
    mix = sum_shares(terms.reshape(rows, -1).astype(jnp.bfloat16))
    resid = ALPHA * tokens.astype(jnp.float32) + mix.astype(jnp.float32)
    first_sums = lax.psum((jnp.sum(resid, axis=1), jnp.sum(resid * resid, axis=1)), "tp")
    first = scaled_rows(resid, first_sums, gain_one, resid.shape[1] * parts).astype(jnp.bfloat16)
    gate_pieces = share_pieces(gate_weight, 1, sizes, places, False, (None, normed, mix))
    up_pieces = share_pieces(up_weight, 1, sizes, places, True, (None, normed, mix))
    down_pieces = share_pieces(down_weight, 0, sizes, places, False, (normed, first, first))
    gate_all = place_pieces(gate_pieces, places)
    gate_all = gate_all.reshape(-1, gate_all.shape[-1])
    up_all = place_pieces(up_pieces, places)
    up_all = up_all.reshape(-1, up_all.shape[-1])
    def feed(part):
        whole_part = all_features(part)
        gate = add_rows(whole_part, gate_all)
        upper = add_rows(whole_part, up_all)
        return (jax.nn.silu(gate) * upper).astype(jnp.bfloat16)

    two = sizes[2] == 2
    if two:
        there = feed(shift(first, sizes, 2))
        here = feed(first)
        down_pieces = [[pair[0]] + [after(piece, there, here) for piece in pair[1:]] for pair in down_pieces]
    else:
        here = feed(first)
    down_all = place_pieces(down_pieces, places)
    down_all = down_all.reshape((-1,) + down_all.shape[-2:])

    def project(hidden):
        made = jnp.einsum("tf,nfc->tnc", hidden, down_all, preferred_element_type=jnp.float32)
        return sum_shares(made.reshape(rows, -1).astype(jnp.bfloat16))

    if two:
        there = project(there)
        sent = shift(there, sizes, 2)
        ffn = project(after(here, there)).astype(jnp.float32) + sent.astype(jnp.float32)
    else:
        ffn = project(here).astype(jnp.float32)
    second = ALPHA * first.astype(jnp.float32) + ffn.astype(jnp.float32)
    last_sums = lax.psum((jnp.sum(second, axis=1), jnp.sum(second * second, axis=1)), "tp")
    return scaled_rows(second, last_sums, gain_two, second.shape[1] * parts).astype(jnp.bfloat16)


MESH = pl.DeviceIdType.MESH
PLANE = 4
CUTS = (2, 2, 4)
LAG = 4
SLOTS = 8


def layer_kernel(
    sizes,
    tok_in,
    u_in,
    v_in,
    sg_gain_in,
    spatial_in,
    bias_in,
    o_in,
    gain_one_in,
    gate_in,
    up_in,
    down_in,
    gain_two_in,
    out,
    tok,
    sg_gain,
    spatial,
    bias,
    gain_one,
    gain_two,
    gate_own,
    up_own,
    gate_turned,
    up_turned,
    tok_o,
    u_all,
    v_all,
    o_all,
    gate_all,
    up_all,
    down_all,
    gated,
    valued,
    normed,
    gated_out,
    st_s,
    st_r,
    terms_r,
    resid,
    first_all,
    hidden,
    gate_acc,
    p_s,
    p_r,
    p_own,
    r_r,
    in_sem,
    sg_r,
    sg_z,
    sg_p,
    a2_s,
    a2_r,
    z_s,
    z_r,
    tok_sem,
    st_sem,
    terms_sem,
    first_s,
    first_r,
    swap_s,
    swap_r,
    d2_s,
    d2_r,
    rs_s,
    rs_r,
):
    nz = sizes[0]
    fs, c = lax.axis_index("fs"), lax.axis_index("tp")
    oc = 1 - c
    z, p = fs // PLANE, fs % PLANE
    y, x = p // 2, p % 2
    peers = [z * PLANE + (y + j // 2) % 2 * 2 + (x + j % 2) % 2 for j in range(PLANE)]
    inplane = [(y + j // 2) % 2 * 2 + (x + j % 2) % 2 for j in range(PLANE)]
    has_up, has_down = z < nz - 1, z > 0
    up_dev = jnp.where(has_up, fs + PLANE, fs - PLANE)
    down_dev = jnp.where(has_down, fs - PLANE, fs + PLANE)
    rows, feats = tok.shape
    kb, width_sg = u_in.shape
    depth = rows // PLANE
    quarter = hidden.shape[1]
    plane_cols = PLANE * kb

    def mult(value, by):
        return pl.multiple_of(value, by)

    def seq(k):
        swapped = jnp.where(k < 2, 1 - k, k)
        return jnp.where(z == 0, k, jnp.where(z == 1, swapped, jnp.where(z == 2, nz - 1 - swapped, nz - 1 - k)))

    def remote(src, dst, send, recv, dev, core=None):
        where_to = (dev, c if core is None else core)
        return pltpu.make_async_remote_copy(
            src_ref=src, dst_ref=dst, send_sem=send, recv_sem=recv, device_id=where_to, device_id_type=MESH
        )

    def start_if(pred, copy):
        pl.when(pred)(lambda: copy.start())

    def sent_if(pred, copy):
        pl.when(pred)(lambda: copy.wait_send())

    own_rows = pl.ds(mult(fs * kb, kb), kb)
    own_quarter = pl.ds(mult(p * quarter, 16), quarter)
    loads = [
        (gate_in, gate_own),
        (up_in, up_own),
        (u_in, u_all.at[own_rows, :]),
        (v_in, v_all.at[own_rows, :]),
        (o_in, o_all.at[:, own_rows]),
        (down_in.at[own_quarter, :], down_all.at[:, own_rows]),
        (tok_in, tok),
        (sg_gain_in, sg_gain),
        (spatial_in, spatial),
        (bias_in, bias),
        (gain_one_in, gain_one),
        (gain_two_in, gain_two),
    ]
    loads = [pltpu.make_async_copy(src, dst, in_sem.at[i]) for i, (src, dst) in enumerate(loads)]
    for load in loads:
        load.start()
    barrier = pltpu.get_barrier_semaphore()
    for dev, core in [(fs, oc)] + [(peers[j], c) for j in range(1, PLANE)]:
        pl.semaphore_signal(barrier, inc=1, device_id=(dev, core), device_id_type=MESH)
    for pred, dev in [(has_up, up_dev), (has_down, down_dev)]:
        @pl.when(pred)
        def _():
            pl.semaphore_signal(barrier, inc=1, device_id=(dev, c), device_id_type=MESH)
    pl.semaphore_wait(barrier, PLANE + jnp.where(has_up, 1, 0) + jnp.where(has_down, 1, 0))

    def rows_of(ref):
        return lambda i: ref.at[pl.ds(mult(i * kb, kb), kb), :]

    def cols_of(ref, part):
        height = width_sg // 2
        return lambda i: ref.at[pl.ds(part * height, height), pl.ds(mult(i * kb, kb), kb)]

    half_o = width_sg // 2
    items = [
        (u_in, rows_of(u_all), 1, 2),
        (v_in, rows_of(v_all), 2, 1),
        (o_in.at[pl.ds(0, half_o), :], cols_of(o_all, 0), 1, 2),
        (o_in.at[pl.ds(half_o, half_o), :], cols_of(o_all, 1), 2, 1),
    ]

    def own_copies(n):
        src, at, one, two = items[n]
        return [
            (has_up, remote(src, at(fs), sg_z.at[n, 0, 0], sg_r.at[n, fs], up_dev)),
            (has_down, remote(src, at(fs), sg_z.at[n, 0, 1], sg_r.at[n, fs], down_dev)),
            (None, remote(src, at(fs), sg_p.at[n, 0, 0], sg_r.at[n, fs], peers[one])),
            (None, remote(src, at(fs), sg_p.at[n, 0, 1], sg_r.at[n, fs], peers[two])),
        ]

    def own_start(n):
        for pred, copy in own_copies(n):
            if pred is None:
                copy.start()
            else:
                start_if(pred, copy)

    def forward_to(b):
        going_up = b < z
        return (going_up & has_up) | ((b > z) & has_down), jnp.where(going_up, up_dev, down_dev)

    def column_copies(n, k):
        _, at, one, two = items[n]
        b = seq(k)
        idx = b * PLANE + p
        pred, dev = forward_to(b)
        ref, recv = at(idx), sg_r.at[n, idx]
        return [
            (pred, remote(ref, ref, sg_z.at[n, k, 0], recv, dev)),
            (None, remote(ref, ref, sg_p.at[n, k, 0], recv, peers[one])),
            (None, remote(ref, ref, sg_p.at[n, k, 1], recv, peers[two])),
        ]

    def column(n, k):
        copies = column_copies(n, k)
        copies[0][1].wait_recv()
        start_if(*copies[0])
        copies[1][1].start()
        copies[2][1].start()

    def beside_copy(n, k):
        _, at, one, two = items[n]
        idx = seq(k) * PLANE + inplane[one]
        ref, recv = at(idx), sg_r.at[n, idx]
        return remote(ref, ref, sg_p.at[n, k, 2], recv, peers[two])

    def beside(n, k):
        copy = beside_copy(n, k)
        copy.wait_recv()
        copy.start()

    def gathered(n):
        _, at, one, two = items[n]

        def arrive(b, carry):
            for j in (two, 3):
                idx = b * PLANE + inplane[j]
                ref = at(idx)
                remote(ref, ref, sg_p.at[n, 0, 0], sg_r.at[n, idx], peers[two]).wait_recv()
            return carry

        lax.fori_loop(0, nz, arrive, 0)

    wides = [(gate_turned, gate_all), (up_turned, up_all), (down_in, down_all)]

    def quarter_copy(w, j):
        src, dst = wides[w]
        theirs = pl.ds(mult(inplane[j] * quarter, 16), quarter)
        mine = pl.ds(mult(fs * kb, kb), kb)
        return remote(src.at[theirs, :], dst.at[:, mine], a2_s.at[w, j - 1], a2_r.at[w, j - 1], peers[j])

    def quarters_start(w):
        for j in range(1, PLANE):
            quarter_copy(w, j).start()

    def block(w, b, h):
        cols = plane_cols // CUTS[w]
        return wides[w][1].at[:, pl.ds(mult(b * plane_cols + h * cols, cols), cols)]

    def own_block_copies(w, h):
        ref, recv = block(w, z, h), z_r.at[w, z, h]
        return [
            (has_up, remote(ref, ref, z_s.at[w, 0, h, 0], recv, up_dev)),
            (has_down, remote(ref, ref, z_s.at[w, 0, h, 1], recv, down_dev)),
        ]

    def own_block(w):
        for j in range(1, PLANE):
            ref = wides[w][1].at[:, pl.ds(mult(peers[j] * kb, kb), kb)]
            remote(ref, ref, a2_s.at[w, j - 1], a2_r.at[w, j - 1], peers[j]).wait_recv()
        for h in range(CUTS[w]):
            for pred, copy in own_block_copies(w, h):
                start_if(pred, copy)

    def pass_copy(w, k, h):
        b = seq(k)
        pred, dev = forward_to(b)
        ref = block(w, b, h)
        return pred, remote(ref, ref, z_s.at[w, k, h, 0], z_r.at[w, b, h], dev)

    def pass_on(w, k, h):
        pred, copy = pass_copy(w, k, h)

        @pl.when(pred)
        def _():
            copy.wait_recv()
            copy.start()

    def need(w, k, h):
        pred, copy = pass_copy(w, k, h)
        pl.when(jnp.logical_not(pred))(lambda: copy.wait_recv())

    lane = lax.broadcasted_iota(jnp.int32, (depth, 128), 1)

    def put_stats(which, place, vals):
        one = jnp.sum(vals, axis=1, keepdims=True)
        two = jnp.sum(vals * vals, axis=1, keepdims=True)
        st_s[which, place, :] = jnp.where(lane == 0, one, two)

    def stats_copy(which):
        return remote(st_s.at[which], st_r.at[which], st_sem.at[which, 0], st_sem.at[which, 1], fs, oc)

    def normalize(which, place, vals, gain, count):
        both = st_s[which, place, :] + st_r[which, place, :]
        mean = both[:, 0:1] / count
        square = both[:, 1:2] / count
        return (vals - mean) * lax.rsqrt(square - mean * mean + EPS) * gain

    def loop(count, body):
        lax.fori_loop(0, count, lambda i, carry: (body(i), carry)[1], 0)

    def part(i):
        return pl.ds(mult(i * depth, depth), depth)

    tok_copy = remote(tok_in, tok_o, tok_sem.at[0], tok_sem.at[1], fs, oc)
    own_start(0)
    own_start(1)

    def turn(src, dst):
        def step(i):
            place = pl.ds(mult(i * kb, kb), kb)
            dst[place, :] = src[:, place].T

        loop(src.shape[1] // kb, step)

    loads[0].wait()
    turn(gate_own, gate_turned)
    quarters_start(0)
    own_start(2)
    own_start(3)
    tok_copy.start()
    for load in loads[1:]:
        load.wait()
    turn(up_own, up_turned)
    gate_all[:, own_rows] = gate_turned[own_quarter, :]
    up_all[:, own_rows] = up_turned[own_quarter, :]

    for n in (0, 1):
        column(n, 1)
    for n in (0, 1):
        column(n, 2)
    for n in (2, 3):
        column(n, 1)
    for n in (0, 1):
        column(n, 3)
    for n in (2, 3):
        column(n, 2)
    own_block(0)
    for k in (0, 1):
        for n in (0, 1):
            beside(n, k)
    for n in (2, 3):
        column(n, 3)
    pass_on(0, 1, 0)
    pass_on(0, 2, 0)
    for n in (0, 1):
        beside(n, 2)
    pass_on(0, 1, 1)
    pass_on(0, 2, 1)
    for n in (0, 1):
        beside(n, 3)
    quarters_start(1)
    for n in (2, 3):
        beside(n, 0)
    for n in (2, 3):
        beside(n, 1)
    pass_on(0, 3, 0)
    for n in (2, 3):
        beside(n, 2)

    tok_copy.wait_recv()
    wide = 256
    mine_k = pl.ds(mult(c * feats, feats), feats)
    their_k = pl.ds(mult(oc * feats, feats), feats)

    def branch(weight, into):
        def step(n):
            cols = pl.ds(mult(n * wide, wide), wide)
            acc = add_rows(tok[...], weight[mine_k, cols]) + add_rows(tok_o[...], weight[their_k, cols])
            into[:, cols] = jax.nn.gelu(acc)

        loop(width_sg // wide, step)

    gathered(0)
    branch(u_all, gated)
    gathered(1)
    branch(v_all, valued)
    for n in (2, 3):
        beside(n, 3)
    pass_on(0, 3, 1)
    loop(rows // depth, lambda i: put_stats(0, part(i), valued[part(i), :]))
    stats_copy(0).start()
    stats_copy(0).wait_recv()

    def norm_gate(i):
        vals = normalize(0, part(i), valued[part(i), :], sg_gain[...], 2 * width_sg)
        normed[part(i), :] = vals.astype(jnp.bfloat16)

    loop(rows // depth, norm_gate)
    groups, spread = spatial.shape[0], spatial.shape[1]
    row_at = lax.broadcasted_iota(jnp.int32, (spread, spread), 0)
    col_at = lax.broadcasted_iota(jnp.int32, (spread, spread), 1)
    group_dim = width_sg // groups

    def mix_block(n):
        place = pl.ds(mult(n * spread, spread), spread)
        for g in range(groups):
            cols = pl.ds(g * group_dim, group_dim)
            weight = jnp.where(col_at <= row_at, spatial[g], jnp.zeros_like(spatial[g]))
            shift_by = jnp.sum(jnp.where(col_at == row_at, bias[g : g + 1, :], 0.0), axis=1, keepdims=True)
            mixed = jnp.dot(weight, normed[place, cols], preferred_element_type=jnp.float32) + shift_by
            gated_out[place, cols] = (gated[place, cols] * mixed).astype(jnp.bfloat16)

    loop(rows // spread, mix_block)
    for n in (2, 3):
        gathered(n)

    terms_s, terms_o = p_s.at[pl.ds(0, rows), :], p_s.at[pl.ds(rows, rows), :]

    def project_out(which, into):
        def step(n):
            cols = pl.ds(mult(which * feats + n * wide, wide), wide)
            to = pl.ds(mult(n * wide, wide), wide)
            into[:, to] = add_rows(gated_out[...], o_all[:, cols]).astype(jnp.bfloat16)

        loop(feats // wide, step)

    project_out(oc, terms_s)
    terms_copy = remote(terms_s, terms_r, terms_sem.at[0], terms_sem.at[1], fs, oc)
    terms_copy.start()
    project_out(c, terms_o)
    own_block(1)
    terms_copy.wait_recv()

    def add_mix(i):
        mix = terms_o[part(i), :].astype(jnp.float32) + terms_r[part(i), :].astype(jnp.float32)
        vals = ALPHA * tok[part(i), :].astype(jnp.float32) + mix.astype(jnp.bfloat16).astype(jnp.float32)
        resid[part(i), :] = vals
        put_stats(1, part(i), vals)

    loop(rows // depth, add_mix)
    stats_copy(1).start()
    stats_copy(1).wait_recv()
    mine_cols = pl.ds(mult(c * feats, feats), feats)
    their_cols = pl.ds(mult(oc * feats, feats), feats)

    def norm_first(i):
        vals = normalize(1, part(i), resid[part(i), :], gain_one[...], 2 * feats)
        vals = vals.astype(jnp.bfloat16)
        first_all[pl.ds(mult(p * rows + i * depth, depth), depth), mine_cols] = vals
        resid[part(i), :] = ALPHA * vals.astype(jnp.float32)

    loop(rows // depth, norm_first)

    def place_of(j):
        return (y + j // 2) % 2 * 2 + (x + j % 2) % 2

    def tokens_of(j, cols):
        return first_all.at[pl.ds(mult(place_of(j) * rows, rows), rows), cols]

    def swap_copy(j):
        ref = tokens_of(j, mine_cols)
        return remote(ref, ref, swap_s.at[j], swap_r.at[j], fs, oc)

    own_tokens = tokens_of(0, mine_cols)
    first_copies = [
        remote(own_tokens, own_tokens, first_s.at[j], first_r.at[j], peers[j]) for j in (1, 2)
    ]

    def corner_copy(j):
        start = mult(place_of(j) * rows + (j - 1) * (rows // 2), rows // 2)
        ref = first_all.at[pl.ds(start, rows // 2), mine_cols]
        return remote(ref, ref, first_s.at[j + 2], first_r.at[j + 2], z * PLANE + place_of(PLANE - 1 - j))

    swap_copy(0).start()
    for copy in first_copies:
        copy.start()
    quarters_start(2)

    for k in range(1, nz):
        for h in range(CUTS[0]):
            need(0, k, h)

    tiles = [(t, min(wide, quarter - t)) for t in range(0, quarter, wide)]

    def across(left, weight, t, n):
        return lax.dot_general(
            left, weight[pl.ds(t, n), :], (((1,), (1,)), ((), ())), preferred_element_type=jnp.float32
        )

    def row_block(j):
        return pl.ds(mult(place_of(j) * rows, rows), rows)

    def gate_step(j):
        @pl.when((j == 1) | (j == 2))
        def _():
            ref = tokens_of(j, mine_cols)
            remote(ref, ref, first_s.at[j], first_r.at[j], fs, oc).wait_recv()
            corner_copy(j).start()

        @pl.when(j == PLANE - 1)
        def _():
            for half in (0, 1):
                start = mult(place_of(j) * rows + half * (rows // 2), rows // 2)
                ref = first_all.at[pl.ds(start, rows // 2), mine_cols]
                remote(ref, ref, first_s.at[half + 3], first_r.at[half + 3], fs, oc).wait_recv()

        @pl.when(j > 0)
        def _():
            swap_copy(j).start()

        ref = tokens_of(j, their_cols)
        remote(ref, ref, swap_s.at[j], swap_r.at[j], fs, oc).wait_recv()
        left = row_block(j)
        for t, n in tiles:
            gate_acc[left, pl.ds(t, n)] = jax.nn.silu(across(first_all[left, :], gate_all, t, n))

        @pl.when(j == 0)
        def _():
            for h in range(CUTS[1]):
                pass_on(1, 1, h)
                pass_on(1, 2, h)

        @pl.when((j == 1) | (j == 2))
        def _():
            pass_on(1, 3, j - 1)

        pl.when(j == 2)(lambda: own_block(2))

    loop(PLANE, gate_step)
    for k in range(1, nz):
        for h in range(CUTS[1]):
            need(1, k, h)

    def up_step(j):
        left = row_block(j)
        for t, n in tiles:
            acc = gate_acc[left, pl.ds(t, n)] * across(first_all[left, :], up_all, t, n)
            hidden[left, pl.ds(t, n)] = acc.astype(jnp.bfloat16)

    terms_copy.wait_send()

    cut = CUTS[2]
    half_cols = plane_cols // cut
    steps = nz * cut
    per_core = steps // 2
    units = steps * PLANE
    early = cut * PLANE

    def unit(t):
        order = jnp.where(t < early, t // cut, (t - early) % PLANE)
        i = jnp.where(t < early, t % cut, cut + (t - early) // PLANE)
        j = jnp.where(order == 0, PLANE - 1, jnp.where(order == PLANE - 1, 0, order))
        inner = (i >= cut) & (i < 3 * cut) & has_up & has_down
        k = jnp.where(inner, 1 + i % 2, i // cut)
        h = jnp.where(inner, (i - cut) // 2, i % cut)
        at = seq(k) * cut + h
        return order, j, k, h, at

    def owned(at):
        return at // per_core == c, pl.ds(mult(at % per_core * half_cols, half_cols), half_cols)

    def pair_copy(t):
        _, j, _, _, at = unit(t)
        ref = (row_block(j), owned(at)[1])
        return remote(p_s.at[ref], p_r.at[ref], d2_s, d2_r.at[at, j], fs, oc)

    def rows_copy(t):
        _, j, _, _, at = unit(t)
        cols = owned(at)[1]
        pick = jnp.maximum(j - 1, 0)
        return remote(
            p_r.at[row_block(j), cols],
            r_r.at[pick, :, cols],
            rs_s,
            rs_r,
            z * PLANE + place_of(j),
        )

    def finish(t):
        _, j, _, _, at = unit(t)
        mine, cols = owned(at)

        @pl.when(mine)
        def _():
            pair_copy(t).wait_recv()
            place = row_block(j)
            both = p_own[t % SLOTS].astype(jnp.float32) + p_r[place, cols].astype(jnp.float32)
            p_r[place, cols] = both.astype(jnp.bfloat16)
            pl.when(j > 0)(lambda: rows_copy(t).start())

    def unit_step(t):
        order, j, k, h, at = unit(t)
        mine, cols = owned(at)
        pl.when((t < early) & (t % cut == 0))(lambda: up_step(j))

        @pl.when((t % cut == 0) & (t > 0) & (t <= early))
        def _():
            pass_on(2, 1, t // cut - 1)
            pass_on(2, 2, t // cut - 1)

        late = (t - early) // PLANE
        third = (t >= early + 3 * PLANE) & (late % 2 == 1) & (late < 2 * cut + 2)

        @pl.when(third & (order == 0))
        def _():
            pass_on(2, 3, (late - 3) // 2)

        pl.when((k > 0) & (order == 0))(lambda: need(2, k, h))

        from_cols = pl.ds(mult(at * half_cols, half_cols), half_cols)
        place = row_block(j)
        made = add_rows(hidden[place, :], down_all[:, from_cols]).astype(jnp.bfloat16)

        @pl.when(mine)
        def _():
            p_own[t % SLOTS] = made

        @pl.when(jnp.logical_not(mine))
        def _():
            p_s[place, cols] = made
            pair_copy(t).start()

        pl.when(t >= LAG)(lambda: finish(t - LAG))

    loop(units, unit_step)
    loop(LAG, lambda i: finish(units - LAG + i))

    remote(r_r, r_r, rs_s, rs_r, peers[1]).wait_recv()

    def add_ffn(i):
        total = p_r[pl.ds(mult(p * rows + i * depth, depth), depth), :].astype(jnp.float32)
        for j in range(1, PLANE):
            total = total + r_r[j - 1, part(i), :].astype(jnp.float32)
        vals = resid[part(i), :] + total.astype(jnp.bfloat16).astype(jnp.float32)
        resid[part(i), :] = vals
        put_stats(2, part(i), vals)

    loop(rows // depth, add_ffn)
    stats_copy(2).start()

    tok_copy.wait_send()
    stats_copy(0).wait_send()
    stats_copy(1).wait_send()
    for copy in first_copies:
        copy.wait_send()
    for j in (1, 2):
        corner_copy(j).wait_send()
    loop(PLANE, lambda j: swap_copy(j).wait_send())
    for n in range(len(items)):
        for pred, copy in own_copies(n):
            sent_if(True if pred is None else pred, copy) if pred is not None else copy.wait_send()

        def sent(i):
            copies = column_copies(n, i + 1)
            sent_if(*copies[0])
            copies[1][1].wait_send()
            copies[2][1].wait_send()

        loop(nz - 1, sent)
        loop(nz, lambda k: beside_copy(n, k).wait_send())
    for w in range(len(wides)):
        for j in range(1, PLANE):
            quarter_copy(w, j).wait_send()
        for h in range(CUTS[w]):
            for pred, copy in own_block_copies(w, h):
                sent_if(pred, copy)
            loop(nz - 1, lambda i: sent_if(*pass_copy(w, i + 1, h)))

    remote(p_s, p_r, d2_s, d2_s, fs, oc).wait_send()
    remote(r_r, r_r, rs_s, rs_r, peers[1]).wait_send()
    stats_copy(2).wait_recv()

    def norm_last(i):
        vals = normalize(2, part(i), resid[part(i), :], gain_two[...], 2 * feats)
        out[part(i), :] = vals.astype(out.dtype)

    loop(rows // depth, norm_last)
    stats_copy(2).wait_send()


def in_one_kernel(*args):
    (tokens, u_weight, v_weight, sg_gain, spatial, bias, out_weight, gain_one, gate, up, down, gain_two) = args
    nz = lax.axis_size("fs") // PLANE
    rows, feats = tokens.shape
    width_sg = u_weight.shape[1]
    quarter = down.shape[0] // PLANE
    wide = 2 * feats
    plane_rows = PLANE * rows
    bf16, f32 = jnp.bfloat16, jnp.float32
    vmem, dma = pltpu.VMEM, pltpu.SemaphoreType.DMA
    steps = nz * CUTS[2]
    half_cols = wide // steps
    scratch = [
        vmem((rows, feats), bf16),
        vmem((1, width_sg), f32),
        vmem(spatial.shape, bf16),
        vmem(bias.shape, f32),
        vmem((1, feats), f32),
        vmem((1, feats), f32),
        vmem(gate.shape, bf16),
        vmem(gate.shape, bf16),
        vmem(gate.shape[::-1], bf16),
        vmem(gate.shape[::-1], bf16),
        vmem((rows, feats), bf16),
        vmem((wide, width_sg), bf16),
        vmem((wide, width_sg), bf16),
        vmem((width_sg, wide), bf16),
        vmem((quarter, wide), bf16),
        vmem((quarter, wide), bf16),
        vmem((quarter, wide), bf16),
        vmem((rows, width_sg), f32),
        vmem((rows, width_sg), f32),
        vmem((rows, width_sg), bf16),
        vmem((rows, width_sg), bf16),
        vmem((3, rows, 128), f32),
        vmem((3, rows, 128), f32),
        vmem((rows, feats), bf16),
        vmem((rows, feats), f32),
        vmem((plane_rows, wide), bf16),
        vmem((plane_rows, quarter), bf16),
        vmem((plane_rows, quarter), f32),
        vmem((plane_rows, feats), bf16),
        vmem((plane_rows, feats), bf16),
        vmem((SLOTS, rows, half_cols), bf16),
        vmem((PLANE - 1, rows, feats), bf16),
        dma((12,)),
        dma((4, nz * PLANE)),
        dma((4, nz, 2)),
        dma((4, nz, 3)),
        dma((3, PLANE - 1)),
        dma((3, PLANE - 1)),
        dma((3, nz, max(CUTS), 2)),
        dma((3, nz, max(CUTS))),
        dma((2,)),
        dma((3, 2)),
        dma((2,)),
        dma((PLANE + 1,)),
        dma((PLANE + 1,)),
        dma((PLANE,)),
        dma((PLANE,)),
        dma(()),
        dma((steps, PLANE)),
        dma(()),
        dma(()),
    ]
    spec = pl.BlockSpec(memory_space=pltpu.VMEM)
    return pl.pallas_call(
        functools.partial(layer_kernel, (nz,)),
        name="layer",
        out_shape=jax.ShapeDtypeStruct((rows, feats), tokens.dtype),
        in_specs=[pl.BlockSpec(memory_space=pl.ANY)] * 12,
        out_specs=spec,
        scratch_shapes=scratch,
        compiler_params=pltpu.CompilerParams(
            collective_id=0, has_side_effects=True, vmem_limit_bytes=67_043_328
        ),
    )(
        tokens,
        u_weight,
        v_weight,
        sg_gain[None],
        spatial,
        bias,
        out_weight,
        gain_one[None],
        gate,
        up,
        down,
        gain_two[None],
    )


def fits(tokens, u_weight, gate_weight, spatial_weight):
    if lax.axis_size("tp") != 2 or lax.axis_size("fs") != 4 * PLANE:
        return False
    quarter = gate_weight.shape[1] % PLANE == 0 and gate_weight.shape[1] // PLANE % 16 == 0
    lanes = u_weight.shape[0] % 128 == 0 and u_weight.shape[1] % 256 == 0
    return quarter and lanes and tokens.shape[0] % (PLANE * spatial_weight.shape[1]) == 0


def choose(*args):
    if fits(args[0], args[1], args[8], args[4]):
        return in_one_kernel(*args)
    return on_device(*args)


def solution(mesh):
    return jax.shard_map(
        choose,
        mesh=mesh,
        in_specs=(
            P("fs", "tp"),
            P("fs", "tp"),
            P("fs", "tp"),
            P("tp"),
            P("tp", None, None),
            P("tp", None),
            P("tp", "fs"),
            P("tp"),
            P("fs", "tp"),
            P("fs", "tp"),
            P("tp", "fs"),
            P("tp"),
        ),
        out_specs=P("fs", "tp"),
        check_vma=False,
    )
```

```python
import functools

import jax
import jax.numpy as jnp
from jax import lax
from jax.experimental import pallas as pl
from jax.experimental.pallas import tpu as pltpu
from jax.sharding import PartitionSpec as P

EPS = 1e-05
ALPHA = 2.0**0.25


def add_rows(left, piece):
    return jnp.dot(left, piece, preferred_element_type=jnp.float32)


def scaled_rows(vals, sums, gain, count):
    mean = sums[0][:, None] / count
    square = sums[1][:, None] / count
    return (vals - mean) * lax.rsqrt(square - mean * mean + EPS) * gain[None, :]


def chip_sizes(count):
    across = 2 if count % 2 == 0 else 1
    down = 2 if (count // across) % 2 == 0 else 1
    return count // (across * down), down, across


def shift(value, sizes, axis, step=1):
    count = sizes[0] * sizes[1] * sizes[2]
    stride = sizes[1] * sizes[2] if axis == 0 else (sizes[2] if axis == 1 else 1)
    pairs = []
    for source in range(count):
        place = (source // stride) % sizes[axis]
        pairs.append((source, source + ((place + step) % sizes[axis] - place) * stride))
    return lax.ppermute(value, "fs", pairs)


def around(value, sizes, axis):
    if sizes[axis] == 4:
        near = shift(value, sizes, axis, 1)
        last = shift(value, sizes, axis, -1)
        return [value, near, shift(near, sizes, axis, 1), last]
    pieces = [value]
    for _ in range(sizes[axis] - 1):
        pieces.append(shift(pieces[-1], sizes, axis))
    return pieces


def ring(value, sizes, axis, place):
    return in_order(around(value, sizes, axis), place)


def other_core(value):
    return lax.ppermute(value, "tp", [(0, 1), (1, 0)])


def all_features(value):
    if lax.axis_size("tp") != 2:
        return lax.all_gather(value, "tp", axis=1, tiled=True)
    return jnp.concatenate(in_two(value, other_core(value), lax.axis_index("tp")), axis=1)


def in_two(mine, other, place):
    return [jnp.where(place == 0, mine, other), jnp.where(place == 0, other, mine)]


def sum_shares(terms):
    if lax.axis_size("tp") != 2:
        return lax.psum_scatter(terms, "tp", scatter_dimension=1, tiled=True)
    core = lax.axis_index("tp")
    half = terms.shape[1] // 2
    mine = lax.dynamic_slice_in_dim(terms, core * half, half, 1)
    sent = lax.dynamic_slice_in_dim(terms, (1 - core) * half, half, 1)
    return (mine.astype(jnp.float32) + other_core(sent).astype(jnp.float32)).astype(jnp.bfloat16)


def in_order(pieces, place):
    count = len(pieces)
    if count == 1:
        return pieces[0][None]
    held = jnp.zeros((count,) + pieces[0].shape, pieces[0].dtype)
    for step, piece in enumerate(pieces):
        start = lax.rem(place - step + count, count)
        held = lax.dynamic_update_slice_in_dim(held, piece[None], start, 0)
    return held


def gather_all(piece, sizes, places, order):
    held = piece
    for axis in order:
        held = ring(held, sizes, axis, places[axis])
    back = [order[::-1].index(axis) for axis in range(3)]
    rest = [3 + i for i in range(piece.ndim)]
    return jnp.transpose(held, back + rest)


def after(value, *others):
    return lax.optimization_barrier((value,) + others)[0]


def share_pieces(weight, dim, sizes, places, level, marks):
    across = sizes[2]
    width = weight.shape[dim] // across
    if across == 2:
        mine = lax.dynamic_slice_in_dim(weight, places[2] * width, width, dim)
        other = lax.dynamic_slice_in_dim(weight, (1 - places[2]) * width, width, dim)
        block = jnp.stack(in_two(mine, shift(other, sizes, 2), places[2]))
    else:
        block = weight[None]
    if sizes[0] != 4 or sizes[1] != 2:
        first = around(block, sizes, 0)
        return [[piece] if sizes[1] == 1 else [piece, shift(piece, sizes, 1)] for piece in first]
    if marks[0] is not None:
        block = after(block, marks[0])
    near, last = shift(block, sizes, 0, 1), shift(block, sizes, 0, -1)
    beside = shift(block if marks[0] is None else after(block, marks[1]), sizes, 1)
    near, last = after(near, marks[1]), after(last, marks[1])
    far = shift(near, sizes, 0)
    near_beside, last_beside = shift(near, sizes, 1), shift(last, sizes, 1)
    if level:
        far_beside = shift(after(near_beside, marks[2]), sizes, 0)
    else:
        far = after(far, marks[2])
        far_beside = shift(far, sizes, 1)
    return [[block, beside], [near, near_beside], [far, far_beside], [last, last_beside]]


def place_pieces(pieces, places):
    shape = pieces[0][0].shape
    count, down = len(pieces), len(pieces[0])
    held = jnp.zeros((count, down) + shape, pieces[0][0].dtype)
    for step, pair in enumerate(pieces):
        start = lax.rem(places[0] - step + count, count)
        for turn, piece in enumerate(pair):
            spot = places[1] if turn == 0 else 1 - places[1]
            held = lax.dynamic_update_slice(held, piece[None, None], [start, spot] + [0] * len(shape))
    return held


def on_device(
    tokens,
    u_weight,
    v_weight,
    sg_gain,
    spatial_weight,
    spatial_bias,
    out_weight,
    gain_one,
    gate_weight,
    up_weight,
    down_weight,
    gain_two,
):
    parts = lax.axis_size("tp")
    sizes = chip_sizes(lax.axis_size("fs"))
    index = lax.axis_index("fs")
    places = (index // (sizes[1] * sizes[2]), (index // sizes[2]) % sizes[1], index % sizes[2])
    whole = all_features(tokens)
    rows = whole.shape[0]
    width_sg = u_weight.shape[1]

    def add_one(piece):
        return add_rows(whole, piece)

    pre_u = add_one(gather_all(u_weight, sizes, places, [0, 1, 2]).reshape(-1, width_sg))
    pre_v = add_one(gather_all(v_weight, sizes, places, [0, 2, 1]).reshape(-1, width_sg))
    gated = jax.nn.gelu(pre_u)
    valued = jax.nn.gelu(pre_v)
    stats = lax.psum((jnp.sum(valued, axis=1), jnp.sum(valued * valued, axis=1)), "tp")
    normed = scaled_rows(valued, stats, sg_gain, width_sg * parts).astype(jnp.bfloat16)
    groups_here = spatial_weight.shape[0]
    block = spatial_weight.shape[1]
    group_width = width_sg // groups_here
    shaped = normed.reshape(rows // block, block, groups_here, group_width)
    lower = jnp.tril(jnp.ones((block, block), jnp.bool_))
    masked = jnp.where(lower[None], spatial_weight, jnp.zeros_like(spatial_weight))
    mixed = jnp.einsum("gij,njgd->nigd", masked, shaped, preferred_element_type=jnp.float32)
    mixed = mixed + spatial_bias.T[None, :, :, None]
    gated_out = (gated * mixed.reshape(rows, width_sg)).astype(jnp.bfloat16)
    out_all = gather_all(out_weight, sizes, places, [0, 1, 2])
    out_all = out_all.reshape((-1,) + out_weight.shape)
    terms = jnp.einsum("tk,nkc->tnc", gated_out, out_all, preferred_element_type=jnp.float32)
    mix = sum_shares(terms.reshape(rows, -1).astype(jnp.bfloat16))
    resid = ALPHA * tokens.astype(jnp.float32) + mix.astype(jnp.float32)
    first_sums = lax.psum((jnp.sum(resid, axis=1), jnp.sum(resid * resid, axis=1)), "tp")
    first = scaled_rows(resid, first_sums, gain_one, resid.shape[1] * parts).astype(jnp.bfloat16)
    gate_pieces = share_pieces(gate_weight, 1, sizes, places, False, (None, normed, mix))
    up_pieces = share_pieces(up_weight, 1, sizes, places, True, (None, normed, mix))
    down_pieces = share_pieces(down_weight, 0, sizes, places, False, (normed, first, first))
    gate_all = place_pieces(gate_pieces, places)
    gate_all = gate_all.reshape(-1, gate_all.shape[-1])
    up_all = place_pieces(up_pieces, places)
    up_all = up_all.reshape(-1, up_all.shape[-1])
    def feed(part):
        whole_part = all_features(part)
        gate = add_rows(whole_part, gate_all)
        upper = add_rows(whole_part, up_all)
        return (jax.nn.silu(gate) * upper).astype(jnp.bfloat16)

    two = sizes[2] == 2
    if two:
        there = feed(shift(first, sizes, 2))
        here = feed(first)
        down_pieces = [[pair[0]] + [after(piece, there, here) for piece in pair[1:]] for pair in down_pieces]
    else:
        here = feed(first)
    down_all = place_pieces(down_pieces, places)
    down_all = down_all.reshape((-1,) + down_all.shape[-2:])

    def project(hidden):
        made = jnp.einsum("tf,nfc->tnc", hidden, down_all, preferred_element_type=jnp.float32)
        return sum_shares(made.reshape(rows, -1).astype(jnp.bfloat16))

    if two:
        there = project(there)
        sent = shift(there, sizes, 2)
        ffn = project(after(here, there)).astype(jnp.float32) + sent.astype(jnp.float32)
    else:
        ffn = project(here).astype(jnp.float32)
    second = ALPHA * first.astype(jnp.float32) + ffn.astype(jnp.float32)
    last_sums = lax.psum((jnp.sum(second, axis=1), jnp.sum(second * second, axis=1)), "tp")
    return scaled_rows(second, last_sums, gain_two, second.shape[1] * parts).astype(jnp.bfloat16)


MESH = pl.DeviceIdType.MESH
PLANE = 4
CUTS = (2, 2, 4)
LAG = 4
SLOTS = 8


def layer_kernel(
    sizes,
    tok_in,
    u_in,
    v_in,
    sg_gain_in,
    spatial_in,
    bias_in,
    o_in,
    gain_one_in,
    gate_in,
    up_in,
    down_in,
    gain_two_in,
    out,
    tok,
    sg_gain,
    spatial,
    bias,
    gain_one,
    gain_two,
    gate_own,
    up_own,
    gate_turned,
    up_turned,
    tok_o,
    u_all,
    v_all,
    o_all,
    gate_all,
    up_all,
    down_all,
    gated,
    valued,
    normed,
    gated_out,
    st_s,
    st_r,
    terms_s,
    terms_o,
    terms_r,
    resid,
    first_all,
    hidden,
    gate_acc,
    p_s,
    p_r,
    p_own,
    r_r,
    in_sem,
    sg_r,
    sg_l,
    sg_z,
    sg_p,
    a2_s,
    a2_r,
    z_s,
    z_r,
    tok_sem,
    st_sem,
    terms_sem,
    first_s,
    first_r,
    swap_s,
    swap_r,
    d2_s,
    d2_r,
    rs_s,
    rs_r,
):
    nz = sizes[0]
    fs, c = lax.axis_index("fs"), lax.axis_index("tp")
    oc = 1 - c
    z, p = fs // PLANE, fs % PLANE
    y, x = p // 2, p % 2
    peers = [z * PLANE + (y + j // 2) % 2 * 2 + (x + j % 2) % 2 for j in range(PLANE)]
    inplane = [(y + j // 2) % 2 * 2 + (x + j % 2) % 2 for j in range(PLANE)]
    has_up, has_down = z < nz - 1, z > 0
    up_dev = jnp.where(has_up, fs + PLANE, fs - PLANE)
    down_dev = jnp.where(has_down, fs - PLANE, fs + PLANE)
    rows, feats = tok.shape
    kb, width_sg = u_in.shape
    depth = rows // PLANE
    quarter = hidden.shape[1]
    plane_cols = PLANE * kb

    def mult(value, by):
        return pl.multiple_of(value, by)

    def seq(k):
        swapped = jnp.where(k < 2, 1 - k, k)
        return jnp.where(z == 0, k, jnp.where(z == 1, swapped, jnp.where(z == 2, nz - 1 - swapped, nz - 1 - k)))

    def remote(src, dst, send, recv, dev, core=None):
        where_to = (dev, c if core is None else core)
        return pltpu.make_async_remote_copy(
            src_ref=src, dst_ref=dst, send_sem=send, recv_sem=recv, device_id=where_to, device_id_type=MESH
        )

    def start_if(pred, copy):
        pl.when(pred)(lambda: copy.start())

    def sent_if(pred, copy):
        pl.when(pred)(lambda: copy.wait_send())

    own_rows = pl.ds(mult(fs * kb, kb), kb)
    own_quarter = pl.ds(mult(p * quarter, 16), quarter)
    loads = [
        (gate_in, gate_own),
        (up_in, up_own),
        (u_in, u_all.at[own_rows, :]),
        (v_in, v_all.at[own_rows, :]),
        (o_in, o_all.at[:, own_rows]),
        (down_in.at[own_quarter, :], down_all.at[:, own_rows]),
        (tok_in, tok),
        (sg_gain_in, sg_gain),
        (spatial_in, spatial),
        (bias_in, bias),
        (gain_one_in, gain_one),
        (gain_two_in, gain_two),
    ]
    loads = [pltpu.make_async_copy(src, dst, in_sem.at[i]) for i, (src, dst) in enumerate(loads)]
    for load in loads:
        load.start()
    barrier = pltpu.get_barrier_semaphore()
    for dev, core in [(fs, oc)] + [(peers[j], c) for j in range(1, PLANE)]:
        pl.semaphore_signal(barrier, inc=1, device_id=(dev, core), device_id_type=MESH)
    for pred, dev in [(has_up, up_dev), (has_down, down_dev)]:
        @pl.when(pred)
        def _():
            pl.semaphore_signal(barrier, inc=1, device_id=(dev, c), device_id_type=MESH)
    pl.semaphore_wait(barrier, PLANE + jnp.where(has_up, 1, 0) + jnp.where(has_down, 1, 0))

    def rows_of(ref):
        return lambda i, count=1: ref.at[pl.ds(mult(i * kb, kb), count * kb), :]

    def cols_of(ref, part):
        height = width_sg // 2
        return lambda i, count=1: ref.at[pl.ds(part * height, height), pl.ds(mult(i * kb, kb), count * kb)]

    half_o = width_sg // 2
    items = [
        (u_in, rows_of(u_all), 1, 2),
        (v_in, rows_of(v_all), 2, 1),
        (o_in.at[pl.ds(0, half_o), :], cols_of(o_all, 0), 1, 2),
        (o_in.at[pl.ds(half_o, half_o), :], cols_of(o_all, 1), 2, 1),
    ]

    def own_copies(n):
        src, at, one, two = items[n]
        return [
            (has_up, remote(src, at(fs), sg_z.at[n, 0], sg_r.at[n, z, 0], up_dev)),
            (has_down, remote(src, at(fs), sg_z.at[n, 1], sg_r.at[n, z, 0], down_dev)),
            (None, remote(src, at(fs), sg_p.at[n], sg_r.at[n, z, 1], peers[one])),
            (None, remote(src, at(fs), sg_p.at[n], sg_l.at[n], peers[two])),
        ]

    def own_start(n):
        for pred, copy in own_copies(n):
            if pred is None:
                copy.start()
            else:
                start_if(pred, copy)

    def forward_to(b):
        going_up = b < z
        dev = jnp.where(going_up, up_dev, down_dev)
        return (going_up & has_up) | ((b > z) & has_down), dev, jnp.where(going_up, 0, 1)

    def column_copies(n, k):
        _, at, one, two = items[n]
        b = seq(k)
        idx = b * PLANE + p
        pred, dev, way = forward_to(b)
        ref = at(idx)
        return [
            (pred, remote(ref, ref, sg_z.at[n, way], sg_r.at[n, b, 0], dev)),
            (None, remote(ref, ref, sg_p.at[n], sg_r.at[n, b, 1], peers[one])),
            (None, remote(ref, ref, sg_p.at[n], sg_l.at[n], peers[two])),
        ]

    def column(n, k):
        copies = column_copies(n, k)
        copies[0][1].wait_recv()
        start_if(*copies[0])
        copies[1][1].start()
        copies[2][1].start()

    def beside(n, k):
        _, at, one, two = items[n]
        b = seq(k)
        ref = at(b * PLANE + inplane[one])
        remote(ref, ref, sg_p.at[n], sg_r.at[n, b, 1], peers[one]).wait_recv()
        remote(ref, ref, sg_p.at[n], sg_l.at[n], peers[two]).start()

    def gathered(n):
        ref = items[n][1](0, 2 * nz)
        remote(ref, ref, sg_p.at[n], sg_l.at[n], peers[1]).wait_recv()

    wides = [(gate_turned, gate_all), (up_turned, up_all), (down_in, down_all)]

    def quarter_copy(w, j):
        src, dst = wides[w]
        theirs = pl.ds(mult(inplane[j] * quarter, 16), quarter)
        mine = pl.ds(mult(fs * kb, kb), kb)
        return remote(src.at[theirs, :], dst.at[:, mine], a2_s.at[w], a2_r.at[w], peers[j])

    def quarters_all(w):
        ref = wides[w][1].at[:, pl.ds(0, (PLANE - 1) * kb)]
        return remote(ref, ref, a2_s.at[w], a2_r.at[w], peers[1])

    def quarters_start(w):
        for j in range(1, PLANE):
            quarter_copy(w, j).start()

    def block(w, b, h):
        cols = plane_cols // CUTS[w]
        return wides[w][1].at[:, pl.ds(mult(b * plane_cols + h * cols, cols), cols)]

    def z_recv(w, b, h):
        return z_r.at[sum(CUTS[:w]) * nz + b * CUTS[w] + h]

    def own_block_copies(w, h):
        ref, recv = block(w, z, h), z_recv(w, z, h)
        return [
            (has_up, remote(ref, ref, z_s.at[w, 0], recv, up_dev)),
            (has_down, remote(ref, ref, z_s.at[w, 1], recv, down_dev)),
        ]

    def own_block(w):
        quarters_all(w).wait_recv()
        for h in range(CUTS[w]):
            for pred, copy in own_block_copies(w, h):
                start_if(pred, copy)

    def pass_copy(w, k, h):
        b = seq(k)
        pred, dev, way = forward_to(b)
        ref = block(w, b, h)
        return pred, remote(ref, ref, z_s.at[w, way], z_recv(w, b, h), dev)

    def blocks_sent(ref_of, sems):
        for n in range(1, nz):
            ref = ref_of(n)
            up = remote(ref, ref, sems(0), sems(0), fs)
            down = remote(ref, ref, sems(1), sems(1), fs)
            pl.when(has_up & (z + 1 == n))(lambda: up.wait_send())
            pl.when(has_down & (nz - z == n))(lambda: down.wait_send())

    def pass_on(w, k, h):
        pred, copy = pass_copy(w, k, h)

        @pl.when(pred)
        def _():
            copy.wait_recv()
            copy.start()

    def need(w, k, h):
        pred, copy = pass_copy(w, k, h)
        pl.when(jnp.logical_not(pred))(lambda: copy.wait_recv())

    lane = lax.broadcasted_iota(jnp.int32, (depth, 128), 1)

    def put_stats(which, place, vals):
        one = jnp.sum(vals, axis=1, keepdims=True)
        two = jnp.sum(vals * vals, axis=1, keepdims=True)
        st_s[which, place, :] = jnp.where(lane == 0, one, two)

    def stats_copy(which):
        return remote(st_s.at[which], st_r.at[which], st_sem.at[which, 0], st_sem.at[which, 1], fs, oc)

    def normalize(which, place, vals, gain, count):
        both = st_s[which, place, :] + st_r[which, place, :]
        mean = both[:, 0:1] / count
        square = both[:, 1:2] / count
        return (vals - mean) * lax.rsqrt(square - mean * mean + EPS) * gain

    def loop(count, body):
        lax.fori_loop(0, count, lambda i, carry: (body(i), carry)[1], 0)

    def part(i):
        return pl.ds(mult(i * depth, depth), depth)

    tok_copy = remote(tok_in, tok_o, tok_sem.at[0], tok_sem.at[1], fs, oc)
    own_start(0)
    own_start(1)

    def turn(src, dst):
        def step(i):
            place = pl.ds(mult(i * kb, kb), kb)
            dst[place, :] = src[:, place].T

        loop(src.shape[1] // kb, step)

    loads[0].wait()
    turn(gate_own, gate_turned)
    quarters_start(0)
    own_start(2)
    own_start(3)
    tok_copy.start()
    for load in loads[1:]:
        load.wait()
    turn(up_own, up_turned)
    gate_all[:, own_rows] = gate_turned[own_quarter, :]
    up_all[:, own_rows] = up_turned[own_quarter, :]

    for n in (0, 1):
        column(n, 1)
    for n in (0, 1):
        column(n, 2)
    for n in (2, 3):
        column(n, 1)
    for n in (0, 1):
        column(n, 3)
    for n in (2, 3):
        column(n, 2)
    own_block(0)
    for k in (0, 1):
        for n in (0, 1):
            beside(n, k)
    for n in (2, 3):
        column(n, 3)
    pass_on(0, 1, 0)
    pass_on(0, 2, 0)
    for n in (0, 1):
        beside(n, 2)
    pass_on(0, 1, 1)
    pass_on(0, 2, 1)
    for n in (0, 1):
        beside(n, 3)
    quarters_start(1)
    for n in (2, 3):
        beside(n, 0)
    for n in (2, 3):
        beside(n, 1)
    pass_on(0, 3, 0)
    for n in (2, 3):
        beside(n, 2)

    tok_copy.wait_recv()
    wide = 256
    mine_k = pl.ds(mult(c * feats, feats), feats)
    their_k = pl.ds(mult(oc * feats, feats), feats)

    def branch(weight, into):
        def step(n):
            cols = pl.ds(mult(n * wide, wide), wide)
            acc = add_rows(tok[...], weight[mine_k, cols]) + add_rows(tok_o[...], weight[their_k, cols])
            into[:, cols] = jax.nn.gelu(acc)

        loop(width_sg // wide, step)

    gathered(0)
    branch(u_all, gated)
    gathered(1)
    branch(v_all, valued)
    for n in (2, 3):
        beside(n, 3)
    pass_on(0, 3, 1)
    loop(rows // depth, lambda i: put_stats(0, part(i), valued[part(i), :]))
    stats_copy(0).start()
    stats_copy(0).wait_recv()

    def norm_gate(i):
        vals = normalize(0, part(i), valued[part(i), :], sg_gain[...], 2 * width_sg)
        normed[part(i), :] = vals.astype(jnp.bfloat16)

    loop(rows // depth, norm_gate)
    groups, spread = spatial.shape[0], spatial.shape[1]
    row_at = lax.broadcasted_iota(jnp.int32, (spread, spread), 0)
    col_at = lax.broadcasted_iota(jnp.int32, (spread, spread), 1)
    group_dim = width_sg // groups

    def mix_block(n):
        place = pl.ds(mult(n * spread, spread), spread)
        for g in range(groups):
            cols = pl.ds(g * group_dim, group_dim)
            weight = jnp.where(col_at <= row_at, spatial[g], jnp.zeros_like(spatial[g]))
            shift_by = jnp.sum(jnp.where(col_at == row_at, bias[g : g + 1, :], 0.0), axis=1, keepdims=True)
            mixed = jnp.dot(weight, normed[place, cols], preferred_element_type=jnp.float32) + shift_by
            gated_out[place, cols] = (gated[place, cols] * mixed).astype(jnp.bfloat16)

    loop(rows // spread, mix_block)
    for n in (2, 3):
        gathered(n)

    def project_out(which, into):
        def step(n):
            cols = pl.ds(mult(which * feats + n * wide, wide), wide)
            to = pl.ds(mult(n * wide, wide), wide)
            into[:, to] = add_rows(gated_out[...], o_all[:, cols]).astype(jnp.bfloat16)

        loop(feats // wide, step)

    project_out(oc, terms_s)
    terms_copy = remote(terms_s, terms_r, terms_sem.at[0], terms_sem.at[1], fs, oc)
    terms_copy.start()
    project_out(c, terms_o)
    own_block(1)
    terms_copy.wait_recv()

    def add_mix(i):
        mix = terms_o[part(i), :].astype(jnp.float32) + terms_r[part(i), :].astype(jnp.float32)
        vals = ALPHA * tok[part(i), :].astype(jnp.float32) + mix.astype(jnp.bfloat16).astype(jnp.float32)
        resid[part(i), :] = vals
        put_stats(1, part(i), vals)

    loop(rows // depth, add_mix)
    stats_copy(1).start()
    stats_copy(1).wait_recv()
    mine_cols = pl.ds(mult(c * feats, feats), feats)
    their_cols = pl.ds(mult(oc * feats, feats), feats)

    def norm_first(i):
        vals = normalize(1, part(i), resid[part(i), :], gain_one[...], 2 * feats)
        vals = vals.astype(jnp.bfloat16)
        first_all[pl.ds(mult(p * rows + i * depth, depth), depth), mine_cols] = vals
        resid[part(i), :] = ALPHA * vals.astype(jnp.float32)

    loop(rows // depth, norm_first)

    def place_of(j):
        return (y + j // 2) % 2 * 2 + (x + j % 2) % 2

    def tokens_of(j, cols):
        return first_all.at[pl.ds(mult(place_of(j) * rows, rows), rows), cols]

    def swap_copy(j):
        ref = tokens_of(j, mine_cols)
        return remote(ref, ref, swap_s, swap_r.at[j], fs, oc)

    own_tokens = tokens_of(0, mine_cols)
    first_copies = [
        remote(own_tokens, own_tokens, first_s, first_r.at[j], peers[j]) for j in (1, 2)
    ]

    def corner_copy(j):
        start = mult(place_of(j) * rows + (j - 1) * (rows // 2), rows // 2)
        ref = first_all.at[pl.ds(start, rows // 2), mine_cols]
        return remote(ref, ref, first_s, first_r.at[j + 2], z * PLANE + place_of(PLANE - 1 - j))

    swap_copy(0).start()
    for copy in first_copies:
        copy.start()
    quarters_start(2)

    for k in range(1, nz):
        for h in range(CUTS[0]):
            need(0, k, h)

    tiles = [(t, min(wide, quarter - t)) for t in range(0, quarter, wide)]

    def across(left, weight, t, n):
        return lax.dot_general(
            left, weight[pl.ds(t, n), :], (((1,), (1,)), ((), ())), preferred_element_type=jnp.float32
        )

    def row_block(j):
        return pl.ds(mult(place_of(j) * rows, rows), rows)

    def gate_step(j):
        @pl.when((j == 1) | (j == 2))
        def _():
            ref = tokens_of(j, mine_cols)
            remote(ref, ref, first_s, first_r.at[j], fs, oc).wait_recv()
            corner_copy(j).start()

        @pl.when(j == PLANE - 1)
        def _():
            for half in (0, 1):
                start = mult(place_of(j) * rows + half * (rows // 2), rows // 2)
                ref = first_all.at[pl.ds(start, rows // 2), mine_cols]
                remote(ref, ref, first_s, first_r.at[half + 3], fs, oc).wait_recv()

        @pl.when(j > 0)
        def _():
            swap_copy(j).start()

        ref = tokens_of(j, their_cols)
        remote(ref, ref, swap_s, swap_r.at[j], fs, oc).wait_recv()
        left = row_block(j)
        for t, n in tiles:
            gate_acc[left, pl.ds(t, n)] = jax.nn.silu(across(first_all[left, :], gate_all, t, n))

        @pl.when(j == 0)
        def _():
            for h in range(CUTS[1]):
                pass_on(1, 1, h)
                pass_on(1, 2, h)

        @pl.when((j == 1) | (j == 2))
        def _():
            pass_on(1, 3, j - 1)

        pl.when(j == 2)(lambda: own_block(2))

    loop(PLANE, gate_step)
    for k in range(1, nz):
        for h in range(CUTS[1]):
            need(1, k, h)

    def up_step(j):
        left = row_block(j)
        for t, n in tiles:
            acc = gate_acc[left, pl.ds(t, n)] * across(first_all[left, :], up_all, t, n)
            hidden[left, pl.ds(t, n)] = acc.astype(jnp.bfloat16)

    terms_copy.wait_send()

    cut = CUTS[2]
    half_cols = plane_cols // cut
    steps = nz * cut
    per_core = steps // 2
    units = steps * PLANE
    early = cut * PLANE

    def unit(t):
        order = jnp.where(t < early, t // cut, (t - early) % PLANE)
        i = jnp.where(t < early, t % cut, cut + (t - early) // PLANE)
        j = jnp.where(order == 0, PLANE - 1, jnp.where(order == PLANE - 1, 0, order))
        inner = (i >= cut) & (i < 3 * cut) & has_up & has_down
        k = jnp.where(inner, 1 + i % 2, i // cut)
        h = jnp.where(inner, (i - cut) // 2, i % cut)
        at = seq(k) * cut + h
        return order, j, k, h, at

    def owned(at):
        return at // per_core == c, at % per_core

    def pair_copy(t):
        _, j, _, _, at = unit(t)
        ref = (owned(at)[1], row_block(j))
        return remote(p_s.at[ref], p_r.at[ref], d2_s, d2_r.at[owned(at)[1], j], fs, oc)

    def rows_copy(t):
        _, j, _, _, at = unit(t)
        q = owned(at)[1]
        pick = jnp.maximum(j - 1, 0)
        return remote(
            p_r.at[q, row_block(j)],
            r_r.at[pick, q],
            rs_s,
            rs_r,
            z * PLANE + place_of(j),
        )

    def finish(t):
        _, j, _, _, at = unit(t)
        mine, q = owned(at)

        @pl.when(mine)
        def _():
            pair_copy(t).wait_recv()
            place = row_block(j)
            both = p_own[t % SLOTS].astype(jnp.float32) + p_r[q, place, :].astype(jnp.float32)
            p_r[q, place, :] = both.astype(jnp.bfloat16)
            pl.when(j > 0)(lambda: rows_copy(t).start())

    def unit_step(t):
        order, j, k, h, at = unit(t)
        mine, q = owned(at)
        pl.when((t < early) & (t % cut == 0))(lambda: up_step(j))

        @pl.when((t % cut == 0) & (t > 0) & (t <= early))
        def _():
            pass_on(2, 1, t // cut - 1)
            pass_on(2, 2, t // cut - 1)

        late = (t - early) // PLANE
        third = (t >= early + 3 * PLANE) & (late % 2 == 1) & (late < 2 * cut + 2)

        @pl.when(third & (order == 0))
        def _():
            pass_on(2, 3, (late - 3) // 2)

        pl.when((k > 0) & (order == 0))(lambda: need(2, k, h))

        from_cols = pl.ds(mult(at * half_cols, half_cols), half_cols)
        place = row_block(j)
        made = add_rows(hidden[place, :], down_all[:, from_cols]).astype(jnp.bfloat16)

        @pl.when(mine)
        def _():
            p_own[t % SLOTS] = made

        @pl.when(jnp.logical_not(mine))
        def _():
            p_s[q, place, :] = made
            pair_copy(t).start()

        pl.when(t >= LAG)(lambda: finish(t - LAG))

    loop(units, unit_step)
    loop(LAG, lambda i: finish(units - LAG + i))

    remote(r_r, r_r, rs_s, rs_r, peers[1]).wait_recv()

    def add_ffn(i):
        for q in range(per_core):
            cols = pl.ds(q * half_cols, half_cols)
            total = p_r[q, pl.ds(mult(p * rows + i * depth, depth), depth), :].astype(jnp.float32)
            for j in range(1, PLANE):
                total = total + r_r[j - 1, q, part(i), :].astype(jnp.float32)
            resid[part(i), cols] = resid[part(i), cols] + total.astype(jnp.bfloat16).astype(jnp.float32)
        put_stats(2, part(i), resid[part(i), :])

    loop(rows // depth, add_ffn)
    stats_copy(2).start()

    tok_copy.wait_send()
    stats_copy(0).wait_send()
    stats_copy(1).wait_send()
    ref = first_all.at[pl.ds(0, (PLANE - 1) * rows), pl.ds(0, feats)]
    remote(ref, ref, first_s, first_s, peers[1]).wait_send()
    ref = first_all.at[pl.ds(0, PLANE * rows), pl.ds(0, feats)]
    remote(ref, ref, swap_s, swap_s, fs, oc).wait_send()
    for n in range(len(items)):
        ref = items[n][1](0, 3 * nz)
        remote(ref, ref, sg_p.at[n], sg_l.at[n], peers[1]).wait_send()
        blocks_sent(lambda count: items[n][1](0, count), lambda way: sg_z.at[n, way])
    for w in range(len(wides)):
        quarters_all(w).wait_send()
        blocks_sent(lambda count: wides[w][1].at[:, pl.ds(0, count * plane_cols)], lambda way: z_s.at[w, way])
    remote(p_s, p_r, d2_s, d2_s, fs, oc).wait_send()
    remote(r_r, r_r, rs_s, rs_r, peers[1]).wait_send()
    stats_copy(2).wait_recv()

    def norm_last(i):
        vals = normalize(2, part(i), resid[part(i), :], gain_two[...], 2 * feats)
        out[part(i), :] = vals.astype(out.dtype)

    loop(rows // depth, norm_last)
    stats_copy(2).wait_send()


def in_one_kernel(*args):
    (tokens, u_weight, v_weight, sg_gain, spatial, bias, out_weight, gain_one, gate, up, down, gain_two) = args
    nz = lax.axis_size("fs") // PLANE
    rows, feats = tokens.shape
    width_sg = u_weight.shape[1]
    quarter = down.shape[0] // PLANE
    wide = 2 * feats
    plane_rows = PLANE * rows
    bf16, f32 = jnp.bfloat16, jnp.float32
    vmem, dma = pltpu.VMEM, pltpu.SemaphoreType.DMA
    steps = nz * CUTS[2]
    half_cols = wide // steps
    scratch = [
        vmem((rows, feats), bf16),
        vmem((1, width_sg), f32),
        vmem(spatial.shape, bf16),
        vmem(bias.shape, f32),
        vmem((1, feats), f32),
        vmem((1, feats), f32),
        vmem(gate.shape, bf16),
        vmem(gate.shape, bf16),
        vmem(gate.shape[::-1], bf16),
        vmem(gate.shape[::-1], bf16),
        vmem((rows, feats), bf16),
        vmem((wide, width_sg), bf16),
        vmem((wide, width_sg), bf16),
        vmem((width_sg, wide), bf16),
        vmem((quarter, wide), bf16),
        vmem((quarter, wide), bf16),
        vmem((quarter, wide), bf16),
        vmem((rows, width_sg), f32),
        vmem((rows, width_sg), f32),
        vmem((rows, width_sg), bf16),
        vmem((rows, width_sg), bf16),
        vmem((3, rows, 128), f32),
        vmem((3, rows, 128), f32),
        vmem((rows, feats), bf16),
        vmem((rows, feats), bf16),
        vmem((rows, feats), bf16),
        vmem((rows, feats), f32),
        vmem((plane_rows, wide), bf16),
        vmem((plane_rows, quarter), bf16),
        vmem((plane_rows, quarter), f32),
        vmem((steps // 2, plane_rows, half_cols), bf16),
        vmem((steps // 2, plane_rows, half_cols), bf16),
        vmem((SLOTS, rows, half_cols), bf16),
        vmem((PLANE - 1, steps // 2, rows, half_cols), bf16),
        dma((12,)),
        dma((4, nz, 2)),
        dma((4,)),
        dma((4, 2)),
        dma((4,)),
        dma((3,)),
        dma((3,)),
        dma((3, 2)),
        dma((sum(CUTS) * nz,)),
        dma((2,)),
        dma((3, 2)),
        dma((2,)),
        dma(()),
        dma((PLANE + 1,)),
        dma(()),
        dma((PLANE,)),
        dma(()),
        dma((steps // 2, PLANE)),
        dma(()),
        dma(()),
    ]
    spec = pl.BlockSpec(memory_space=pltpu.VMEM)
    return pl.pallas_call(
        functools.partial(layer_kernel, (nz,)),
        name="layer",
        out_shape=jax.ShapeDtypeStruct((rows, feats), tokens.dtype),
        in_specs=[pl.BlockSpec(memory_space=pl.ANY)] * 12,
        out_specs=spec,
        scratch_shapes=scratch,
        compiler_params=pltpu.CompilerParams(
            collective_id=0, has_side_effects=True, vmem_limit_bytes=67_043_328
        ),
    )(
        tokens,
        u_weight,
        v_weight,
        sg_gain[None],
        spatial,
        bias,
        out_weight,
        gain_one[None],
        gate,
        up,
        down,
        gain_two[None],
    )


def fits(tokens, u_weight, gate_weight, spatial_weight):
    if lax.axis_size("tp") != 2 or lax.axis_size("fs") != 4 * PLANE:
        return False
    quarter = gate_weight.shape[1] % PLANE == 0 and gate_weight.shape[1] // PLANE % 16 == 0
    lanes = u_weight.shape[0] % 128 == 0 and u_weight.shape[1] % 256 == 0
    return quarter and lanes and tokens.shape[0] % (PLANE * spatial_weight.shape[1]) == 0


def choose(*args):
    if fits(args[0], args[1], args[8], args[4]):
        return in_one_kernel(*args)
    return on_device(*args)


def solution(mesh):
    return jax.shard_map(
        choose,
        mesh=mesh,
        in_specs=(
            P("fs", "tp"),
            P("fs", "tp"),
            P("fs", "tp"),
            P("tp"),
            P("tp", None, None),
            P("tp", None),
            P("tp", "fs"),
            P("tp"),
            P("fs", "tp"),
            P("fs", "tp"),
            P("tp", "fs"),
            P("tp"),
        ),
        out_specs=P("fs", "tp"),
        check_vma=False,
    )
```

```python
import functools

import jax
import jax.numpy as jnp
from jax import lax
from jax.experimental import pallas as pl
from jax.experimental.pallas import tpu as pltpu
from jax.sharding import PartitionSpec as P

EPS = 1e-05
ALPHA = 2.0**0.25


def add_rows(left, piece):
    return jnp.dot(left, piece, preferred_element_type=jnp.float32)


def scaled_rows(vals, sums, gain, count):
    mean = sums[0][:, None] / count
    square = sums[1][:, None] / count
    return (vals - mean) * lax.rsqrt(square - mean * mean + EPS) * gain[None, :]


def chip_sizes(count):
    across = 2 if count % 2 == 0 else 1
    down = 2 if (count // across) % 2 == 0 else 1
    return count // (across * down), down, across


def shift(value, sizes, axis, step=1):
    count = sizes[0] * sizes[1] * sizes[2]
    stride = sizes[1] * sizes[2] if axis == 0 else (sizes[2] if axis == 1 else 1)
    pairs = []
    for source in range(count):
        place = (source // stride) % sizes[axis]
        pairs.append((source, source + ((place + step) % sizes[axis] - place) * stride))
    return lax.ppermute(value, "fs", pairs)


def around(value, sizes, axis):
    if sizes[axis] == 4:
        near = shift(value, sizes, axis, 1)
        last = shift(value, sizes, axis, -1)
        return [value, near, shift(near, sizes, axis, 1), last]
    pieces = [value]
    for _ in range(sizes[axis] - 1):
        pieces.append(shift(pieces[-1], sizes, axis))
    return pieces


def ring(value, sizes, axis, place):
    return in_order(around(value, sizes, axis), place)


def other_core(value):
    return lax.ppermute(value, "tp", [(0, 1), (1, 0)])


def all_features(value):
    if lax.axis_size("tp") != 2:
        return lax.all_gather(value, "tp", axis=1, tiled=True)
    return jnp.concatenate(in_two(value, other_core(value), lax.axis_index("tp")), axis=1)


def in_two(mine, other, place):
    return [jnp.where(place == 0, mine, other), jnp.where(place == 0, other, mine)]


def sum_shares(terms):
    if lax.axis_size("tp") != 2:
        return lax.psum_scatter(terms, "tp", scatter_dimension=1, tiled=True)
    core = lax.axis_index("tp")
    half = terms.shape[1] // 2
    mine = lax.dynamic_slice_in_dim(terms, core * half, half, 1)
    sent = lax.dynamic_slice_in_dim(terms, (1 - core) * half, half, 1)
    return (mine.astype(jnp.float32) + other_core(sent).astype(jnp.float32)).astype(jnp.bfloat16)


def in_order(pieces, place):
    count = len(pieces)
    if count == 1:
        return pieces[0][None]
    held = jnp.zeros((count,) + pieces[0].shape, pieces[0].dtype)
    for step, piece in enumerate(pieces):
        start = lax.rem(place - step + count, count)
        held = lax.dynamic_update_slice_in_dim(held, piece[None], start, 0)
    return held


def gather_all(piece, sizes, places, order):
    held = piece
    for axis in order:
        held = ring(held, sizes, axis, places[axis])
    back = [order[::-1].index(axis) for axis in range(3)]
    rest = [3 + i for i in range(piece.ndim)]
    return jnp.transpose(held, back + rest)


def after(value, *others):
    return lax.optimization_barrier((value,) + others)[0]


def share_pieces(weight, dim, sizes, places, level, marks):
    across = sizes[2]
    width = weight.shape[dim] // across
    if across == 2:
        mine = lax.dynamic_slice_in_dim(weight, places[2] * width, width, dim)
        other = lax.dynamic_slice_in_dim(weight, (1 - places[2]) * width, width, dim)
        block = jnp.stack(in_two(mine, shift(other, sizes, 2), places[2]))
    else:
        block = weight[None]
    if sizes[0] != 4 or sizes[1] != 2:
        first = around(block, sizes, 0)
        return [[piece] if sizes[1] == 1 else [piece, shift(piece, sizes, 1)] for piece in first]
    if marks[0] is not None:
        block = after(block, marks[0])
    near, last = shift(block, sizes, 0, 1), shift(block, sizes, 0, -1)
    beside = shift(block if marks[0] is None else after(block, marks[1]), sizes, 1)
    near, last = after(near, marks[1]), after(last, marks[1])
    far = shift(near, sizes, 0)
    near_beside, last_beside = shift(near, sizes, 1), shift(last, sizes, 1)
    if level:
        far_beside = shift(after(near_beside, marks[2]), sizes, 0)
    else:
        far = after(far, marks[2])
        far_beside = shift(far, sizes, 1)
    return [[block, beside], [near, near_beside], [far, far_beside], [last, last_beside]]


def place_pieces(pieces, places):
    shape = pieces[0][0].shape
    count, down = len(pieces), len(pieces[0])
    held = jnp.zeros((count, down) + shape, pieces[0][0].dtype)
    for step, pair in enumerate(pieces):
        start = lax.rem(places[0] - step + count, count)
        for turn, piece in enumerate(pair):
            spot = places[1] if turn == 0 else 1 - places[1]
            held = lax.dynamic_update_slice(held, piece[None, None], [start, spot] + [0] * len(shape))
    return held


def on_device(
    tokens,
    u_weight,
    v_weight,
    sg_gain,
    spatial_weight,
    spatial_bias,
    out_weight,
    gain_one,
    gate_weight,
    up_weight,
    down_weight,
    gain_two,
):
    parts = lax.axis_size("tp")
    sizes = chip_sizes(lax.axis_size("fs"))
    index = lax.axis_index("fs")
    places = (index // (sizes[1] * sizes[2]), (index // sizes[2]) % sizes[1], index % sizes[2])
    whole = all_features(tokens)
    rows = whole.shape[0]
    width_sg = u_weight.shape[1]

    def add_one(piece):
        return add_rows(whole, piece)

    pre_u = add_one(gather_all(u_weight, sizes, places, [0, 1, 2]).reshape(-1, width_sg))
    pre_v = add_one(gather_all(v_weight, sizes, places, [0, 2, 1]).reshape(-1, width_sg))
    gated = jax.nn.gelu(pre_u)
    valued = jax.nn.gelu(pre_v)
    stats = lax.psum((jnp.sum(valued, axis=1), jnp.sum(valued * valued, axis=1)), "tp")
    normed = scaled_rows(valued, stats, sg_gain, width_sg * parts).astype(jnp.bfloat16)
    groups_here = spatial_weight.shape[0]
    block = spatial_weight.shape[1]
    group_width = width_sg // groups_here
    shaped = normed.reshape(rows // block, block, groups_here, group_width)
    lower = jnp.tril(jnp.ones((block, block), jnp.bool_))
    masked = jnp.where(lower[None], spatial_weight, jnp.zeros_like(spatial_weight))
    mixed = jnp.einsum("gij,njgd->nigd", masked, shaped, preferred_element_type=jnp.float32)
    mixed = mixed + spatial_bias.T[None, :, :, None]
    gated_out = (gated * mixed.reshape(rows, width_sg)).astype(jnp.bfloat16)
    out_all = gather_all(out_weight, sizes, places, [0, 1, 2])
    out_all = out_all.reshape((-1,) + out_weight.shape)
    terms = jnp.einsum("tk,nkc->tnc", gated_out, out_all, preferred_element_type=jnp.float32)
    mix = sum_shares(terms.reshape(rows, -1).astype(jnp.bfloat16))
    resid = ALPHA * tokens.astype(jnp.float32) + mix.astype(jnp.float32)
    first_sums = lax.psum((jnp.sum(resid, axis=1), jnp.sum(resid * resid, axis=1)), "tp")
    first = scaled_rows(resid, first_sums, gain_one, resid.shape[1] * parts).astype(jnp.bfloat16)
    gate_pieces = share_pieces(gate_weight, 1, sizes, places, False, (None, normed, mix))
    up_pieces = share_pieces(up_weight, 1, sizes, places, True, (None, normed, mix))
    down_pieces = share_pieces(down_weight, 0, sizes, places, False, (normed, first, first))
    gate_all = place_pieces(gate_pieces, places)
    gate_all = gate_all.reshape(-1, gate_all.shape[-1])
    up_all = place_pieces(up_pieces, places)
    up_all = up_all.reshape(-1, up_all.shape[-1])
    def feed(part):
        whole_part = all_features(part)
        gate = add_rows(whole_part, gate_all)
        upper = add_rows(whole_part, up_all)
        return (jax.nn.silu(gate) * upper).astype(jnp.bfloat16)

    two = sizes[2] == 2
    if two:
        there = feed(shift(first, sizes, 2))
        here = feed(first)
        down_pieces = [[pair[0]] + [after(piece, there, here) for piece in pair[1:]] for pair in down_pieces]
    else:
        here = feed(first)
    down_all = place_pieces(down_pieces, places)
    down_all = down_all.reshape((-1,) + down_all.shape[-2:])

    def project(hidden):
        made = jnp.einsum("tf,nfc->tnc", hidden, down_all, preferred_element_type=jnp.float32)
        return sum_shares(made.reshape(rows, -1).astype(jnp.bfloat16))

    if two:
        there = project(there)
        sent = shift(there, sizes, 2)
        ffn = project(after(here, there)).astype(jnp.float32) + sent.astype(jnp.float32)
    else:
        ffn = project(here).astype(jnp.float32)
    second = ALPHA * first.astype(jnp.float32) + ffn.astype(jnp.float32)
    last_sums = lax.psum((jnp.sum(second, axis=1), jnp.sum(second * second, axis=1)), "tp")
    return scaled_rows(second, last_sums, gain_two, second.shape[1] * parts).astype(jnp.bfloat16)


MESH = pl.DeviceIdType.MESH
PLANE = 4
CUTS = (2, 2, 4)
LAG = 3
RELAY_LAGS = (6, 12)
SLOTS = 4


def layer_kernel(
    sizes,
    tok_in,
    u_in,
    v_in,
    sg_gain_in,
    spatial_in,
    bias_in,
    o_in,
    gain_one_in,
    gate_in,
    up_in,
    down_in,
    gain_two_in,
    out,
    tok,
    sg_gain,
    spatial,
    bias,
    gain_one,
    gain_two,
    gate_own,
    up_own,
    gate_turned,
    up_turned,
    tok_o,
    u_all,
    v_all,
    o_all,
    gate_all,
    up_all,
    down_all,
    gated,
    valued,
    normed,
    gated_out,
    st_s,
    st_r,
    terms_s,
    terms_o,
    terms_r,
    resid,
    first_all,
    hidden,
    gate_acc,
    p_s,
    p_r,
    p_own,
    r_r,
    in_sem,
    sg_r,
    sg_l,
    sg_z,
    sg_p,
    a2_s,
    a2_r,
    z_s,
    z_r,
    tok_sem,
    st_sem,
    terms_sem,
    first_s,
    first_r,
    swap_s,
    swap_r,
    d2_s,
    d2_r,
    rs_s,
    rs_r,
):
    nz = sizes[0]
    fs, c = lax.axis_index("fs"), lax.axis_index("tp")
    oc = 1 - c
    z, p = fs // PLANE, fs % PLANE
    y, x = p // 2, p % 2
    peers = [z * PLANE + (y + j // 2) % 2 * 2 + (x + j % 2) % 2 for j in range(PLANE)]
    inplane = [(y + j // 2) % 2 * 2 + (x + j % 2) % 2 for j in range(PLANE)]
    has_up, has_down = z < nz - 1, z > 0
    up_dev = jnp.where(has_up, fs + PLANE, fs - PLANE)
    down_dev = jnp.where(has_down, fs - PLANE, fs + PLANE)
    rows, feats = tok.shape
    kb, width_sg = u_in.shape
    depth = rows // PLANE
    quarter = hidden.shape[1]
    plane_cols = PLANE * kb

    def mult(value, by):
        return pl.multiple_of(value, by)

    def seq(k):
        swapped = jnp.where(k < 2, 1 - k, k)
        return jnp.where(z == 0, k, jnp.where(z == 1, swapped, jnp.where(z == 2, nz - 1 - swapped, nz - 1 - k)))

    def remote(src, dst, send, recv, dev, core=None):
        where_to = (dev, c if core is None else core)
        return pltpu.make_async_remote_copy(
            src_ref=src, dst_ref=dst, send_sem=send, recv_sem=recv, device_id=where_to, device_id_type=MESH
        )

    def start_if(pred, copy):
        pl.when(pred)(lambda: copy.start())

    def sent_if(pred, copy):
        pl.when(pred)(lambda: copy.wait_send())

    own_rows = pl.ds(mult(fs * kb, kb), kb)
    own_quarter = pl.ds(mult(p * quarter, 16), quarter)
    loads = [
        (gate_in, gate_own),
        (up_in, up_own),
        (u_in, u_all.at[own_rows, :]),
        (v_in, v_all.at[own_rows, :]),
        (o_in, o_all.at[:, own_rows]),
        (down_in.at[own_quarter, :], down_all.at[:, own_rows]),
        (tok_in, tok),
        (sg_gain_in, sg_gain),
        (spatial_in, spatial),
        (bias_in, bias),
        (gain_one_in, gain_one),
        (gain_two_in, gain_two),
    ]
    loads = [pltpu.make_async_copy(src, dst, in_sem.at[i]) for i, (src, dst) in enumerate(loads)]
    for load in loads:
        load.start()
    barrier = pltpu.get_barrier_semaphore()
    for dev, core in [(fs, oc)] + [(peers[j], c) for j in range(1, PLANE)]:
        pl.semaphore_signal(barrier, inc=1, device_id=(dev, core), device_id_type=MESH)
    for pred, dev in [(has_up, up_dev), (has_down, down_dev)]:
        @pl.when(pred)
        def _():
            pl.semaphore_signal(barrier, inc=1, device_id=(dev, c), device_id_type=MESH)
    pl.semaphore_wait(barrier, PLANE + jnp.where(has_up, 1, 0) + jnp.where(has_down, 1, 0))

    def rows_of(ref):
        return lambda i, count=1: ref.at[pl.ds(mult(i * kb, kb), count * kb), :]

    def cols_of(ref, part):
        height = width_sg // 2
        return lambda i, count=1: ref.at[pl.ds(part * height, height), pl.ds(mult(i * kb, kb), count * kb)]

    half_o = width_sg // 2
    items = [
        (u_in, rows_of(u_all), 1, 2),
        (v_in, rows_of(v_all), 2, 1),
        (o_in.at[pl.ds(0, half_o), :], cols_of(o_all, 0), 1, 2),
        (o_in.at[pl.ds(half_o, half_o), :], cols_of(o_all, 1), 2, 1),
    ]

    def own_copies(n):
        src, at, one, two = items[n]
        return [
            (has_up, remote(src, at(fs), sg_z.at[n, 0], sg_r.at[n, z, 0], up_dev)),
            (has_down, remote(src, at(fs), sg_z.at[n, 1], sg_r.at[n, z, 0], down_dev)),
            (None, remote(src, at(fs), sg_p.at[n], sg_r.at[n, z, 1], peers[one])),
            (None, remote(src, at(fs), sg_p.at[n], sg_l.at[n], peers[two])),
        ]

    def own_start(n):
        for pred, copy in own_copies(n):
            if pred is None:
                copy.start()
            else:
                start_if(pred, copy)

    def forward_to(b):
        going_up = b < z
        dev = jnp.where(going_up, up_dev, down_dev)
        return (going_up & has_up) | ((b > z) & has_down), dev, jnp.where(going_up, 0, 1)

    def column_copies(n, k):
        _, at, one, two = items[n]
        b = seq(k)
        idx = b * PLANE + p
        pred, dev, way = forward_to(b)
        ref = at(idx)
        return [
            (pred, remote(ref, ref, sg_z.at[n, way], sg_r.at[n, b, 0], dev)),
            (None, remote(ref, ref, sg_p.at[n], sg_r.at[n, b, 1], peers[one])),
            (None, remote(ref, ref, sg_p.at[n], sg_l.at[n], peers[two])),
        ]

    def column(n, k):
        copies = column_copies(n, k)
        copies[0][1].wait_recv()
        start_if(*copies[0])
        copies[1][1].start()
        copies[2][1].start()

    def beside(n, k):
        _, at, one, two = items[n]
        b = seq(k)
        ref = at(b * PLANE + inplane[one])
        remote(ref, ref, sg_p.at[n], sg_r.at[n, b, 1], peers[one]).wait_recv()
        remote(ref, ref, sg_p.at[n], sg_l.at[n], peers[two]).start()

    def gathered(n):
        ref = items[n][1](0, 2 * nz)
        remote(ref, ref, sg_p.at[n], sg_l.at[n], peers[1]).wait_recv()

    wides = [(gate_turned, gate_all), (up_turned, up_all), (down_in, down_all)]

    def quarter_copy(w, j):
        src, dst = wides[w]
        theirs = pl.ds(mult(inplane[j] * quarter, 16), quarter)
        mine = pl.ds(mult(fs * kb, kb), kb)
        return remote(src.at[theirs, :], dst.at[:, mine], a2_s.at[w], a2_r.at[w], peers[j])

    def quarters_all(w):
        ref = wides[w][1].at[:, pl.ds(0, (PLANE - 1) * kb)]
        return remote(ref, ref, a2_s.at[w], a2_r.at[w], peers[1])

    def quarters_start(w):
        for j in range(1, PLANE):
            quarter_copy(w, j).start()

    def block(w, b, h):
        cols = plane_cols // CUTS[w]
        return wides[w][1].at[:, pl.ds(mult(b * plane_cols + h * cols, cols), cols)]

    def z_recv(w, b, h):
        return z_r.at[sum(CUTS[:w]) * nz + b * CUTS[w] + h]

    def own_block_copies(w, h):
        ref, recv = block(w, z, h), z_recv(w, z, h)
        return [
            (has_up, remote(ref, ref, z_s.at[w, 0], recv, up_dev)),
            (has_down, remote(ref, ref, z_s.at[w, 1], recv, down_dev)),
        ]

    def own_block(w):
        quarters_all(w).wait_recv()
        for h in range(CUTS[w]):
            for pred, copy in own_block_copies(w, h):
                start_if(pred, copy)

    def pass_copy(w, k, h):
        b = seq(k)
        pred, dev, way = forward_to(b)
        ref = block(w, b, h)
        return pred, remote(ref, ref, z_s.at[w, way], z_recv(w, b, h), dev)

    def blocks_sent(ref_of, sems):
        for n in range(1, nz):
            ref = ref_of(n)
            up = remote(ref, ref, sems(0), sems(0), fs)
            down = remote(ref, ref, sems(1), sems(1), fs)
            pl.when(has_up & (z + 1 == n))(lambda: up.wait_send())
            pl.when(has_down & (nz - z == n))(lambda: down.wait_send())

    def pass_on(w, k, h):
        pred, copy = pass_copy(w, k, h)

        @pl.when(pred)
        def _():
            copy.wait_recv()
            copy.start()

    def need(w, k, h):
        pred, copy = pass_copy(w, k, h)
        pl.when(jnp.logical_not(pred))(lambda: copy.wait_recv())

    lane = lax.broadcasted_iota(jnp.int32, (depth, 128), 1)

    def put_stats(which, place, vals):
        one = jnp.sum(vals, axis=1, keepdims=True)
        two = jnp.sum(vals * vals, axis=1, keepdims=True)
        st_s[which, place, :] = jnp.where(lane == 0, one, two)

    def stats_copy(which):
        return remote(st_s.at[which], st_r.at[which], st_sem.at[which, 0], st_sem.at[which, 1], fs, oc)

    def normalize(which, place, vals, gain, count):
        both = st_s[which, place, :] + st_r[which, place, :]
        mean = both[:, 0:1] / count
        square = both[:, 1:2] / count
        return (vals - mean) * lax.rsqrt(square - mean * mean + EPS) * gain

    def loop(count, body):
        lax.fori_loop(0, count, lambda i, carry: (body(i), carry)[1], 0)

    def part(i):
        return pl.ds(mult(i * depth, depth), depth)

    tok_copy = remote(tok_in, tok_o, tok_sem.at[0], tok_sem.at[1], fs, oc)
    own_start(0)
    own_start(1)

    def turn(src, dst):
        def step(i):
            place = pl.ds(mult(i * kb, kb), kb)
            dst[place, :] = src[:, place].T

        loop(src.shape[1] // kb, step)

    loads[0].wait()
    turn(gate_own, gate_turned)
    quarters_start(0)
    own_start(2)
    own_start(3)
    tok_copy.start()
    for load in loads[1:]:
        load.wait()
    turn(up_own, up_turned)
    gate_all[:, own_rows] = gate_turned[own_quarter, :]
    up_all[:, own_rows] = up_turned[own_quarter, :]

    for n in (0, 1):
        column(n, 1)
    for n in (0, 1):
        column(n, 2)
    for n in (2, 3):
        column(n, 1)
    for n in (0, 1):
        column(n, 3)
    for n in (2, 3):
        column(n, 2)
    own_block(0)
    for k in (0, 1):
        for n in (0, 1):
            beside(n, k)
    for n in (2, 3):
        column(n, 3)
    pass_on(0, 1, 0)
    pass_on(0, 2, 0)
    for n in (0, 1):
        beside(n, 2)
    pass_on(0, 1, 1)
    pass_on(0, 2, 1)
    for n in (0, 1):
        beside(n, 3)
    quarters_start(1)
    for n in (2, 3):
        beside(n, 0)
    for n in (2, 3):
        beside(n, 1)
    pass_on(0, 3, 0)
    for n in (2, 3):
        beside(n, 2)

    tok_copy.wait_recv()
    wide = 256
    mine_k = pl.ds(mult(c * feats, feats), feats)
    their_k = pl.ds(mult(oc * feats, feats), feats)

    def branch(weight, into):
        def step(n):
            cols = pl.ds(mult(n * wide, wide), wide)
            acc = add_rows(tok[...], weight[mine_k, cols]) + add_rows(tok_o[...], weight[their_k, cols])
            into[:, cols] = jax.nn.gelu(acc)

        loop(width_sg // wide, step)

    gathered(0)
    branch(u_all, gated)
    gathered(1)
    branch(v_all, valued)
    for n in (2, 3):
        beside(n, 3)
    pass_on(0, 3, 1)
    loop(rows // depth, lambda i: put_stats(0, part(i), valued[part(i), :]))
    stats_copy(0).start()
    stats_copy(0).wait_recv()

    def norm_gate(i):
        vals = normalize(0, part(i), valued[part(i), :], sg_gain[...], 2 * width_sg)
        normed[part(i), :] = vals.astype(jnp.bfloat16)

    loop(rows // depth, norm_gate)
    groups, spread = spatial.shape[0], spatial.shape[1]
    row_at = lax.broadcasted_iota(jnp.int32, (spread, spread), 0)
    col_at = lax.broadcasted_iota(jnp.int32, (spread, spread), 1)
    group_dim = width_sg // groups

    def mix_block(n):
        place = pl.ds(mult(n * spread, spread), spread)
        for g in range(groups):
            cols = pl.ds(g * group_dim, group_dim)
            weight = jnp.where(col_at <= row_at, spatial[g], jnp.zeros_like(spatial[g]))
            shift_by = jnp.sum(jnp.where(col_at == row_at, bias[g : g + 1, :], 0.0), axis=1, keepdims=True)
            mixed = jnp.dot(weight, normed[place, cols], preferred_element_type=jnp.float32) + shift_by
            gated_out[place, cols] = (gated[place, cols] * mixed).astype(jnp.bfloat16)

    loop(rows // spread, mix_block)
    for n in (2, 3):
        gathered(n)

    def project_out(which, into):
        def step(n):
            cols = pl.ds(mult(which * feats + n * wide, wide), wide)
            to = pl.ds(mult(n * wide, wide), wide)
            into[:, to] = add_rows(gated_out[...], o_all[:, cols]).astype(jnp.bfloat16)

        loop(feats // wide, step)

    project_out(oc, terms_s)
    terms_copy = remote(terms_s, terms_r, terms_sem.at[0], terms_sem.at[1], fs, oc)
    terms_copy.start()
    project_out(c, terms_o)
    own_block(1)
    terms_copy.wait_recv()

    def add_mix(i):
        mix = terms_o[part(i), :].astype(jnp.float32) + terms_r[part(i), :].astype(jnp.float32)
        vals = ALPHA * tok[part(i), :].astype(jnp.float32) + mix.astype(jnp.bfloat16).astype(jnp.float32)
        resid[part(i), :] = vals
        put_stats(1, part(i), vals)

    loop(rows // depth, add_mix)
    stats_copy(1).start()
    stats_copy(1).wait_recv()
    mine_cols = pl.ds(mult(c * feats, feats), feats)
    their_cols = pl.ds(mult(oc * feats, feats), feats)

    def norm_first(i):
        vals = normalize(1, part(i), resid[part(i), :], gain_one[...], 2 * feats)
        vals = vals.astype(jnp.bfloat16)
        first_all[pl.ds(mult(p * rows + i * depth, depth), depth), mine_cols] = vals
        resid[part(i), :] = ALPHA * vals.astype(jnp.float32)

    loop(rows // depth, norm_first)

    def place_of(j):
        return (y + j // 2) % 2 * 2 + (x + j % 2) % 2

    def tokens_of(j, cols):
        return first_all.at[pl.ds(mult(place_of(j) * rows, rows), rows), cols]

    def swap_copy(j):
        ref = tokens_of(j, mine_cols)
        return remote(ref, ref, swap_s, swap_r.at[j], fs, oc)

    own_tokens = tokens_of(0, mine_cols)
    first_copies = [
        remote(own_tokens, own_tokens, first_s, first_r.at[j], peers[j]) for j in (1, 2)
    ]

    def corner_copy(j):
        start = mult(place_of(j) * rows + (j - 1) * (rows // 2), rows // 2)
        ref = first_all.at[pl.ds(start, rows // 2), mine_cols]
        return remote(ref, ref, first_s, first_r.at[j + 2], z * PLANE + place_of(PLANE - 1 - j))

    swap_copy(0).start()
    for copy in first_copies:
        copy.start()
    quarters_start(2)

    for k in range(1, nz):
        for h in range(CUTS[0]):
            need(0, k, h)

    tiles = [(t, min(wide, quarter - t)) for t in range(0, quarter, wide)]

    def across(left, weight, t, n):
        return lax.dot_general(
            left, weight[pl.ds(t, n), :], (((1,), (1,)), ((), ())), preferred_element_type=jnp.float32
        )

    def row_block(j):
        return pl.ds(mult(place_of(j) * rows, rows), rows)

    def gate_step(j):
        @pl.when((j == 1) | (j == 2))
        def _():
            ref = tokens_of(j, mine_cols)
            remote(ref, ref, first_s, first_r.at[j], fs, oc).wait_recv()
            corner_copy(j).start()

        @pl.when(j == PLANE - 1)
        def _():
            for half in (0, 1):
                start = mult(place_of(j) * rows + half * (rows // 2), rows // 2)
                ref = first_all.at[pl.ds(start, rows // 2), mine_cols]
                remote(ref, ref, first_s, first_r.at[half + 3], fs, oc).wait_recv()

        @pl.when(j > 0)
        def _():
            swap_copy(j).start()

        ref = tokens_of(j, their_cols)
        remote(ref, ref, swap_s, swap_r.at[j], fs, oc).wait_recv()
        left = row_block(j)
        for t, n in tiles:
            gate_acc[left, pl.ds(t, n)] = jax.nn.silu(across(first_all[left, :], gate_all, t, n))

        @pl.when(j == 0)
        def _():
            for h in range(CUTS[1]):
                pass_on(1, 1, h)
                pass_on(1, 2, h)

        @pl.when((j == 1) | (j == 2))
        def _():
            pass_on(1, 3, j - 1)

        pl.when(j == 2)(lambda: own_block(2))

    loop(PLANE, gate_step)
    for k in range(1, nz):
        for h in range(CUTS[1]):
            need(1, k, h)

    def up_step(j):
        left = row_block(j)
        for t, n in tiles:
            acc = gate_acc[left, pl.ds(t, n)] * across(first_all[left, :], up_all, t, n)
            hidden[left, pl.ds(t, n)] = acc.astype(jnp.bfloat16)

    terms_copy.wait_send()

    cut = CUTS[2]
    half_cols = plane_cols // cut
    steps = nz * cut
    per_core = steps // 2
    pair = 2
    early = cut // pair * PLANE
    first_units = (nz - 1) * early
    last_units = cut * PLANE

    def turn_of(order):
        return jnp.where(order == 0, PLANE - 1, jnp.where(order == PLANE - 1, 0, order))

    def wide_unit(t):
        per = cut // pair
        order = jnp.where(t < early, t // per, (t - early) % PLANE)
        i = jnp.where(t < early, t % per, per + (t - early) // PLANE)
        inner = (i >= per) & has_up & has_down
        k = jnp.where(inner, 1 + i % 2, i // per)
        h = jnp.where(inner, (i - per) // 2, i % per)
        at = seq(k) * per + h
        own = per_core // pair
        return order, turn_of(order), k, h * pair, at * pair, at // own == c, at % own * pair, at % own, 1 + at % 2

    def last_unit(t):
        h, order = t // PLANE, t % PLANE
        at = seq(nz - 1) * cut + h
        return order, turn_of(order), nz - 1, h, at, at // per_core == c, at % per_core, per_core // pair + h, 0

    def pair_copy(unit, pieces, t):
        _, j, _, _, _, _, q, sem, _ = unit(t)
        ref = (pl.ds(q, pieces), row_block(j))
        return remote(p_s.at[ref], p_r.at[ref], d2_s, d2_r.at[sem, j], fs, oc)

    def rows_copy(unit, pieces, t):
        _, j, _, _, _, _, q, sem, via = unit(t)
        pick = jnp.maximum(j - 1, 0)
        corner = j == PLANE - 1
        relayed = pieces == pair
        recv = jnp.where(corner, 2 + sem if relayed else 1, 0)
        dev = z * PLANE + place_of(jnp.where(corner, via, j) if relayed else j)
        span = pl.ds(q, pieces)
        return remote(p_r.at[span, row_block(j)], r_r.at[pick, span], rs_s, rs_r.at[recv], dev)

    def held(unit, t):
        _, j, _, _, _, _, _, _, via = unit(t)
        return (via > 0) & (j == 3 - via)

    def finish(unit, pieces, t):
        _, j, _, _, _, mine, q, _, _ = unit(t)

        @pl.when(mine)
        def _():
            pair_copy(unit, pieces, t).wait_recv()
            place = row_block(j)
            for e in range(pieces):
                both = p_own[t % SLOTS, :, pl.ds(e * half_cols, half_cols)].astype(jnp.float32)
                both = both + p_r[q + e, place, :].astype(jnp.float32)
                p_r[q + e, place, :] = both.astype(jnp.bfloat16)
            pl.when((j > 0) & jnp.logical_not(held(unit, t)))(lambda: rows_copy(unit, pieces, t).start())

    def relay(t):
        _, j, _, _, _, mine, q, sem, _ = wide_unit(t)

        @pl.when(mine & held(wide_unit, t))
        def _():
            ref = r_r.at[PLANE - 2, pl.ds(q, pair)]
            remote(ref, ref, rs_s, rs_r.at[2 + sem], peers[1]).wait_recv()
            place = row_block(j)
            for e in range(pair):
                both = r_r[PLANE - 2, q + e].astype(jnp.float32) + p_r[q + e, place, :].astype(jnp.float32)
                p_r[q + e, place, :] = both.astype(jnp.bfloat16)
            rows_copy(wide_unit, pair, t).start()

    def project(unit, pieces, t):
        _, j, _, _, at, mine, q, _, _ = unit(t)
        from_cols = pl.ds(mult(at * half_cols, pieces * half_cols), pieces * half_cols)
        place = row_block(j)
        made = add_rows(hidden[place, :], down_all[:, from_cols]).astype(jnp.bfloat16)

        @pl.when(mine)
        def _():
            p_own[t % SLOTS, :, pl.ds(0, pieces * half_cols)] = made

        @pl.when(jnp.logical_not(mine))
        def _():
            for e in range(pieces):
                p_s[q + e, place, :] = made[:, e * half_cols : (e + 1) * half_cols]
            pair_copy(unit, pieces, t).start()

    relay_lag = jnp.where(has_up & has_down, RELAY_LAGS[1], RELAY_LAGS[0])

    def wide_step(t):
        order, j, k, h = wide_unit(t)[:4]
        pl.when((t < early) & (t % (cut // pair) == 0))(lambda: up_step(j))

        @pl.when((t % (early // cut) == 0) & (t > 0) & (t <= early))
        def _():
            pass_on(2, 1, t // (early // cut) - 1)
            pass_on(2, 2, t // (early // cut) - 1)

        @pl.when((k > 0) & (order == 0))
        def _():
            for e in range(pair):
                need(2, k, h + e)

        project(wide_unit, pair, t)
        pl.when(t >= LAG)(lambda: finish(wide_unit, pair, t - LAG))
        pl.when(t >= relay_lag)(lambda: relay(t - relay_lag))

    def last_step(t):
        order, _, k, h = last_unit(t)[:4]

        @pl.when(order == 0)
        def _():
            pass_on(2, k, h)
            need(2, k, h)

        project(last_unit, 1, t)
        pl.when(t >= LAG)(lambda: finish(last_unit, 1, t - LAG))
        pl.when(t < relay_lag)(lambda: relay(first_units - relay_lag + t))

    loop(first_units, wide_step)
    loop(LAG, lambda i: finish(wide_unit, pair, first_units - LAG + i))
    loop(last_units, last_step)
    loop(LAG, lambda i: finish(last_unit, 1, last_units - LAG + i))

    ref = r_r.at[pl.ds(0, 2)]
    remote(ref, ref, rs_s, rs_r.at[0], peers[1]).wait_recv()
    direct = seq(nz - 1)

    @pl.when(direct * cut // per_core == c)
    def _():
        ref = r_r.at[PLANE - 2, pl.ds(0, cut)]
        remote(ref, ref, rs_s, rs_r.at[1], peers[1]).wait_recv()

    def add_ffn(i):
        for q in range(per_core):
            cols = pl.ds(q * half_cols, half_cols)
            total = p_r[q, pl.ds(mult(p * rows + i * depth, depth), depth), :].astype(jnp.float32)
            for j in (1, 2):
                total = total + r_r[j - 1, q, part(i), :].astype(jnp.float32)
            corner = r_r[PLANE - 2, q, part(i), :].astype(jnp.float32)
            total = total + jnp.where((c * per_core + q) // cut == direct, corner, 0.0)
            resid[part(i), cols] = resid[part(i), cols] + total.astype(jnp.bfloat16).astype(jnp.float32)
        put_stats(2, part(i), resid[part(i), :])

    loop(rows // depth, add_ffn)
    stats_copy(2).start()

    tok_copy.wait_send()
    stats_copy(0).wait_send()
    stats_copy(1).wait_send()
    ref = first_all.at[pl.ds(0, (PLANE - 1) * rows), pl.ds(0, feats)]
    remote(ref, ref, first_s, first_s, peers[1]).wait_send()
    ref = first_all.at[pl.ds(0, PLANE * rows), pl.ds(0, feats)]
    remote(ref, ref, swap_s, swap_s, fs, oc).wait_send()
    for n in range(len(items)):
        ref = items[n][1](0, 3 * nz)
        remote(ref, ref, sg_p.at[n], sg_l.at[n], peers[1]).wait_send()
        blocks_sent(lambda count: items[n][1](0, count), lambda way: sg_z.at[n, way])
    for w in range(len(wides)):
        quarters_all(w).wait_send()
        blocks_sent(lambda count: wides[w][1].at[:, pl.ds(0, count * plane_cols)], lambda way: z_s.at[w, way])
    remote(p_s, p_r, d2_s, d2_s, fs, oc).wait_send()
    remote(r_r, r_r, rs_s, rs_r.at[0], peers[1]).wait_send()
    stats_copy(2).wait_recv()

    def norm_last(i):
        vals = normalize(2, part(i), resid[part(i), :], gain_two[...], 2 * feats)
        out[part(i), :] = vals.astype(out.dtype)

    loop(rows // depth, norm_last)
    stats_copy(2).wait_send()


def in_one_kernel(*args):
    (tokens, u_weight, v_weight, sg_gain, spatial, bias, out_weight, gain_one, gate, up, down, gain_two) = args
    nz = lax.axis_size("fs") // PLANE
    rows, feats = tokens.shape
    width_sg = u_weight.shape[1]
    quarter = down.shape[0] // PLANE
    wide = 2 * feats
    plane_rows = PLANE * rows
    bf16, f32 = jnp.bfloat16, jnp.float32
    vmem, dma = pltpu.VMEM, pltpu.SemaphoreType.DMA
    steps = nz * CUTS[2]
    half_cols = wide // steps
    scratch = [
        vmem((rows, feats), bf16),
        vmem((1, width_sg), f32),
        vmem(spatial.shape, bf16),
        vmem(bias.shape, f32),
        vmem((1, feats), f32),
        vmem((1, feats), f32),
        vmem(gate.shape, bf16),
        vmem(gate.shape, bf16),
        vmem(gate.shape[::-1], bf16),
        vmem(gate.shape[::-1], bf16),
        vmem((rows, feats), bf16),
        vmem((wide, width_sg), bf16),
        vmem((wide, width_sg), bf16),
        vmem((width_sg, wide), bf16),
        vmem((quarter, wide), bf16),
        vmem((quarter, wide), bf16),
        vmem((quarter, wide), bf16),
        vmem((rows, width_sg), f32),
        vmem((rows, width_sg), f32),
        vmem((rows, width_sg), bf16),
        vmem((rows, width_sg), bf16),
        vmem((3, rows, 128), f32),
        vmem((3, rows, 128), f32),
        vmem((rows, feats), bf16),
        vmem((rows, feats), bf16),
        vmem((rows, feats), bf16),
        vmem((rows, feats), f32),
        vmem((plane_rows, wide), bf16),
        vmem((plane_rows, quarter), bf16),
        vmem((plane_rows, quarter), f32),
        vmem((steps // 2, plane_rows, half_cols), bf16),
        vmem((steps // 2, plane_rows, half_cols), bf16),
        vmem((SLOTS, rows, 2 * half_cols), bf16),
        vmem((PLANE - 1, steps // 2, rows, half_cols), bf16),
        dma((12,)),
        dma((4, nz, 2)),
        dma((4,)),
        dma((4, 2)),
        dma((4,)),
        dma((3,)),
        dma((3,)),
        dma((3, 2)),
        dma((sum(CUTS) * nz,)),
        dma((2,)),
        dma((3, 2)),
        dma((2,)),
        dma(()),
        dma((PLANE + 1,)),
        dma(()),
        dma((PLANE,)),
        dma(()),
        dma((steps // 2, PLANE)),
        dma(()),
        dma((2 + steps // 4,)),
    ]
    spec = pl.BlockSpec(memory_space=pltpu.VMEM)
    return pl.pallas_call(
        functools.partial(layer_kernel, (nz,)),
        name="layer",
        out_shape=jax.ShapeDtypeStruct((rows, feats), tokens.dtype),
        in_specs=[pl.BlockSpec(memory_space=pl.ANY)] * 12,
        out_specs=spec,
        scratch_shapes=scratch,
        compiler_params=pltpu.CompilerParams(
            collective_id=0, has_side_effects=True, vmem_limit_bytes=67_043_328
        ),
    )(
        tokens,
        u_weight,
        v_weight,
        sg_gain[None],
        spatial,
        bias,
        out_weight,
        gain_one[None],
        gate,
        up,
        down,
        gain_two[None],
    )


def fits(tokens, u_weight, gate_weight, spatial_weight):
    if lax.axis_size("tp") != 2 or lax.axis_size("fs") != 4 * PLANE:
        return False
    quarter = gate_weight.shape[1] % PLANE == 0 and gate_weight.shape[1] // PLANE % 16 == 0
    lanes = u_weight.shape[0] % 128 == 0 and u_weight.shape[1] % 256 == 0
    return quarter and lanes and tokens.shape[0] % (PLANE * spatial_weight.shape[1]) == 0


def choose(*args):
    if fits(args[0], args[1], args[8], args[4]):
        return in_one_kernel(*args)
    return on_device(*args)


def solution(mesh):
    return jax.shard_map(
        choose,
        mesh=mesh,
        in_specs=(
            P("fs", "tp"),
            P("fs", "tp"),
            P("fs", "tp"),
            P("tp"),
            P("tp", None, None),
            P("tp", None),
            P("tp", "fs"),
            P("tp"),
            P("fs", "tp"),
            P("fs", "tp"),
            P("tp", "fs"),
            P("tp"),
        ),
        out_specs=P("fs", "tp"),
        check_vma=False,
    )
```

```python
import functools

import jax
import jax.numpy as jnp
from jax import lax
from jax.experimental import pallas as pl
from jax.experimental.pallas import tpu as pltpu
from jax.sharding import PartitionSpec as P

EPS = 1e-05
ALPHA = 2.0**0.25


def add_rows(left, piece):
    return jnp.dot(left, piece, preferred_element_type=jnp.float32)


def scaled_rows(vals, sums, gain, count):
    mean = sums[0][:, None] / count
    square = sums[1][:, None] / count
    return (vals - mean) * lax.rsqrt(square - mean * mean + EPS) * gain[None, :]


def chip_sizes(count):
    across = 2 if count % 2 == 0 else 1
    down = 2 if (count // across) % 2 == 0 else 1
    return count // (across * down), down, across


def shift(value, sizes, axis, step=1):
    count = sizes[0] * sizes[1] * sizes[2]
    stride = sizes[1] * sizes[2] if axis == 0 else (sizes[2] if axis == 1 else 1)
    pairs = []
    for source in range(count):
        place = (source // stride) % sizes[axis]
        pairs.append((source, source + ((place + step) % sizes[axis] - place) * stride))
    return lax.ppermute(value, "fs", pairs)


def around(value, sizes, axis):
    if sizes[axis] == 4:
        near = shift(value, sizes, axis, 1)
        last = shift(value, sizes, axis, -1)
        return [value, near, shift(near, sizes, axis, 1), last]
    pieces = [value]
    for _ in range(sizes[axis] - 1):
        pieces.append(shift(pieces[-1], sizes, axis))
    return pieces


def ring(value, sizes, axis, place):
    return in_order(around(value, sizes, axis), place)


def other_core(value):
    return lax.ppermute(value, "tp", [(0, 1), (1, 0)])


def all_features(value):
    if lax.axis_size("tp") != 2:
        return lax.all_gather(value, "tp", axis=1, tiled=True)
    return jnp.concatenate(in_two(value, other_core(value), lax.axis_index("tp")), axis=1)


def in_two(mine, other, place):
    return [jnp.where(place == 0, mine, other), jnp.where(place == 0, other, mine)]


def sum_shares(terms):
    if lax.axis_size("tp") != 2:
        return lax.psum_scatter(terms, "tp", scatter_dimension=1, tiled=True)
    core = lax.axis_index("tp")
    half = terms.shape[1] // 2
    mine = lax.dynamic_slice_in_dim(terms, core * half, half, 1)
    sent = lax.dynamic_slice_in_dim(terms, (1 - core) * half, half, 1)
    return (mine.astype(jnp.float32) + other_core(sent).astype(jnp.float32)).astype(jnp.bfloat16)


def in_order(pieces, place):
    count = len(pieces)
    if count == 1:
        return pieces[0][None]
    held = jnp.zeros((count,) + pieces[0].shape, pieces[0].dtype)
    for step, piece in enumerate(pieces):
        start = lax.rem(place - step + count, count)
        held = lax.dynamic_update_slice_in_dim(held, piece[None], start, 0)
    return held


def gather_all(piece, sizes, places, order):
    held = piece
    for axis in order:
        held = ring(held, sizes, axis, places[axis])
    back = [order[::-1].index(axis) for axis in range(3)]
    rest = [3 + i for i in range(piece.ndim)]
    return jnp.transpose(held, back + rest)


def after(value, *others):
    return lax.optimization_barrier((value,) + others)[0]


def share_pieces(weight, dim, sizes, places, level, marks):
    across = sizes[2]
    width = weight.shape[dim] // across
    if across == 2:
        mine = lax.dynamic_slice_in_dim(weight, places[2] * width, width, dim)
        other = lax.dynamic_slice_in_dim(weight, (1 - places[2]) * width, width, dim)
        block = jnp.stack(in_two(mine, shift(other, sizes, 2), places[2]))
    else:
        block = weight[None]
    if sizes[0] != 4 or sizes[1] != 2:
        first = around(block, sizes, 0)
        return [[piece] if sizes[1] == 1 else [piece, shift(piece, sizes, 1)] for piece in first]
    if marks[0] is not None:
        block = after(block, marks[0])
    near, last = shift(block, sizes, 0, 1), shift(block, sizes, 0, -1)
    beside = shift(block if marks[0] is None else after(block, marks[1]), sizes, 1)
    near, last = after(near, marks[1]), after(last, marks[1])
    far = shift(near, sizes, 0)
    near_beside, last_beside = shift(near, sizes, 1), shift(last, sizes, 1)
    if level:
        far_beside = shift(after(near_beside, marks[2]), sizes, 0)
    else:
        far = after(far, marks[2])
        far_beside = shift(far, sizes, 1)
    return [[block, beside], [near, near_beside], [far, far_beside], [last, last_beside]]


def place_pieces(pieces, places):
    shape = pieces[0][0].shape
    count, down = len(pieces), len(pieces[0])
    held = jnp.zeros((count, down) + shape, pieces[0][0].dtype)
    for step, pair in enumerate(pieces):
        start = lax.rem(places[0] - step + count, count)
        for turn, piece in enumerate(pair):
            spot = places[1] if turn == 0 else 1 - places[1]
            held = lax.dynamic_update_slice(held, piece[None, None], [start, spot] + [0] * len(shape))
    return held


def on_device(
    tokens,
    u_weight,
    v_weight,
    sg_gain,
    spatial_weight,
    spatial_bias,
    out_weight,
    gain_one,
    gate_weight,
    up_weight,
    down_weight,
    gain_two,
):
    parts = lax.axis_size("tp")
    sizes = chip_sizes(lax.axis_size("fs"))
    index = lax.axis_index("fs")
    places = (index // (sizes[1] * sizes[2]), (index // sizes[2]) % sizes[1], index % sizes[2])
    whole = all_features(tokens)
    rows = whole.shape[0]
    width_sg = u_weight.shape[1]

    def add_one(piece):
        return add_rows(whole, piece)

    pre_u = add_one(gather_all(u_weight, sizes, places, [0, 1, 2]).reshape(-1, width_sg))
    pre_v = add_one(gather_all(v_weight, sizes, places, [0, 2, 1]).reshape(-1, width_sg))
    gated = jax.nn.gelu(pre_u)
    valued = jax.nn.gelu(pre_v)
    stats = lax.psum((jnp.sum(valued, axis=1), jnp.sum(valued * valued, axis=1)), "tp")
    normed = scaled_rows(valued, stats, sg_gain, width_sg * parts).astype(jnp.bfloat16)
    groups_here = spatial_weight.shape[0]
    block = spatial_weight.shape[1]
    group_width = width_sg // groups_here
    shaped = normed.reshape(rows // block, block, groups_here, group_width)
    lower = jnp.tril(jnp.ones((block, block), jnp.bool_))
    masked = jnp.where(lower[None], spatial_weight, jnp.zeros_like(spatial_weight))
    mixed = jnp.einsum("gij,njgd->nigd", masked, shaped, preferred_element_type=jnp.float32)
    mixed = mixed + spatial_bias.T[None, :, :, None]
    gated_out = (gated * mixed.reshape(rows, width_sg)).astype(jnp.bfloat16)
    out_all = gather_all(out_weight, sizes, places, [0, 1, 2])
    out_all = out_all.reshape((-1,) + out_weight.shape)
    terms = jnp.einsum("tk,nkc->tnc", gated_out, out_all, preferred_element_type=jnp.float32)
    mix = sum_shares(terms.reshape(rows, -1).astype(jnp.bfloat16))
    resid = ALPHA * tokens.astype(jnp.float32) + mix.astype(jnp.float32)
    first_sums = lax.psum((jnp.sum(resid, axis=1), jnp.sum(resid * resid, axis=1)), "tp")
    first = scaled_rows(resid, first_sums, gain_one, resid.shape[1] * parts).astype(jnp.bfloat16)
    gate_pieces = share_pieces(gate_weight, 1, sizes, places, False, (None, normed, mix))
    up_pieces = share_pieces(up_weight, 1, sizes, places, True, (None, normed, mix))
    down_pieces = share_pieces(down_weight, 0, sizes, places, False, (normed, first, first))
    gate_all = place_pieces(gate_pieces, places)
    gate_all = gate_all.reshape(-1, gate_all.shape[-1])
    up_all = place_pieces(up_pieces, places)
    up_all = up_all.reshape(-1, up_all.shape[-1])
    def feed(part):
        whole_part = all_features(part)
        gate = add_rows(whole_part, gate_all)
        upper = add_rows(whole_part, up_all)
        return (jax.nn.silu(gate) * upper).astype(jnp.bfloat16)

    two = sizes[2] == 2
    if two:
        there = feed(shift(first, sizes, 2))
        here = feed(first)
        down_pieces = [[pair[0]] + [after(piece, there, here) for piece in pair[1:]] for pair in down_pieces]
    else:
        here = feed(first)
    down_all = place_pieces(down_pieces, places)
    down_all = down_all.reshape((-1,) + down_all.shape[-2:])

    def project(hidden):
        made = jnp.einsum("tf,nfc->tnc", hidden, down_all, preferred_element_type=jnp.float32)
        return sum_shares(made.reshape(rows, -1).astype(jnp.bfloat16))

    if two:
        there = project(there)
        sent = shift(there, sizes, 2)
        ffn = project(after(here, there)).astype(jnp.float32) + sent.astype(jnp.float32)
    else:
        ffn = project(here).astype(jnp.float32)
    second = ALPHA * first.astype(jnp.float32) + ffn.astype(jnp.float32)
    last_sums = lax.psum((jnp.sum(second, axis=1), jnp.sum(second * second, axis=1)), "tp")
    return scaled_rows(second, last_sums, gain_two, second.shape[1] * parts).astype(jnp.bfloat16)


MESH = pl.DeviceIdType.MESH
PLANE = 4
CUTS = (2, 2, 4)
BLOCKS = 2
LAG = 1
RELAY_LAGS = (6, 12)
SLOTS = 4


def layer_kernel(
    sizes,
    tok_in,
    u_in,
    v_in,
    sg_gain_in,
    spatial_in,
    bias_in,
    o_in,
    gain_one_in,
    gate_in,
    up_in,
    down_in,
    resid_out,
    mine_out,
    theirs_out,
    tok,
    sg_gain,
    spatial,
    bias,
    gain_one,
    gate_own,
    up_own,
    gate_turned,
    up_turned,
    tok_o,
    u_all,
    v_all,
    o_all,
    gate_all,
    up_all,
    down_all,
    gated,
    valued,
    normed,
    gated_out,
    st_s,
    st_r,
    terms_s,
    terms_o,
    terms_r,
    resid,
    first_all,
    hidden,
    gate_acc,
    p_s,
    p_r,
    p_own,
    r_r,
    in_sem,
    out_sem,
    sg_r,
    sg_l,
    sg_z,
    sg_p,
    a2_s,
    a2_r,
    z_s,
    z_r,
    tok_sem,
    st_sem,
    terms_sem,
    first_s,
    first_r,
    swap_s,
    swap_r,
    d2_s,
    d2_r,
    rs_s,
    rs_r,
):
    nz = sizes[0]
    fs, c = lax.axis_index("fs"), lax.axis_index("tp")
    oc = 1 - c
    z, p = fs // PLANE, fs % PLANE
    y, x = p // 2, p % 2
    peers = [z * PLANE + (y + j // 2) % 2 * 2 + (x + j % 2) % 2 for j in range(PLANE)]
    inplane = [(y + j // 2) % 2 * 2 + (x + j % 2) % 2 for j in range(PLANE)]
    has_up, has_down = z < nz - 1, z > 0
    up_dev = jnp.where(has_up, fs + PLANE, fs - PLANE)
    down_dev = jnp.where(has_down, fs - PLANE, fs + PLANE)
    rows, feats = tok.shape
    kb, width_sg = u_in.shape
    depth = rows // PLANE
    quarter = hidden.shape[1]
    plane_cols = PLANE * kb

    def mult(value, by):
        return pl.multiple_of(value, by)

    def seq(k):
        swapped = jnp.where(k < 2, 1 - k, k)
        return jnp.where(z == 0, k, jnp.where(z == 1, swapped, jnp.where(z == 2, nz - 1 - swapped, nz - 1 - k)))

    def remote(src, dst, send, recv, dev, core=None):
        where_to = (dev, c if core is None else core)
        return pltpu.make_async_remote_copy(
            src_ref=src, dst_ref=dst, send_sem=send, recv_sem=recv, device_id=where_to, device_id_type=MESH
        )

    def start_if(pred, copy):
        pl.when(pred)(lambda: copy.start())

    def sent_if(pred, copy):
        pl.when(pred)(lambda: copy.wait_send())

    own_rows = pl.ds(mult(fs * kb, kb), kb)
    own_quarter = pl.ds(mult(p * quarter, 16), quarter)
    loads = [
        (gate_in, gate_own),
        (up_in, up_own),
        (u_in, u_all.at[own_rows, :]),
        (v_in, v_all.at[own_rows, :]),
        (o_in, o_all.at[:, own_rows]),
        (down_in.at[own_quarter, :], down_all.at[:, own_rows]),
        (tok_in, tok),
        (sg_gain_in, sg_gain),
        (spatial_in, spatial),
        (bias_in, bias),
        (gain_one_in, gain_one),
    ]
    loads = [pltpu.make_async_copy(src, dst, in_sem.at[i]) for i, (src, dst) in enumerate(loads)]
    for load in loads:
        load.start()
    barrier = pltpu.get_barrier_semaphore()
    for dev, core in [(fs, oc)] + [(peers[j], c) for j in range(1, PLANE)]:
        pl.semaphore_signal(barrier, inc=1, device_id=(dev, core), device_id_type=MESH)
    for pred, dev in [(has_up, up_dev), (has_down, down_dev)]:
        @pl.when(pred)
        def _():
            pl.semaphore_signal(barrier, inc=1, device_id=(dev, c), device_id_type=MESH)
    pl.semaphore_wait(barrier, PLANE + jnp.where(has_up, 1, 0) + jnp.where(has_down, 1, 0))

    def rows_of(ref):
        return lambda i, count=1: ref.at[pl.ds(mult(i * kb, kb), count * kb), :]

    def cols_of(ref, part):
        height = width_sg // 2
        return lambda i, count=1: ref.at[pl.ds(part * height, height), pl.ds(mult(i * kb, kb), count * kb)]

    half_o = width_sg // 2
    items = [
        (u_in, rows_of(u_all), 1, 2),
        (v_in, rows_of(v_all), 2, 1),
        (o_in.at[pl.ds(0, half_o), :], cols_of(o_all, 0), 1, 2),
        (o_in.at[pl.ds(half_o, half_o), :], cols_of(o_all, 1), 2, 1),
    ]

    def own_copies(n):
        src, at, one, two = items[n]
        return [
            (has_up, remote(src, at(fs), sg_z.at[n, 0], sg_r.at[n, z, 0], up_dev)),
            (has_down, remote(src, at(fs), sg_z.at[n, 1], sg_r.at[n, z, 0], down_dev)),
            (None, remote(src, at(fs), sg_p.at[n], sg_r.at[n, z, 1], peers[one])),
            (None, remote(src, at(fs), sg_p.at[n], sg_l.at[n], peers[two])),
        ]

    def own_start(n):
        for pred, copy in own_copies(n):
            if pred is None:
                copy.start()
            else:
                start_if(pred, copy)

    def forward_to(b):
        going_up = b < z
        dev = jnp.where(going_up, up_dev, down_dev)
        return (going_up & has_up) | ((b > z) & has_down), dev, jnp.where(going_up, 0, 1)

    def column_copies(n, k):
        _, at, one, two = items[n]
        b = seq(k)
        idx = b * PLANE + p
        pred, dev, way = forward_to(b)
        ref = at(idx)
        return [
            (pred, remote(ref, ref, sg_z.at[n, way], sg_r.at[n, b, 0], dev)),
            (None, remote(ref, ref, sg_p.at[n], sg_r.at[n, b, 1], peers[one])),
            (None, remote(ref, ref, sg_p.at[n], sg_l.at[n], peers[two])),
        ]

    def column(n, k):
        copies = column_copies(n, k)
        copies[0][1].wait_recv()
        start_if(*copies[0])
        copies[1][1].start()
        copies[2][1].start()

    def beside(n, k):
        _, at, one, two = items[n]
        b = seq(k)
        ref = at(b * PLANE + inplane[one])
        remote(ref, ref, sg_p.at[n], sg_r.at[n, b, 1], peers[one]).wait_recv()
        remote(ref, ref, sg_p.at[n], sg_l.at[n], peers[two]).start()

    def gathered(n):
        ref = items[n][1](0, 2 * nz)
        remote(ref, ref, sg_p.at[n], sg_l.at[n], peers[1]).wait_recv()

    wides = [(gate_turned, gate_all), (up_turned, up_all), (down_in, down_all)]

    def quarter_copy(w, j):
        src, dst = wides[w]
        theirs = pl.ds(mult(inplane[j] * quarter, 16), quarter)
        mine = pl.ds(mult(fs * kb, kb), kb)
        return remote(src.at[theirs, :], dst.at[:, mine], a2_s.at[w], a2_r.at[w], peers[j])

    def quarters_all(w):
        ref = wides[w][1].at[:, pl.ds(0, (PLANE - 1) * kb)]
        return remote(ref, ref, a2_s.at[w], a2_r.at[w], peers[1])

    def quarters_start(w):
        for j in range(1, PLANE):
            quarter_copy(w, j).start()

    def block(w, b, h):
        cols = plane_cols // CUTS[w]
        return wides[w][1].at[:, pl.ds(mult(b * plane_cols + h * cols, cols), cols)]

    def z_recv(w, b, h):
        return z_r.at[sum(CUTS[:w]) * nz + b * CUTS[w] + h]

    def own_block_copies(w, h):
        ref, recv = block(w, z, h), z_recv(w, z, h)
        return [
            (has_up, remote(ref, ref, z_s.at[w, 0], recv, up_dev)),
            (has_down, remote(ref, ref, z_s.at[w, 1], recv, down_dev)),
        ]

    def own_block(w):
        quarters_all(w).wait_recv()
        for h in range(CUTS[w]):
            for pred, copy in own_block_copies(w, h):
                start_if(pred, copy)

    def pass_copy(w, k, h):
        b = seq(k)
        pred, dev, way = forward_to(b)
        ref = block(w, b, h)
        return pred, remote(ref, ref, z_s.at[w, way], z_recv(w, b, h), dev)

    def blocks_sent(ref_of, sems):
        for n in range(1, nz):
            ref = ref_of(n)
            up = remote(ref, ref, sems(0), sems(0), fs)
            down = remote(ref, ref, sems(1), sems(1), fs)
            pl.when(has_up & (z + 1 == n))(lambda: up.wait_send())
            pl.when(has_down & (nz - z == n))(lambda: down.wait_send())

    def pass_on(w, k, h):
        pred, copy = pass_copy(w, k, h)

        @pl.when(pred)
        def _():
            copy.wait_recv()
            copy.start()

    def need(w, k, h):
        pred, copy = pass_copy(w, k, h)
        pl.when(jnp.logical_not(pred))(lambda: copy.wait_recv())

    lane = lax.broadcasted_iota(jnp.int32, (depth, 128), 1)

    def put_stats(which, place, vals):
        one = jnp.sum(vals, axis=1, keepdims=True)
        two = jnp.sum(vals * vals, axis=1, keepdims=True)
        st_s[which, place, :] = jnp.where(lane == 0, one, two)

    def stats_copy(which):
        theirs = theirs_out if which == 2 else st_r.at[which]
        return remote(st_s.at[which], theirs, st_sem.at[which, 0], st_sem.at[which, 1], fs, oc)

    def normalize(which, place, vals, gain, count):
        both = st_s[which, place, :] + st_r[which, place, :]
        mean = both[:, 0:1] / count
        square = both[:, 1:2] / count
        return (vals - mean) * lax.rsqrt(square - mean * mean + EPS) * gain

    def loop(count, body):
        lax.fori_loop(0, count, lambda i, carry: (body(i), carry)[1], 0)

    def part(i):
        return pl.ds(mult(i * depth, depth), depth)

    tok_copy = remote(tok_in, tok_o, tok_sem.at[0], tok_sem.at[1], fs, oc)
    own_start(0)
    own_start(1)

    def turn(src, dst):
        def step(i):
            place = pl.ds(mult(i * kb, kb), kb)
            dst[place, :] = src[:, place].T

        loop(src.shape[1] // kb, step)

    loads[0].wait()
    turn(gate_own, gate_turned)
    quarters_start(0)
    own_start(2)
    own_start(3)
    tok_copy.start()
    for load in loads[1:]:
        load.wait()
    turn(up_own, up_turned)
    gate_all[:, own_rows] = gate_turned[own_quarter, :]
    up_all[:, own_rows] = up_turned[own_quarter, :]

    for n in (0, 1):
        column(n, 1)
    for n in (0, 1):
        column(n, 2)
    for n in (2, 3):
        column(n, 1)
    for n in (0, 1):
        column(n, 3)
    for n in (2, 3):
        column(n, 2)
    own_block(0)
    for k in (0, 1):
        for n in (0, 1):
            beside(n, k)
    for n in (2, 3):
        column(n, 3)
    pass_on(0, 1, 0)
    pass_on(0, 2, 0)
    for n in (0, 1):
        beside(n, 2)
    pass_on(0, 1, 1)
    pass_on(0, 2, 1)
    for n in (0, 1):
        beside(n, 3)
    quarters_start(1)
    for n in (2, 3):
        beside(n, 0)
    for n in (2, 3):
        beside(n, 1)
    pass_on(0, 3, 0)
    for n in (2, 3):
        beside(n, 2)

    tok_copy.wait_recv()
    wide = 256
    mine_k = pl.ds(mult(c * feats, feats), feats)
    their_k = pl.ds(mult(oc * feats, feats), feats)

    def branch(weight, into):
        def step(n):
            cols = pl.ds(mult(n * wide, wide), wide)
            acc = add_rows(tok[...], weight[mine_k, cols]) + add_rows(tok_o[...], weight[their_k, cols])
            into[:, cols] = jax.nn.gelu(acc)

        loop(width_sg // wide, step)

    gathered(0)
    branch(u_all, gated)
    gathered(1)
    branch(v_all, valued)
    for n in (2, 3):
        beside(n, 3)
    pass_on(0, 3, 1)
    loop(rows // depth, lambda i: put_stats(0, part(i), valued[part(i), :]))
    stats_copy(0).start()
    stats_copy(0).wait_recv()

    def norm_gate(i):
        vals = normalize(0, part(i), valued[part(i), :], sg_gain[...], 2 * width_sg)
        normed[part(i), :] = vals.astype(jnp.bfloat16)

    loop(rows // depth, norm_gate)
    groups, spread = spatial.shape[0], spatial.shape[1]
    row_at = lax.broadcasted_iota(jnp.int32, (spread, spread), 0)
    col_at = lax.broadcasted_iota(jnp.int32, (spread, spread), 1)
    group_dim = width_sg // groups

    def mix_block(n):
        place = pl.ds(mult(n * spread, spread), spread)
        for g in range(groups):
            cols = pl.ds(g * group_dim, group_dim)
            weight = jnp.where(col_at <= row_at, spatial[g], jnp.zeros_like(spatial[g]))
            shift_by = jnp.sum(jnp.where(col_at == row_at, bias[g : g + 1, :], 0.0), axis=1, keepdims=True)
            mixed = jnp.dot(weight, normed[place, cols], preferred_element_type=jnp.float32) + shift_by
            gated_out[place, cols] = (gated[place, cols] * mixed).astype(jnp.bfloat16)

    loop(rows // spread, mix_block)
    for n in (2, 3):
        gathered(n)

    def project_out(which, into):
        def step(n):
            cols = pl.ds(mult(which * feats + n * wide, wide), wide)
            to = pl.ds(mult(n * wide, wide), wide)
            into[:, to] = add_rows(gated_out[...], o_all[:, cols]).astype(jnp.bfloat16)

        loop(feats // wide, step)

    project_out(oc, terms_s)
    terms_copy = remote(terms_s, terms_r, terms_sem.at[0], terms_sem.at[1], fs, oc)
    terms_copy.start()
    project_out(c, terms_o)
    own_block(1)
    terms_copy.wait_recv()

    def add_mix(i):
        mix = terms_o[part(i), :].astype(jnp.float32) + terms_r[part(i), :].astype(jnp.float32)
        vals = ALPHA * tok[part(i), :].astype(jnp.float32) + mix.astype(jnp.bfloat16).astype(jnp.float32)
        resid[part(i), :] = vals
        put_stats(1, part(i), vals)

    loop(rows // depth, add_mix)
    stats_copy(1).start()
    stats_copy(1).wait_recv()
    mine_cols = pl.ds(mult(c * feats, feats), feats)
    their_cols = pl.ds(mult(oc * feats, feats), feats)

    def norm_first(i):
        vals = normalize(1, part(i), resid[part(i), :], gain_one[...], 2 * feats)
        vals = vals.astype(jnp.bfloat16)
        first_all[pl.ds(mult(p * rows + i * depth, depth), depth), mine_cols] = vals
        resid[part(i), :] = ALPHA * vals.astype(jnp.float32)

    loop(rows // depth, norm_first)

    def place_of(j):
        return (y + j // 2) % 2 * 2 + (x + j % 2) % 2

    def tokens_of(j, cols):
        return first_all.at[pl.ds(mult(place_of(j) * rows, rows), rows), cols]

    def swap_copy(j):
        ref = tokens_of(j, mine_cols)
        return remote(ref, ref, swap_s, swap_r.at[j], fs, oc)

    own_tokens = tokens_of(0, mine_cols)
    first_copies = [
        remote(own_tokens, own_tokens, first_s, first_r.at[j], peers[j]) for j in (1, 2)
    ]

    def corner_copy(j):
        start = mult(place_of(j) * rows + (j - 1) * (rows // 2), rows // 2)
        ref = first_all.at[pl.ds(start, rows // 2), mine_cols]
        return remote(ref, ref, first_s, first_r.at[j + 2], z * PLANE + place_of(PLANE - 1 - j))

    swap_copy(0).start()
    for copy in first_copies:
        copy.start()
    quarters_start(2)

    for k in range(1, nz):
        for h in range(CUTS[0]):
            need(0, k, h)

    tiles = [(t, min(wide, quarter - t)) for t in range(0, quarter, wide)]

    def across(left, weight, t, n):
        return lax.dot_general(
            left, weight[pl.ds(t, n), :], (((1,), (1,)), ((), ())), preferred_element_type=jnp.float32
        )

    def row_block(j):
        return pl.ds(mult(place_of(j) * rows, rows), rows)

    def gate_step(j):
        @pl.when((j == 1) | (j == 2))
        def _():
            ref = tokens_of(j, mine_cols)
            remote(ref, ref, first_s, first_r.at[j], fs, oc).wait_recv()
            corner_copy(j).start()

        @pl.when(j == PLANE - 1)
        def _():
            for half in (0, 1):
                start = mult(place_of(j) * rows + half * (rows // 2), rows // 2)
                ref = first_all.at[pl.ds(start, rows // 2), mine_cols]
                remote(ref, ref, first_s, first_r.at[half + 3], fs, oc).wait_recv()

        @pl.when(j > 0)
        def _():
            swap_copy(j).start()

        ref = tokens_of(j, their_cols)
        remote(ref, ref, swap_s, swap_r.at[j], fs, oc).wait_recv()
        left = row_block(j)
        for t, n in tiles:
            gate_acc[left, pl.ds(t, n)] = jax.nn.silu(across(first_all[left, :], gate_all, t, n))

        @pl.when(j == 0)
        def _():
            for h in range(CUTS[1]):
                pass_on(1, 1, h)
                pass_on(1, 2, h)

        @pl.when((j == 1) | (j == 2))
        def _():
            pass_on(1, 3, j - 1)

        pl.when(j == 2)(lambda: own_block(2))

    loop(PLANE, gate_step)
    for k in range(1, nz):
        for h in range(CUTS[1]):
            need(1, k, h)

    def up_step(j):
        left = row_block(j)
        for t, n in tiles:
            acc = gate_acc[left, pl.ds(t, n)] * across(first_all[left, :], up_all, t, n)
            hidden[left, pl.ds(t, n)] = acc.astype(jnp.bfloat16)

    terms_copy.wait_send()

    cut = CUTS[2]
    half_cols = plane_cols // cut
    steps = nz * cut
    per_core = steps // 2
    pair = 2
    early = cut // pair * PLANE
    first_units = (nz - 1) * early
    last_units = cut * PLANE

    def turn_of(order):
        return jnp.where(order == 0, PLANE - 1, jnp.where(order == PLANE - 1, 0, order))

    def wide_unit(t):
        per = cut // pair
        order = jnp.where(t < early, t // per, (t - early) % PLANE)
        i = jnp.where(t < early, t % per, per + (t - early) // PLANE)
        inner = (i >= per) & has_up & has_down
        k = jnp.where(inner, 1 + i % 2, i // per)
        h = jnp.where(inner, (i - per) // 2, i % per)
        at = seq(k) * per + h
        own = per_core // pair
        return order, turn_of(order), k, h * pair, at * pair, at // own == c, at % own * pair, at % own, 1 + at % 2

    def last_unit(t):
        h, order = t // PLANE, t % PLANE
        at = seq(nz - 1) * cut + h
        return order, turn_of(order), nz - 1, h, at, at // per_core == c, at % per_core, per_core // pair + h, 0

    def pair_copy(unit, pieces, t):
        _, j, _, _, _, _, q, sem, _ = unit(t)
        ref = (pl.ds(q, pieces), row_block(j))
        return remote(p_s.at[ref], p_r.at[ref], d2_s, d2_r.at[sem, j], fs, oc)

    def rows_copy(unit, pieces, t):
        _, j, _, _, _, _, q, sem, via = unit(t)
        pick = jnp.maximum(j - 1, 0)
        corner = j == PLANE - 1
        relayed = pieces == pair
        recv = jnp.where(corner, 2 + sem if relayed else 1, 0)
        dev = z * PLANE + place_of(jnp.where(corner, via, j) if relayed else j)
        span = pl.ds(q, pieces)
        return remote(p_r.at[span, row_block(j)], r_r.at[pick, span], rs_s, rs_r.at[recv], dev)

    def held(unit, t):
        _, j, _, _, _, _, _, _, via = unit(t)
        return (via > 0) & (j == 3 - via)

    def finish(unit, pieces, t):
        _, j, _, _, _, mine, q, _, _ = unit(t)

        @pl.when(mine)
        def _():
            pair_copy(unit, pieces, t).wait_recv()
            place = row_block(j)
            for e in range(pieces):
                both = p_own[t % SLOTS, :, pl.ds(e * half_cols, half_cols)].astype(jnp.float32)
                both = both + p_r[q + e, place, :].astype(jnp.float32)
                p_r[q + e, place, :] = both.astype(jnp.bfloat16)
            pl.when((j > 0) & jnp.logical_not(held(unit, t)))(lambda: rows_copy(unit, pieces, t).start())

    def relay(t):
        _, j, _, _, _, mine, q, sem, _ = wide_unit(t)

        @pl.when(mine & held(wide_unit, t))
        def _():
            ref = r_r.at[PLANE - 2, pl.ds(q, pair)]
            remote(ref, ref, rs_s, rs_r.at[2 + sem], peers[1]).wait_recv()
            place = row_block(j)
            for e in range(pair):
                both = r_r[PLANE - 2, q + e].astype(jnp.float32) + p_r[q + e, place, :].astype(jnp.float32)
                p_r[q + e, place, :] = both.astype(jnp.bfloat16)
            rows_copy(wide_unit, pair, t).start()

    def project(unit, pieces, t):
        _, j, _, _, at, mine, q, _, _ = unit(t)
        from_cols = pl.ds(mult(at * half_cols, pieces * half_cols), pieces * half_cols)
        place = row_block(j)
        made = add_rows(hidden[place, :], down_all[:, from_cols]).astype(jnp.bfloat16)

        @pl.when(mine)
        def _():
            p_own[t % SLOTS, :, pl.ds(0, pieces * half_cols)] = made

        @pl.when(jnp.logical_not(mine))
        def _():
            for e in range(pieces):
                p_s[q + e, place, :] = made[:, e * half_cols : (e + 1) * half_cols]
            pair_copy(unit, pieces, t).start()

    relay_lag = jnp.where(has_up & has_down, RELAY_LAGS[1], RELAY_LAGS[0])

    def wide_step(t):
        order, j, k, h = wide_unit(t)[:4]
        pl.when((t < early) & (t % (cut // pair) == 0))(lambda: up_step(j))

        @pl.when((t % (early // cut) == 0) & (t > 0) & (t <= early))
        def _():
            pass_on(2, 1, t // (early // cut) - 1)
            pass_on(2, 2, t // (early // cut) - 1)

        @pl.when((k > 0) & (order == 0))
        def _():
            for e in range(pair):
                need(2, k, h + e)

        project(wide_unit, pair, t)
        pl.when(t >= LAG)(lambda: finish(wide_unit, pair, t - LAG))
        pl.when(t >= relay_lag)(lambda: relay(t - relay_lag))

    def last_step(t):
        order, _, k, h = last_unit(t)[:4]

        @pl.when(order == 0)
        def _():
            pass_on(2, k, h)
            need(2, k, h)

        project(last_unit, 1, t)
        pl.when(t >= LAG)(lambda: finish(last_unit, 1, t - LAG))
        pl.when(t < relay_lag)(lambda: relay(first_units - relay_lag + t))

    loop(first_units, wide_step)
    loop(LAG, lambda i: finish(wide_unit, pair, first_units - LAG + i))
    loop(last_units, last_step)
    loop(LAG, lambda i: finish(last_unit, 1, last_units - LAG + i))

    ref = r_r.at[pl.ds(0, 2)]
    remote(ref, ref, rs_s, rs_r.at[0], peers[1]).wait_recv()
    direct = seq(nz - 1)

    @pl.when(direct * cut // per_core == c)
    def _():
        ref = r_r.at[PLANE - 2, pl.ds(0, cut)]
        remote(ref, ref, rs_s, rs_r.at[1], peers[1]).wait_recv()

    def add_ffn(i):
        for q in range(per_core):
            cols = pl.ds(q * half_cols, half_cols)
            total = p_r[q, pl.ds(mult(p * rows + i * depth, depth), depth), :].astype(jnp.float32)
            for j in (1, 2):
                total = total + r_r[j - 1, q, part(i), :].astype(jnp.float32)
            corner = r_r[PLANE - 2, q, part(i), :].astype(jnp.float32)
            total = total + jnp.where((c * per_core + q) // cut == direct, corner, 0.0)
            resid[part(i), cols] = resid[part(i), cols] + total.astype(jnp.bfloat16).astype(jnp.float32)
        resid_copy(i).start()
        put_stats(2, part(i), resid[part(i), :])

    def resid_copy(i):
        return pltpu.make_async_copy(resid.at[part(i), :], resid_out.at[part(i), :], out_sem.at[i])

    loop(rows // depth, add_ffn)
    stats_copy(2).start()
    mine_copy = pltpu.make_async_copy(st_s.at[2], mine_out, out_sem.at[rows // depth])
    mine_copy.start()

    tok_copy.wait_send()
    stats_copy(0).wait_send()
    stats_copy(1).wait_send()
    ref = first_all.at[pl.ds(0, (PLANE - 1) * rows), pl.ds(0, feats)]
    remote(ref, ref, first_s, first_s, peers[1]).wait_send()
    ref = first_all.at[pl.ds(0, PLANE * rows), pl.ds(0, feats)]
    remote(ref, ref, swap_s, swap_s, fs, oc).wait_send()
    for n in range(len(items)):
        ref = items[n][1](0, 3 * nz)
        remote(ref, ref, sg_p.at[n], sg_l.at[n], peers[1]).wait_send()
        blocks_sent(lambda count: items[n][1](0, count), lambda way: sg_z.at[n, way])
    for w in range(len(wides)):
        quarters_all(w).wait_send()
        blocks_sent(lambda count: wides[w][1].at[:, pl.ds(0, count * plane_cols)], lambda way: z_s.at[w, way])
    remote(p_s, p_r, d2_s, d2_s, fs, oc).wait_send()
    remote(r_r, r_r, rs_s, rs_r.at[0], peers[1]).wait_send()
    loop(rows // depth, lambda i: resid_copy(i).wait())
    mine_copy.wait()
    stats_copy(2).wait()


def last_norm(count, second, mine, theirs, gain, out):
    both = mine[...] + theirs[...]
    mean = both[:, 0:1] / count
    square = both[:, 1:2] / count
    out[...] = ((second[...] - mean) * lax.rsqrt(square - mean * mean + EPS) * gain[...]).astype(out.dtype)


def in_one_kernel(*args):
    (tokens, u_weight, v_weight, sg_gain, spatial, bias, out_weight, gain_one, gate, up, down, gain_two) = args
    nz = lax.axis_size("fs") // PLANE
    rows, feats = tokens.shape
    width_sg = u_weight.shape[1]
    quarter = down.shape[0] // PLANE
    wide = 2 * feats
    plane_rows = PLANE * rows
    bf16, f32 = jnp.bfloat16, jnp.float32
    vmem, dma = pltpu.VMEM, pltpu.SemaphoreType.DMA
    steps = nz * CUTS[2]
    half_cols = wide // steps
    scratch = [
        vmem((rows, feats), bf16),
        vmem((1, width_sg), f32),
        vmem(spatial.shape, bf16),
        vmem(bias.shape, f32),
        vmem((1, feats), f32),
        vmem(gate.shape, bf16),
        vmem(gate.shape, bf16),
        vmem(gate.shape[::-1], bf16),
        vmem(gate.shape[::-1], bf16),
        vmem((rows, feats), bf16),
        vmem((wide, width_sg), bf16),
        vmem((wide, width_sg), bf16),
        vmem((width_sg, wide), bf16),
        vmem((quarter, wide), bf16),
        vmem((quarter, wide), bf16),
        vmem((quarter, wide), bf16),
        vmem((rows, width_sg), f32),
        vmem((rows, width_sg), f32),
        vmem((rows, width_sg), bf16),
        vmem((rows, width_sg), bf16),
        vmem((3, rows, 128), f32),
        vmem((3, rows, 128), f32),
        vmem((rows, feats), bf16),
        vmem((rows, feats), bf16),
        vmem((rows, feats), bf16),
        vmem((rows, feats), f32),
        vmem((plane_rows, wide), bf16),
        vmem((plane_rows, quarter), bf16),
        vmem((plane_rows, quarter), f32),
        vmem((steps // 2, plane_rows, half_cols), bf16),
        vmem((steps // 2, plane_rows, half_cols), bf16),
        vmem((SLOTS, rows, 2 * half_cols), bf16),
        vmem((PLANE - 1, steps // 2, rows, half_cols), bf16),
        dma((11,)),
        dma((PLANE + 1,)),
        dma((4, nz, 2)),
        dma((4,)),
        dma((4, 2)),
        dma((4,)),
        dma((3,)),
        dma((3,)),
        dma((3, 2)),
        dma((sum(CUTS) * nz,)),
        dma((2,)),
        dma((3, 2)),
        dma((2,)),
        dma(()),
        dma((PLANE + 1,)),
        dma(()),
        dma((PLANE,)),
        dma(()),
        dma((steps // 2, PLANE)),
        dma(()),
        dma((2 + steps // 4,)),
    ]
    spec = pl.BlockSpec(memory_space=pl.ANY)
    stats = jax.ShapeDtypeStruct((rows, 128), f32)
    second, mine, theirs = pl.pallas_call(
        functools.partial(layer_kernel, (nz,)),
        name="layer",
        out_shape=(jax.ShapeDtypeStruct((rows, feats), f32), stats, stats),
        in_specs=[spec] * 11,
        out_specs=(spec, spec, spec),
        scratch_shapes=scratch,
        compiler_params=pltpu.CompilerParams(
            collective_id=0, has_side_effects=True, vmem_limit_bytes=67_043_328
        ),
    )(
        tokens,
        u_weight,
        v_weight,
        sg_gain[None],
        spatial,
        bias,
        out_weight,
        gain_one[None],
        gate,
        up,
        down,
    )
    tall = rows // BLOCKS
    each = pl.BlockSpec((tall, feats), lambda i: (i, 0))
    few = pl.BlockSpec((tall, 128), lambda i: (i, 0))
    return pl.pallas_call(
        functools.partial(last_norm, wide),
        name="last_norm",
        out_shape=jax.ShapeDtypeStruct((rows, feats), tokens.dtype),
        grid=(BLOCKS,),
        in_specs=[each, few, few, pl.BlockSpec((1, feats), lambda i: (0, 0))],
        out_specs=each,
    )(second, mine, theirs, gain_two[None])


def fits(tokens, u_weight, gate_weight, spatial_weight):
    if lax.axis_size("tp") != 2 or lax.axis_size("fs") != 4 * PLANE:
        return False
    quarter = gate_weight.shape[1] % PLANE == 0 and gate_weight.shape[1] // PLANE % 16 == 0
    lanes = u_weight.shape[0] % 128 == 0 and u_weight.shape[1] % 256 == 0
    return quarter and lanes and tokens.shape[0] % (PLANE * spatial_weight.shape[1]) == 0


def choose(*args):
    if fits(args[0], args[1], args[8], args[4]):
        return in_one_kernel(*args)
    return on_device(*args)


def solution(mesh):
    return jax.shard_map(
        choose,
        mesh=mesh,
        in_specs=(
            P("fs", "tp"),
            P("fs", "tp"),
            P("fs", "tp"),
            P("tp"),
            P("tp", None, None),
            P("tp", None),
            P("tp", "fs"),
            P("tp"),
            P("fs", "tp"),
            P("fs", "tp"),
            P("tp", "fs"),
            P("tp"),
        ),
        out_specs=P("fs", "tp"),
        check_vma=False,
    )
```

```python
import functools

import jax
import jax.numpy as jnp
from jax import lax
from jax.experimental import pallas as pl
from jax.experimental.pallas import tpu as pltpu
from jax.sharding import PartitionSpec as P

EPS = 1e-05
ALPHA = 2.0**0.25


def add_rows(left, piece):
    return jnp.dot(left, piece, preferred_element_type=jnp.float32)


def scaled_rows(vals, sums, gain, count):
    mean = sums[0][:, None] / count
    square = sums[1][:, None] / count
    return (vals - mean) * lax.rsqrt(square - mean * mean + EPS) * gain[None, :]


def chip_sizes(count):
    across = 2 if count % 2 == 0 else 1
    down = 2 if (count // across) % 2 == 0 else 1
    return count // (across * down), down, across


def shift(value, sizes, axis, step=1):
    count = sizes[0] * sizes[1] * sizes[2]
    stride = sizes[1] * sizes[2] if axis == 0 else (sizes[2] if axis == 1 else 1)
    pairs = []
    for source in range(count):
        place = (source // stride) % sizes[axis]
        pairs.append((source, source + ((place + step) % sizes[axis] - place) * stride))
    return lax.ppermute(value, "fs", pairs)


def around(value, sizes, axis):
    if sizes[axis] == 4:
        near = shift(value, sizes, axis, 1)
        last = shift(value, sizes, axis, -1)
        return [value, near, shift(near, sizes, axis, 1), last]
    pieces = [value]
    for _ in range(sizes[axis] - 1):
        pieces.append(shift(pieces[-1], sizes, axis))
    return pieces


def ring(value, sizes, axis, place):
    return in_order(around(value, sizes, axis), place)


def other_core(value):
    return lax.ppermute(value, "tp", [(0, 1), (1, 0)])


def all_features(value):
    if lax.axis_size("tp") != 2:
        return lax.all_gather(value, "tp", axis=1, tiled=True)
    return jnp.concatenate(in_two(value, other_core(value), lax.axis_index("tp")), axis=1)


def in_two(mine, other, place):
    return [jnp.where(place == 0, mine, other), jnp.where(place == 0, other, mine)]


def sum_shares(terms):
    if lax.axis_size("tp") != 2:
        return lax.psum_scatter(terms, "tp", scatter_dimension=1, tiled=True)
    core = lax.axis_index("tp")
    half = terms.shape[1] // 2
    mine = lax.dynamic_slice_in_dim(terms, core * half, half, 1)
    sent = lax.dynamic_slice_in_dim(terms, (1 - core) * half, half, 1)
    return (mine.astype(jnp.float32) + other_core(sent).astype(jnp.float32)).astype(jnp.bfloat16)


def in_order(pieces, place):
    count = len(pieces)
    if count == 1:
        return pieces[0][None]
    held = jnp.zeros((count,) + pieces[0].shape, pieces[0].dtype)
    for step, piece in enumerate(pieces):
        start = lax.rem(place - step + count, count)
        held = lax.dynamic_update_slice_in_dim(held, piece[None], start, 0)
    return held


def gather_all(piece, sizes, places, order):
    held = piece
    for axis in order:
        held = ring(held, sizes, axis, places[axis])
    back = [order[::-1].index(axis) for axis in range(3)]
    rest = [3 + i for i in range(piece.ndim)]
    return jnp.transpose(held, back + rest)


def after(value, *others):
    return lax.optimization_barrier((value,) + others)[0]


def share_pieces(weight, dim, sizes, places, level, marks):
    across = sizes[2]
    width = weight.shape[dim] // across
    if across == 2:
        mine = lax.dynamic_slice_in_dim(weight, places[2] * width, width, dim)
        other = lax.dynamic_slice_in_dim(weight, (1 - places[2]) * width, width, dim)
        block = jnp.stack(in_two(mine, shift(other, sizes, 2), places[2]))
    else:
        block = weight[None]
    if sizes[0] != 4 or sizes[1] != 2:
        first = around(block, sizes, 0)
        return [[piece] if sizes[1] == 1 else [piece, shift(piece, sizes, 1)] for piece in first]
    if marks[0] is not None:
        block = after(block, marks[0])
    near, last = shift(block, sizes, 0, 1), shift(block, sizes, 0, -1)
    beside = shift(block if marks[0] is None else after(block, marks[1]), sizes, 1)
    near, last = after(near, marks[1]), after(last, marks[1])
    far = shift(near, sizes, 0)
    near_beside, last_beside = shift(near, sizes, 1), shift(last, sizes, 1)
    if level:
        far_beside = shift(after(near_beside, marks[2]), sizes, 0)
    else:
        far = after(far, marks[2])
        far_beside = shift(far, sizes, 1)
    return [[block, beside], [near, near_beside], [far, far_beside], [last, last_beside]]


def place_pieces(pieces, places):
    shape = pieces[0][0].shape
    count, down = len(pieces), len(pieces[0])
    held = jnp.zeros((count, down) + shape, pieces[0][0].dtype)
    for step, pair in enumerate(pieces):
        start = lax.rem(places[0] - step + count, count)
        for turn, piece in enumerate(pair):
            spot = places[1] if turn == 0 else 1 - places[1]
            held = lax.dynamic_update_slice(held, piece[None, None], [start, spot] + [0] * len(shape))
    return held


def on_device(
    tokens,
    u_weight,
    v_weight,
    sg_gain,
    spatial_weight,
    spatial_bias,
    out_weight,
    gain_one,
    gate_weight,
    up_weight,
    down_weight,
    gain_two,
):
    parts = lax.axis_size("tp")
    sizes = chip_sizes(lax.axis_size("fs"))
    index = lax.axis_index("fs")
    places = (index // (sizes[1] * sizes[2]), (index // sizes[2]) % sizes[1], index % sizes[2])
    whole = all_features(tokens)
    rows = whole.shape[0]
    width_sg = u_weight.shape[1]

    def add_one(piece):
        return add_rows(whole, piece)

    pre_u = add_one(gather_all(u_weight, sizes, places, [0, 1, 2]).reshape(-1, width_sg))
    pre_v = add_one(gather_all(v_weight, sizes, places, [0, 2, 1]).reshape(-1, width_sg))
    gated = jax.nn.gelu(pre_u)
    valued = jax.nn.gelu(pre_v)
    stats = lax.psum((jnp.sum(valued, axis=1), jnp.sum(valued * valued, axis=1)), "tp")
    normed = scaled_rows(valued, stats, sg_gain, width_sg * parts).astype(jnp.bfloat16)
    groups_here = spatial_weight.shape[0]
    block = spatial_weight.shape[1]
    group_width = width_sg // groups_here
    shaped = normed.reshape(rows // block, block, groups_here, group_width)
    lower = jnp.tril(jnp.ones((block, block), jnp.bool_))
    masked = jnp.where(lower[None], spatial_weight, jnp.zeros_like(spatial_weight))
    mixed = jnp.einsum("gij,njgd->nigd", masked, shaped, preferred_element_type=jnp.float32)
    mixed = mixed + spatial_bias.T[None, :, :, None]
    gated_out = (gated * mixed.reshape(rows, width_sg)).astype(jnp.bfloat16)
    out_all = gather_all(out_weight, sizes, places, [0, 1, 2])
    out_all = out_all.reshape((-1,) + out_weight.shape)
    terms = jnp.einsum("tk,nkc->tnc", gated_out, out_all, preferred_element_type=jnp.float32)
    mix = sum_shares(terms.reshape(rows, -1).astype(jnp.bfloat16))
    resid = ALPHA * tokens.astype(jnp.float32) + mix.astype(jnp.float32)
    first_sums = lax.psum((jnp.sum(resid, axis=1), jnp.sum(resid * resid, axis=1)), "tp")
    first = scaled_rows(resid, first_sums, gain_one, resid.shape[1] * parts).astype(jnp.bfloat16)
    gate_pieces = share_pieces(gate_weight, 1, sizes, places, False, (None, normed, mix))
    up_pieces = share_pieces(up_weight, 1, sizes, places, True, (None, normed, mix))
    down_pieces = share_pieces(down_weight, 0, sizes, places, False, (normed, first, first))
    gate_all = place_pieces(gate_pieces, places)
    gate_all = gate_all.reshape(-1, gate_all.shape[-1])
    up_all = place_pieces(up_pieces, places)
    up_all = up_all.reshape(-1, up_all.shape[-1])
    def feed(part):
        whole_part = all_features(part)
        gate = add_rows(whole_part, gate_all)
        upper = add_rows(whole_part, up_all)
        return (jax.nn.silu(gate) * upper).astype(jnp.bfloat16)

    two = sizes[2] == 2
    if two:
        there = feed(shift(first, sizes, 2))
        here = feed(first)
        down_pieces = [[pair[0]] + [after(piece, there, here) for piece in pair[1:]] for pair in down_pieces]
    else:
        here = feed(first)
    down_all = place_pieces(down_pieces, places)
    down_all = down_all.reshape((-1,) + down_all.shape[-2:])

    def project(hidden):
        made = jnp.einsum("tf,nfc->tnc", hidden, down_all, preferred_element_type=jnp.float32)
        return sum_shares(made.reshape(rows, -1).astype(jnp.bfloat16))

    if two:
        there = project(there)
        sent = shift(there, sizes, 2)
        ffn = project(after(here, there)).astype(jnp.float32) + sent.astype(jnp.float32)
    else:
        ffn = project(here).astype(jnp.float32)
    second = ALPHA * first.astype(jnp.float32) + ffn.astype(jnp.float32)
    last_sums = lax.psum((jnp.sum(second, axis=1), jnp.sum(second * second, axis=1)), "tp")
    return scaled_rows(second, last_sums, gain_two, second.shape[1] * parts).astype(jnp.bfloat16)


MESH = pl.DeviceIdType.MESH
PLANE = 4
CUTS = (2, 2, 4)
BLOCKS = 2
LAG = 1
RELAY_LAGS = (4, 12)
SLOTS = 4


def layer_kernel(
    sizes,
    tok_in,
    u_in,
    v_in,
    sg_gain_in,
    spatial_in,
    bias_in,
    o_in,
    gain_one_in,
    gate_in,
    up_in,
    down_in,
    resid_out,
    mine_out,
    theirs_out,
    tok,
    sg_gain,
    spatial,
    bias,
    gain_one,
    gate_own,
    up_own,
    gate_turned,
    up_turned,
    tok_o,
    u_all,
    v_all,
    o_all,
    gate_all,
    up_all,
    down_all,
    gated,
    valued,
    normed,
    gated_out,
    st_s,
    st_r,
    terms_s,
    terms_o,
    terms_r,
    resid,
    first_all,
    hidden,
    gate_acc,
    p_s,
    p_r,
    p_own,
    r_r,
    in_sem,
    out_sem,
    sg_r,
    sg_l,
    sg_z,
    sg_p,
    a2_s,
    a2_r,
    z_s,
    z_r,
    tok_sem,
    st_sem,
    terms_sem,
    first_s,
    first_r,
    swap_s,
    swap_r,
    d2_s,
    d2_r,
    rs_s,
    rs_r,
):
    nz = sizes[0]
    fs, c = lax.axis_index("fs"), lax.axis_index("tp")
    oc = 1 - c
    z, p = fs // PLANE, fs % PLANE
    y, x = p // 2, p % 2
    peers = [z * PLANE + (y + j // 2) % 2 * 2 + (x + j % 2) % 2 for j in range(PLANE)]
    inplane = [(y + j // 2) % 2 * 2 + (x + j % 2) % 2 for j in range(PLANE)]
    has_up, has_down = z < nz - 1, z > 0
    up_dev = jnp.where(has_up, fs + PLANE, fs - PLANE)
    down_dev = jnp.where(has_down, fs - PLANE, fs + PLANE)
    rows, feats = tok.shape
    kb, width_sg = u_in.shape
    depth = rows // PLANE
    quarter = hidden.shape[1]
    plane_cols = PLANE * kb

    def mult(value, by):
        return pl.multiple_of(value, by)

    def seq(k):
        swapped = jnp.where(k < 2, 1 - k, k)
        return jnp.where(z == 0, k, jnp.where(z == 1, swapped, jnp.where(z == 2, nz - 1 - swapped, nz - 1 - k)))

    def remote(src, dst, send, recv, dev, core=None):
        where_to = (dev, c if core is None else core)
        return pltpu.make_async_remote_copy(
            src_ref=src, dst_ref=dst, send_sem=send, recv_sem=recv, device_id=where_to, device_id_type=MESH
        )

    def start_if(pred, copy):
        pl.when(pred)(lambda: copy.start())

    def sent_if(pred, copy):
        pl.when(pred)(lambda: copy.wait_send())

    own_rows = pl.ds(mult(fs * kb, kb), kb)
    own_quarter = pl.ds(mult(p * quarter, 16), quarter)
    loads = [
        (gate_in, gate_own),
        (up_in, up_own),
        (u_in, u_all.at[own_rows, :]),
        (v_in, v_all.at[own_rows, :]),
        (o_in, o_all.at[:, own_rows]),
        (down_in.at[own_quarter, :], down_all.at[:, own_rows]),
        (tok_in, tok),
        (sg_gain_in, sg_gain),
        (spatial_in, spatial),
        (bias_in, bias),
        (gain_one_in, gain_one),
    ]
    loads = [pltpu.make_async_copy(src, dst, in_sem.at[i]) for i, (src, dst) in enumerate(loads)]
    for load in loads:
        load.start()
    barrier = pltpu.get_barrier_semaphore()
    for dev, core in [(fs, oc)] + [(peers[j], c) for j in range(1, PLANE)]:
        pl.semaphore_signal(barrier, inc=1, device_id=(dev, core), device_id_type=MESH)
    for pred, dev in [(has_up, up_dev), (has_down, down_dev)]:
        @pl.when(pred)
        def _():
            pl.semaphore_signal(barrier, inc=1, device_id=(dev, c), device_id_type=MESH)
    pl.semaphore_wait(barrier, PLANE + jnp.where(has_up, 1, 0) + jnp.where(has_down, 1, 0))

    def rows_of(ref):
        return lambda i, count=1: ref.at[pl.ds(mult(i * kb, kb), count * kb), :]

    def cols_of(ref, part):
        height = width_sg // 2
        return lambda i, count=1: ref.at[pl.ds(part * height, height), pl.ds(mult(i * kb, kb), count * kb)]

    half_o = width_sg // 2
    items = [
        (u_in, rows_of(u_all), 1, 2),
        (v_in, rows_of(v_all), 2, 1),
        (o_in.at[pl.ds(0, half_o), :], cols_of(o_all, 0), 1, 2),
        (o_in.at[pl.ds(half_o, half_o), :], cols_of(o_all, 1), 2, 1),
    ]

    def own_copies(n):
        src, at, one, two = items[n]
        return [
            (has_up, remote(src, at(fs), sg_z.at[n, 0], sg_r.at[n, z, 0], up_dev)),
            (has_down, remote(src, at(fs), sg_z.at[n, 1], sg_r.at[n, z, 0], down_dev)),
            (None, remote(src, at(fs), sg_p.at[n], sg_r.at[n, z, 1], peers[one])),
            (None, remote(src, at(fs), sg_p.at[n], sg_l.at[n], peers[two])),
        ]

    def own_start(n):
        for pred, copy in own_copies(n):
            if pred is None:
                copy.start()
            else:
                start_if(pred, copy)

    def forward_to(b):
        going_up = b < z
        dev = jnp.where(going_up, up_dev, down_dev)
        return (going_up & has_up) | ((b > z) & has_down), dev, jnp.where(going_up, 0, 1)

    def column_copies(n, k):
        _, at, one, two = items[n]
        b = seq(k)
        idx = b * PLANE + p
        pred, dev, way = forward_to(b)
        ref = at(idx)
        return [
            (pred, remote(ref, ref, sg_z.at[n, way], sg_r.at[n, b, 0], dev)),
            (None, remote(ref, ref, sg_p.at[n], sg_r.at[n, b, 1], peers[one])),
            (None, remote(ref, ref, sg_p.at[n], sg_l.at[n], peers[two])),
        ]

    def column(n, k):
        copies = column_copies(n, k)
        copies[0][1].wait_recv()
        start_if(*copies[0])
        copies[1][1].start()
        copies[2][1].start()

    def beside(n, k):
        _, at, one, two = items[n]
        b = seq(k)
        ref = at(b * PLANE + inplane[one])
        remote(ref, ref, sg_p.at[n], sg_r.at[n, b, 1], peers[one]).wait_recv()
        remote(ref, ref, sg_p.at[n], sg_l.at[n], peers[two]).start()

    def gathered(n):
        ref = items[n][1](0, 2 * nz)
        remote(ref, ref, sg_p.at[n], sg_l.at[n], peers[1]).wait_recv()

    wides = [(gate_turned, gate_all), (up_turned, up_all), (down_in, down_all)]

    def quarter_copy(w, j):
        src, dst = wides[w]
        theirs = pl.ds(mult(inplane[j] * quarter, 16), quarter)
        mine = pl.ds(mult(fs * kb, kb), kb)
        return remote(src.at[theirs, :], dst.at[:, mine], a2_s.at[w], a2_r.at[w], peers[j])

    def quarters_all(w):
        ref = wides[w][1].at[:, pl.ds(0, (PLANE - 1) * kb)]
        return remote(ref, ref, a2_s.at[w], a2_r.at[w], peers[1])

    def quarters_start(w):
        for j in range(1, PLANE):
            quarter_copy(w, j).start()

    def block(w, b, h):
        cols = plane_cols // CUTS[w]
        return wides[w][1].at[:, pl.ds(mult(b * plane_cols + h * cols, cols), cols)]

    def z_recv(w, b, h):
        return z_r.at[sum(CUTS[:w]) * nz + b * CUTS[w] + h]

    def own_block_copies(w, h):
        ref, recv = block(w, z, h), z_recv(w, z, h)
        return [
            (has_up, remote(ref, ref, z_s.at[w, 0], recv, up_dev)),
            (has_down, remote(ref, ref, z_s.at[w, 1], recv, down_dev)),
        ]

    def own_block(w):
        quarters_all(w).wait_recv()
        for h in range(CUTS[w]):
            for pred, copy in own_block_copies(w, h):
                start_if(pred, copy)

    def pass_copy(w, k, h):
        b = seq(k)
        pred, dev, way = forward_to(b)
        ref = block(w, b, h)
        return pred, remote(ref, ref, z_s.at[w, way], z_recv(w, b, h), dev)

    def blocks_sent(ref_of, sems):
        for n in range(1, nz):
            ref = ref_of(n)
            up = remote(ref, ref, sems(0), sems(0), fs)
            down = remote(ref, ref, sems(1), sems(1), fs)
            pl.when(has_up & (z + 1 == n))(lambda: up.wait_send())
            pl.when(has_down & (nz - z == n))(lambda: down.wait_send())

    def pass_on(w, k, h):
        pred, copy = pass_copy(w, k, h)

        @pl.when(pred)
        def _():
            copy.wait_recv()
            copy.start()

    def need(w, k, h):
        pred, copy = pass_copy(w, k, h)
        pl.when(jnp.logical_not(pred))(lambda: copy.wait_recv())

    lane = lax.broadcasted_iota(jnp.int32, (depth, 128), 1)

    def put_stats(which, place, vals):
        one = jnp.sum(vals, axis=1, keepdims=True)
        two = jnp.sum(vals * vals, axis=1, keepdims=True)
        st_s[which, place, :] = jnp.where(lane == 0, one, two)

    def stats_copy(which):
        theirs = theirs_out if which == 2 else st_r.at[which]
        return remote(st_s.at[which], theirs, st_sem.at[which, 0], st_sem.at[which, 1], fs, oc)

    def normalize(which, place, vals, gain, count):
        both = st_s[which, place, :] + st_r[which, place, :]
        mean = both[:, 0:1] / count
        square = both[:, 1:2] / count
        return (vals - mean) * lax.rsqrt(square - mean * mean + EPS) * gain

    def loop(count, body):
        lax.fori_loop(0, count, lambda i, carry: (body(i), carry)[1], 0)

    def part(i):
        return pl.ds(mult(i * depth, depth), depth)

    tok_copy = remote(tok_in, tok_o, tok_sem.at[0], tok_sem.at[1], fs, oc)
    own_start(0)
    own_start(1)

    def turn(src, dst):
        def step(i):
            place = pl.ds(mult(i * kb, kb), kb)
            dst[place, :] = src[:, place].T

        loop(src.shape[1] // kb, step)

    loads[0].wait()
    turn(gate_own, gate_turned)
    quarters_start(0)
    own_start(2)
    own_start(3)
    tok_copy.start()
    for load in loads[1:]:
        load.wait()
    turn(up_own, up_turned)
    gate_all[:, own_rows] = gate_turned[own_quarter, :]
    up_all[:, own_rows] = up_turned[own_quarter, :]

    for n in (0, 1):
        column(n, 1)
    for n in (0, 1):
        column(n, 2)
    for n in (2, 3):
        column(n, 1)
    for n in (0, 1):
        column(n, 3)
    for n in (2, 3):
        column(n, 2)
    own_block(0)
    for k in (0, 1):
        for n in (0, 1):
            beside(n, k)
    for n in (2, 3):
        column(n, 3)
    pass_on(0, 1, 0)
    pass_on(0, 2, 0)
    for n in (0, 1):
        beside(n, 2)
    pass_on(0, 1, 1)
    pass_on(0, 2, 1)
    for n in (0, 1):
        beside(n, 3)
    quarters_start(1)
    for n in (2, 3):
        beside(n, 0)
    for n in (2, 3):
        beside(n, 1)
    pass_on(0, 3, 0)
    for n in (2, 3):
        beside(n, 2)

    tok_copy.wait_recv()
    wide = 256
    mine_k = pl.ds(mult(c * feats, feats), feats)
    their_k = pl.ds(mult(oc * feats, feats), feats)

    def branch(weight, into):
        def step(n):
            cols = pl.ds(mult(n * wide, wide), wide)
            acc = add_rows(tok[...], weight[mine_k, cols]) + add_rows(tok_o[...], weight[their_k, cols])
            into[:, cols] = jax.nn.gelu(acc)

        loop(width_sg // wide, step)

    gathered(0)
    branch(u_all, gated)
    gathered(1)
    branch(v_all, valued)
    for n in (2, 3):
        beside(n, 3)
    pass_on(0, 3, 1)
    loop(rows // depth, lambda i: put_stats(0, part(i), valued[part(i), :]))
    stats_copy(0).start()
    stats_copy(0).wait_recv()

    def norm_gate(i):
        vals = normalize(0, part(i), valued[part(i), :], sg_gain[...], 2 * width_sg)
        normed[part(i), :] = vals.astype(jnp.bfloat16)

    loop(rows // depth, norm_gate)
    groups, spread = spatial.shape[0], spatial.shape[1]
    row_at = lax.broadcasted_iota(jnp.int32, (spread, spread), 0)
    col_at = lax.broadcasted_iota(jnp.int32, (spread, spread), 1)
    group_dim = width_sg // groups

    def mix_block(n):
        place = pl.ds(mult(n * spread, spread), spread)
        for g in range(groups):
            cols = pl.ds(g * group_dim, group_dim)
            weight = jnp.where(col_at <= row_at, spatial[g], jnp.zeros_like(spatial[g]))
            shift_by = jnp.sum(jnp.where(col_at == row_at, bias[g : g + 1, :], 0.0), axis=1, keepdims=True)
            mixed = jnp.dot(weight, normed[place, cols], preferred_element_type=jnp.float32) + shift_by
            gated_out[place, cols] = (gated[place, cols] * mixed).astype(jnp.bfloat16)

    loop(rows // spread, mix_block)
    for n in (2, 3):
        gathered(n)

    def project_out(which, into):
        def step(n):
            cols = pl.ds(mult(which * feats + n * wide, wide), wide)
            to = pl.ds(mult(n * wide, wide), wide)
            into[:, to] = add_rows(gated_out[...], o_all[:, cols]).astype(jnp.bfloat16)

        loop(feats // wide, step)

    project_out(oc, terms_s)
    terms_copy = remote(terms_s, terms_r, terms_sem.at[0], terms_sem.at[1], fs, oc)
    terms_copy.start()
    project_out(c, terms_o)
    own_block(1)
    terms_copy.wait_recv()

    def add_mix(i):
        mix = terms_o[part(i), :].astype(jnp.float32) + terms_r[part(i), :].astype(jnp.float32)
        vals = ALPHA * tok[part(i), :].astype(jnp.float32) + mix.astype(jnp.bfloat16).astype(jnp.float32)
        resid[part(i), :] = vals
        put_stats(1, part(i), vals)

    loop(rows // depth, add_mix)
    stats_copy(1).start()
    stats_copy(1).wait_recv()
    mine_cols = pl.ds(mult(c * feats, feats), feats)
    their_cols = pl.ds(mult(oc * feats, feats), feats)

    def norm_first(i):
        vals = normalize(1, part(i), resid[part(i), :], gain_one[...], 2 * feats)
        vals = vals.astype(jnp.bfloat16)
        first_all[pl.ds(mult(p * rows + i * depth, depth), depth), mine_cols] = vals
        resid[part(i), :] = ALPHA * vals.astype(jnp.float32)

    loop(rows // depth, norm_first)

    def place_of(j):
        return (y + j // 2) % 2 * 2 + (x + j % 2) % 2

    def tokens_of(j, cols):
        return first_all.at[pl.ds(mult(place_of(j) * rows, rows), rows), cols]

    def swap_copy(j):
        ref = tokens_of(j, mine_cols)
        return remote(ref, ref, swap_s, swap_r.at[j], fs, oc)

    own_tokens = tokens_of(0, mine_cols)
    first_copies = [
        remote(own_tokens, own_tokens, first_s, first_r.at[j], peers[j]) for j in (1, 2)
    ]

    def corner_copy(j):
        start = mult(place_of(j) * rows + (j - 1) * (rows // 2), rows // 2)
        ref = first_all.at[pl.ds(start, rows // 2), mine_cols]
        return remote(ref, ref, first_s, first_r.at[j + 2], z * PLANE + place_of(PLANE - 1 - j))

    swap_copy(0).start()
    for copy in first_copies:
        copy.start()
    quarters_start(2)

    for k in range(1, nz):
        for h in range(CUTS[0]):
            need(0, k, h)

    tiles = [(t, min(wide, quarter - t)) for t in range(0, quarter, wide)]

    def across(left, weight, t, n):
        return lax.dot_general(
            left, weight[pl.ds(t, n), :], (((1,), (1,)), ((), ())), preferred_element_type=jnp.float32
        )

    def row_block(j):
        return pl.ds(mult(place_of(j) * rows, rows), rows)

    def gate_step(j):
        @pl.when((j == 1) | (j == 2))
        def _():
            ref = tokens_of(j, mine_cols)
            remote(ref, ref, first_s, first_r.at[j], fs, oc).wait_recv()
            corner_copy(j).start()

        @pl.when(j == PLANE - 1)
        def _():
            for half in (0, 1):
                start = mult(place_of(j) * rows + half * (rows // 2), rows // 2)
                ref = first_all.at[pl.ds(start, rows // 2), mine_cols]
                remote(ref, ref, first_s, first_r.at[half + 3], fs, oc).wait_recv()

        @pl.when(j > 0)
        def _():
            swap_copy(j).start()

        ref = tokens_of(j, their_cols)
        remote(ref, ref, swap_s, swap_r.at[j], fs, oc).wait_recv()
        left = row_block(j)
        for t, n in tiles:
            gate_acc[left, pl.ds(t, n)] = jax.nn.silu(across(first_all[left, :], gate_all, t, n))

        @pl.when(j == 0)
        def _():
            for h in range(CUTS[1]):
                pass_on(1, 1, h)
                pass_on(1, 2, h)

        @pl.when((j == 1) | (j == 2))
        def _():
            pass_on(1, 3, j - 1)

        pl.when(j == 2)(lambda: own_block(2))

    loop(PLANE, gate_step)
    for k in range(1, nz):
        for h in range(CUTS[1]):
            need(1, k, h)

    def up_step(j):
        left = row_block(j)
        for t, n in tiles:
            acc = gate_acc[left, pl.ds(t, n)] * across(first_all[left, :], up_all, t, n)
            hidden[left, pl.ds(t, n)] = acc.astype(jnp.bfloat16)

    terms_copy.wait_send()

    cut = CUTS[2]
    half_cols = plane_cols // cut
    steps = nz * cut
    per_core = steps // 2
    pair = 2
    early = cut // pair * PLANE
    first_units = (nz - 1) * early
    last_units = cut * PLANE

    def turn_of(order):
        return jnp.where(order == 0, PLANE - 1, jnp.where(order == PLANE - 1, 0, order))

    def wide_unit(t):
        per = cut // pair
        order = jnp.where(t < early, t // per, (t - early) % PLANE)
        i = jnp.where(t < early, t % per, per + (t - early) // PLANE)
        inner = (i >= per) & has_up & has_down
        k = jnp.where(inner, 1 + i % 2, i // per)
        h = jnp.where(inner, (i - per) // 2, i % per)
        at = seq(k) * per + h
        own = per_core // pair
        return order, turn_of(order), k, h * pair, at * pair, at // own == c, at % own * pair, at % own, 1 + at % 2

    def last_unit(t):
        h, order = t // PLANE, t % PLANE
        at = seq(nz - 1) * cut + h
        return order, turn_of(order), nz - 1, h, at, at // per_core == c, at % per_core, per_core // pair + h, 0

    def pair_copy(unit, pieces, t):
        _, j, _, _, _, _, q, sem, _ = unit(t)
        ref = (pl.ds(q, pieces), row_block(j))
        return remote(p_s.at[ref], p_r.at[ref], d2_s, d2_r.at[sem, j], fs, oc)

    def rows_copy(unit, pieces, t):
        _, j, _, _, _, _, q, sem, via = unit(t)
        pick = jnp.maximum(j - 1, 0)
        corner = j == PLANE - 1
        relayed = pieces == pair
        recv = jnp.where(corner, 2 + sem if relayed else 1, 0)
        dev = z * PLANE + place_of(jnp.where(corner, via, j) if relayed else j)
        span = pl.ds(q, pieces)
        return remote(p_r.at[span, row_block(j)], r_r.at[pick, span], rs_s, rs_r.at[recv], dev)

    def held(unit, t):
        _, j, _, _, _, _, _, _, via = unit(t)
        return (via > 0) & (j == 3 - via)

    def finish(unit, pieces, t):
        _, j, _, _, _, mine, q, _, _ = unit(t)

        @pl.when(mine)
        def _():
            pair_copy(unit, pieces, t).wait_recv()
            place = row_block(j)
            for e in range(pieces):
                both = p_own[t % SLOTS, :, pl.ds(e * half_cols, half_cols)].astype(jnp.float32)
                both = both + p_r[q + e, place, :].astype(jnp.float32)
                p_r[q + e, place, :] = both.astype(jnp.bfloat16)
            pl.when((j > 0) & jnp.logical_not(held(unit, t)))(lambda: rows_copy(unit, pieces, t).start())

    def relay(t):
        _, j, _, _, _, mine, q, sem, _ = wide_unit(t)

        @pl.when(mine & held(wide_unit, t))
        def _():
            ref = r_r.at[PLANE - 2, pl.ds(q, pair)]
            remote(ref, ref, rs_s, rs_r.at[2 + sem], peers[1]).wait_recv()
            place = row_block(j)
            for e in range(pair):
                both = r_r[PLANE - 2, q + e].astype(jnp.float32) + p_r[q + e, place, :].astype(jnp.float32)
                p_r[q + e, place, :] = both.astype(jnp.bfloat16)
            rows_copy(wide_unit, pair, t).start()

    def project(unit, pieces, t):
        _, j, _, _, at, mine, q, _, _ = unit(t)
        from_cols = pl.ds(mult(at * half_cols, pieces * half_cols), pieces * half_cols)
        place = row_block(j)
        made = add_rows(hidden[place, :], down_all[:, from_cols]).astype(jnp.bfloat16)

        @pl.when(mine)
        def _():
            p_own[t % SLOTS, :, pl.ds(0, pieces * half_cols)] = made

        @pl.when(jnp.logical_not(mine))
        def _():
            for e in range(pieces):
                p_s[q + e, place, :] = made[:, e * half_cols : (e + 1) * half_cols]
            pair_copy(unit, pieces, t).start()

    relay_lag = jnp.where(has_up & has_down, RELAY_LAGS[1], RELAY_LAGS[0])

    def wide_step(t):
        order, j, k, h = wide_unit(t)[:4]
        pl.when((t < early) & (t % (cut // pair) == 0))(lambda: up_step(j))

        @pl.when((t % (early // cut) == 0) & (t > 0) & (t <= early))
        def _():
            pass_on(2, 1, t // (early // cut) - 1)
            pass_on(2, 2, t // (early // cut) - 1)

        @pl.when((k > 0) & (order == 0))
        def _():
            for e in range(pair):
                need(2, k, h + e)

        project(wide_unit, pair, t)
        pl.when(t >= LAG)(lambda: finish(wide_unit, pair, t - LAG))
        pl.when(t >= relay_lag)(lambda: relay(t - relay_lag))

    def last_step(t):
        order, _, k, h = last_unit(t)[:4]

        @pl.when(order == 0)
        def _():
            pass_on(2, k, h)
            need(2, k, h)

        project(last_unit, 1, t)
        pl.when(t >= LAG)(lambda: finish(last_unit, 1, t - LAG))
        pl.when(t < relay_lag)(lambda: relay(first_units - relay_lag + t))

    loop(first_units, wide_step)
    loop(LAG, lambda i: finish(wide_unit, pair, first_units - LAG + i))
    loop(last_units, last_step)
    loop(LAG, lambda i: finish(last_unit, 1, last_units - LAG + i))

    ref = r_r.at[pl.ds(0, 2)]
    remote(ref, ref, rs_s, rs_r.at[0], peers[1]).wait_recv()
    direct = seq(nz - 1)

    @pl.when(direct * cut // per_core == c)
    def _():
        ref = r_r.at[PLANE - 2, pl.ds(0, cut)]
        remote(ref, ref, rs_s, rs_r.at[1], peers[1]).wait_recv()

    def add_ffn(i):
        for q in range(per_core):
            cols = pl.ds(q * half_cols, half_cols)
            total = p_r[q, pl.ds(mult(p * rows + i * depth, depth), depth), :].astype(jnp.float32)
            for j in (1, 2):
                total = total + r_r[j - 1, q, part(i), :].astype(jnp.float32)
            corner = r_r[PLANE - 2, q, part(i), :].astype(jnp.float32)
            total = total + jnp.where((c * per_core + q) // cut == direct, corner, 0.0)
            resid[part(i), cols] = resid[part(i), cols] + total.astype(jnp.bfloat16).astype(jnp.float32)
        resid_copy(i).start()
        put_stats(2, part(i), resid[part(i), :])

    def resid_copy(i):
        return pltpu.make_async_copy(resid.at[part(i), :], resid_out.at[part(i), :], out_sem.at[i])

    loop(rows // depth, add_ffn)
    stats_copy(2).start()
    mine_copy = pltpu.make_async_copy(st_s.at[2], mine_out, out_sem.at[rows // depth])
    mine_copy.start()

    tok_copy.wait_send()
    stats_copy(0).wait_send()
    stats_copy(1).wait_send()
    ref = first_all.at[pl.ds(0, (PLANE - 1) * rows), pl.ds(0, feats)]
    remote(ref, ref, first_s, first_s, peers[1]).wait_send()
    ref = first_all.at[pl.ds(0, PLANE * rows), pl.ds(0, feats)]
    remote(ref, ref, swap_s, swap_s, fs, oc).wait_send()
    for n in range(len(items)):
        ref = items[n][1](0, 3 * nz)
        remote(ref, ref, sg_p.at[n], sg_l.at[n], peers[1]).wait_send()
        blocks_sent(lambda count: items[n][1](0, count), lambda way: sg_z.at[n, way])
    for w in range(len(wides)):
        quarters_all(w).wait_send()
        blocks_sent(lambda count: wides[w][1].at[:, pl.ds(0, count * plane_cols)], lambda way: z_s.at[w, way])
    remote(p_s, p_r, d2_s, d2_s, fs, oc).wait_send()
    remote(r_r, r_r, rs_s, rs_r.at[0], peers[1]).wait_send()
    loop(rows // depth, lambda i: resid_copy(i).wait())
    mine_copy.wait()
    stats_copy(2).wait()


def last_norm(count, second, mine, theirs, gain, out):
    both = mine[...] + theirs[...]
    mean = both[:, 0:1] / count
    square = both[:, 1:2] / count
    out[...] = ((second[...] - mean) * lax.rsqrt(square - mean * mean + EPS) * gain[...]).astype(out.dtype)


def in_one_kernel(*args):
    (tokens, u_weight, v_weight, sg_gain, spatial, bias, out_weight, gain_one, gate, up, down, gain_two) = args
    nz = lax.axis_size("fs") // PLANE
    rows, feats = tokens.shape
    width_sg = u_weight.shape[1]
    quarter = down.shape[0] // PLANE
    wide = 2 * feats
    plane_rows = PLANE * rows
    bf16, f32 = jnp.bfloat16, jnp.float32
    vmem, dma = pltpu.VMEM, pltpu.SemaphoreType.DMA
    steps = nz * CUTS[2]
    half_cols = wide // steps
    scratch = [
        vmem((rows, feats), bf16),
        vmem((1, width_sg), f32),
        vmem(spatial.shape, bf16),
        vmem(bias.shape, f32),
        vmem((1, feats), f32),
        vmem(gate.shape, bf16),
        vmem(gate.shape, bf16),
        vmem(gate.shape[::-1], bf16),
        vmem(gate.shape[::-1], bf16),
        vmem((rows, feats), bf16),
        vmem((wide, width_sg), bf16),
        vmem((wide, width_sg), bf16),
        vmem((width_sg, wide), bf16),
        vmem((quarter, wide), bf16),
        vmem((quarter, wide), bf16),
        vmem((quarter, wide), bf16),
        vmem((rows, width_sg), f32),
        vmem((rows, width_sg), f32),
        vmem((rows, width_sg), bf16),
        vmem((rows, width_sg), bf16),
        vmem((3, rows, 128), f32),
        vmem((3, rows, 128), f32),
        vmem((rows, feats), bf16),
        vmem((rows, feats), bf16),
        vmem((rows, feats), bf16),
        vmem((rows, feats), f32),
        vmem((plane_rows, wide), bf16),
        vmem((plane_rows, quarter), bf16),
        vmem((plane_rows, quarter), f32),
        vmem((steps // 2, plane_rows, half_cols), bf16),
        vmem((steps // 2, plane_rows, half_cols), bf16),
        vmem((SLOTS, rows, 2 * half_cols), bf16),
        vmem((PLANE - 1, steps // 2, rows, half_cols), bf16),
        dma((11,)),
        dma((PLANE + 1,)),
        dma((4, nz, 2)),
        dma((4,)),
        dma((4, 2)),
        dma((4,)),
        dma((3,)),
        dma((3,)),
        dma((3, 2)),
        dma((sum(CUTS) * nz,)),
        dma((2,)),
        dma((3, 2)),
        dma((2,)),
        dma(()),
        dma((PLANE + 1,)),
        dma(()),
        dma((PLANE,)),
        dma(()),
        dma((steps // 2, PLANE)),
        dma(()),
        dma((2 + steps // 4,)),
    ]
    spec = pl.BlockSpec(memory_space=pl.ANY)
    stats = jax.ShapeDtypeStruct((rows, 128), f32)
    second, mine, theirs = pl.pallas_call(
        functools.partial(layer_kernel, (nz,)),
        name="layer",
        out_shape=(jax.ShapeDtypeStruct((rows, feats), f32), stats, stats),
        in_specs=[spec] * 11,
        out_specs=(spec, spec, spec),
        scratch_shapes=scratch,
        compiler_params=pltpu.CompilerParams(
            collective_id=0, has_side_effects=True, vmem_limit_bytes=67_043_328
        ),
    )(
        tokens,
        u_weight,
        v_weight,
        sg_gain[None],
        spatial,
        bias,
        out_weight,
        gain_one[None],
        gate,
        up,
        down,
    )
    tall = rows // BLOCKS
    each = pl.BlockSpec((tall, feats), lambda i: (i, 0))
    few = pl.BlockSpec((tall, 128), lambda i: (i, 0))
    return pl.pallas_call(
        functools.partial(last_norm, wide),
        name="last_norm",
        out_shape=jax.ShapeDtypeStruct((rows, feats), tokens.dtype),
        grid=(BLOCKS,),
        in_specs=[each, few, few, pl.BlockSpec((1, feats), lambda i: (0, 0))],
        out_specs=each,
    )(second, mine, theirs, gain_two[None])


def fits(tokens, u_weight, gate_weight, spatial_weight):
    if lax.axis_size("tp") != 2 or lax.axis_size("fs") != 4 * PLANE:
        return False
    quarter = gate_weight.shape[1] % PLANE == 0 and gate_weight.shape[1] // PLANE % 16 == 0
    lanes = u_weight.shape[0] % 128 == 0 and u_weight.shape[1] % 256 == 0
    return quarter and lanes and tokens.shape[0] % (PLANE * spatial_weight.shape[1]) == 0


def choose(*args):
    if fits(args[0], args[1], args[8], args[4]):
        return in_one_kernel(*args)
    return on_device(*args)


def solution(mesh):
    return jax.shard_map(
        choose,
        mesh=mesh,
        in_specs=(
            P("fs", "tp"),
            P("fs", "tp"),
            P("fs", "tp"),
            P("tp"),
            P("tp", None, None),
            P("tp", None),
            P("tp", "fs"),
            P("tp"),
            P("fs", "tp"),
            P("fs", "tp"),
            P("tp", "fs"),
            P("tp"),
        ),
        out_specs=P("fs", "tp"),
        check_vma=False,
    )
```
